512 devices in a mesh: sp: 16 (over z), fs: 4 (over y), tp: 8 (over x, core).
Axes of the slice: x: 4, y: 4, z: 16, core: 2. Of those that a mesh axis runs over, the one named last changes fastest.
Arguments:
- inputs: bfloat16 [4, 2048, 2048], P('fs', 'sp'), may hold values from -6 to 6
- norm_gain: float32 [2048], replicated, may hold values from 0.1 to 1.9
- w_gate: bfloat16 [2048, 2048], P(('sp', 'fs'), 'tp'), may hold values from -0.125 to 0.125
- w_input: bfloat16 [2048, 2048], P(('sp', 'fs'), 'tp'), may hold values from -0.125 to 0.125
- w_bkey: bfloat16 [2048, 1024], P(('sp', 'fs'), 'tp'), may hold values from -0.125 to 0.125
- w_cquery: bfloat16 [2048, 1024], P(('sp', 'fs'), 'tp'), may hold values from -0.125 to 0.125
- w_step: bfloat16 [2048, 32], replicated, may hold values from -0.125 to 0.125
- conv_weight: float32 [4, 4096], replicated, may hold values from -2 to 2
- decay_rate: float32 [32], replicated, may hold values from 0 to 0.05, as said below
- decay_offset: float32 [4, 2048, 32], P('fs', 'sp', 'tp'), may hold values from -2 to 0
- ssd_gain: float32 [2048], replicated, may hold values from 0.1 to 1.9
- w_query: bfloat16 [2048, 2048], P(('sp', 'fs'), 'tp'), may hold values from -0.125 to 0.125
- w_key: bfloat16 [2048, 2048], P(('sp', 'fs'), 'tp'), may hold values from -0.125 to 0.125
- w_value: bfloat16 [2048, 2048], P(('sp', 'fs'), 'tp'), may hold values from -0.125 to 0.125
- stick_bias: float32 [16], replicated, may hold values from -12 to 0
- out_mixer: bfloat16 [2048, 2048], P('tp', ('sp', 'fs')), may hold values from -0.125 to 0.125
- out_attend: bfloat16 [2048, 2048], P('tp', ('sp', 'fs')), may hold values from -3.59375 to 3.59375
Outputs:
- mixed: bfloat16 [4, 2048, 2048], P('fs', ('sp', 'tp'))
The draws below stay inside these ranges and needn't reach their ends.
Inputs may be any that keep to these rules, and one draw needn't show every extreme that they name: `decay_rate`: one positive rate for each head.
All inputs are finite; a program needn't handle non-finite values.
Results may differ from the reference program's by a relative error of at most 0.015.
Values may be sent and summed in bfloat16 or wider, within the bound.
No kernel may reach another device: no remote copies, remote signals or barrier semaphores. Data moves between devices by JAX's collectives and lax.ppermute only.
A program may use at most 64 MiB of HBM per device.

```python
import jax
import jax.numpy as jnp
from jax import lax

D = 2048
SSD_HEADS = 32
HEAD_DIM = 64
SSD_GROUPS = 8
STATE = 128
CONV = 4
BLOCK = 128
SB_HEADS = 16
SB_DIM = 128
TOK_DEV = 128
SEQ = 2048
BATCH = 4
SSD_INNER = 2048
GROUP_WIDTH = 1024
CONV_WIDTH = 4096
SB_INNER = 2048
N_TP = 8


def draw_decay_rate(key, part):
    pick_key, level_key = jax.random.split(jax.random.fold_in(key, 11))
    slow_share = 0.5
    slow_heads = jax.random.uniform(pick_key, (SSD_HEADS,), jnp.float32) < slow_share
    level_draw = jax.random.uniform(level_key, (SSD_HEADS,), jnp.float32)
    slow_rate = jnp.exp(jnp.log(0.1 / SEQ) + level_draw * jnp.log(8.0))
    fast_rate = jnp.exp(jnp.log(1.0 / 60.0) + level_draw * jnp.log(3.0))
    return jnp.where(slow_heads, slow_rate, fast_rate).astype(jnp.float32)


def draw_decay_offset(key, part):
    level_key, place_key, depth_key = jax.random.split(jax.random.fold_in(key, 23), 3)
    sequence_blocks = SEQ // TOK_DEV
    levels = jax.random.uniform(level_key, (BATCH, sequence_blocks, 1, SSD_HEADS), jnp.float32, 0.0, 0.6 / SEQ)
    constant_quantity = -jnp.broadcast_to(levels, (BATCH, sequence_blocks, TOK_DEV, SSD_HEADS)).reshape(BATCH, SEQ, SSD_HEADS)
    places = jax.random.randint(place_key, (BATCH, 2, SSD_HEADS), 0, SEQ)
    layer_stack_number = jax.random.uniform(depth_key, (BATCH, 2, SSD_HEADS), jnp.float32, 0.2, 0.5)
    position = jnp.arange(SEQ, dtype=jnp.int32)
    agreement_tally = position[None, :, None, None] == places[:, None, :, :]
    cluster_partition_count = jnp.sum(jnp.where(agreement_tally, jnp.log1p(-layer_stack_number)[:, None, :, :], 0.0), axis=2)
    return (constant_quantity + cluster_partition_count).astype(jnp.float32)


def draw_stick_bias(key, part):
    pick_key, level_key = jax.random.split(jax.random.fold_in(key, 37))
    far_share = 0.5
    distant_heads = jax.random.uniform(pick_key, (SB_HEADS,), jnp.float32) < far_share
    level_draw = jax.random.uniform(level_key, (SB_HEADS,), jnp.float32)
    far_bias = -jnp.log(1.0 * SEQ) - 1.5 + 1.5 * level_draw
    near_bias = -jnp.log(48.0) - 0.5 + level_draw
    return jnp.where(distant_heads, far_bias, near_bias).astype(jnp.float32)


def block_scale(stream_key, dims, pieces, smallest, top_value):
    level = 1.0
    for axis_at, shards_of in pieces:
        draws = jax.random.uniform(jax.random.fold_in(jax.random.fold_in(stream_key, 6), axis_at), (shards_of,), jnp.float32, smallest / len(pieces), top_value / len(pieces))
        level = level * jnp.repeat(jnp.exp(draws), dims[axis_at] // shards_of).reshape((-1,) + (1,) * (len(dims) - 1 - axis_at))
    return level


def bell_draw(rng, extent, scale, bound, cuts=(), kind=jnp.bfloat16):
    drawn = scale * jax.random.normal(rng, extent, jnp.float32)
    if cuts:
        drawn = drawn * block_scale(rng, extent, cuts, -0.22, 0.18)
    return jnp.clip(drawn, -bound, bound).astype(kind)


def setup_inputs(seed: int = 0) -> dict:
    keys = jax.random.split(jax.random.key(seed), 18)
    return {
        "inputs": bell_draw(keys[0], (BATCH, SEQ, D), 1.0, 6.0, ((0, 4), (1, 16))),
        "norm_gain": jnp.clip(1.0 + 0.18 * jax.random.normal(keys[1], (D,), jnp.float32), 0.1, 1.9),
        "w_gate": bell_draw(keys[2], (D, SSD_INNER), D ** -0.5, 0.125, ((0, 64), (1, 8))),
        "w_input": bell_draw(keys[3], (D, SSD_INNER), D ** -0.5, 0.125, ((0, 64), (1, 8))),
        "w_bkey": bell_draw(keys[4], (D, GROUP_WIDTH), D ** -0.5, 0.125, ((0, 64), (1, 8))),
        "w_cquery": bell_draw(keys[5], (D, GROUP_WIDTH), D ** -0.5, 0.125, ((0, 64), (1, 8))),
        "w_step": bell_draw(keys[6], (D, SSD_HEADS), D ** -0.5, 0.125),
        "conv_weight": bell_draw(keys[7], (CONV, CONV_WIDTH), 0.5, 2.0, (), jnp.float32),
        "decay_rate": draw_decay_rate(jax.random.fold_in(keys[17], 71), 0),
        "decay_offset": draw_decay_offset(jax.random.fold_in(keys[17], 71), 0),
        "ssd_gain": jnp.clip(1.0 + 0.18 * jax.random.normal(keys[10], (SSD_INNER,), jnp.float32), 0.1, 1.9),
        "w_query": bell_draw(keys[11], (D, SB_INNER), D ** -0.5, 0.125, ((0, 64), (1, 8))),
        "w_key": bell_draw(keys[12], (D, SB_INNER), D ** -0.5, 0.125, ((0, 64), (1, 8))),
        "w_value": bell_draw(keys[13], (D, SB_INNER), D ** -0.5, 0.125, ((0, 64), (1, 8))),
        "stick_bias": draw_stick_bias(jax.random.fold_in(keys[17], 71), 0),
        "out_mixer": bell_draw(keys[15], (SSD_INNER, D), SSD_INNER ** -0.5, 0.125, ((0, 8), (1, 64))),
        "out_attend": bell_draw(keys[16], (SB_INNER, D), 0.6, 3.59375, ((0, 8), (1, 64))),
    }


EPS = 1e-06

def short_conv(rim_rows, current, weights):
    padded = jnp.concatenate([rim_rows, current], axis=0).astype(jnp.float32)
    length = current.shape[0]
    summed = weights[0] * padded[0:length]
    for tap_index in range(1, weights.shape[0]):
        summed = summed + weights[tap_index] * padded[tap_index:tap_index + length]
    return jax.nn.silu(summed).astype(jnp.bfloat16)

def block_terms(input_blocks, bkey_blocks, cquery_blocks, step_blocks, decay_blocks):
    cumulative = jnp.cumsum(decay_blocks, axis=1)
    cum_turned = jnp.transpose(cumulative, (0, 2, 3, 1))
    step_turned = jnp.transpose(step_blocks, (0, 2, 3, 1))
    length = input_blocks.shape[1]
    row_index = lax.broadcasted_iota(jnp.int32, (length, length), 0)
    col_index = lax.broadcasted_iota(jnp.int32, (length, length), 1)
    lower_mask = row_index >= col_index
    spread = cum_turned[..., :, None] - cum_turned[..., None, :]
    inner_prod = jnp.einsum('blgn,bsgn->bgls', cquery_blocks, bkey_blocks, preferred_element_type=jnp.float32)
    mixing = jnp.where(lower_mask, inner_prod[:, :, None] * jnp.exp(jnp.where(lower_mask, spread, 0.0)) * step_turned[..., None, :], 0.0)
    y_inner = jnp.einsum('bgrls,bsgrp->blgrp', mixing.astype(jnp.bfloat16), input_blocks, preferred_element_type=jnp.float32)
    to_end = jnp.exp(cumulative[:, -1:] - cumulative) * step_blocks
    weighted = (bkey_blocks.astype(jnp.float32)[:, :, :, None, :] * to_end[..., None]).astype(jnp.bfloat16)
    states = jnp.einsum('blgrp,blgrn->bgrpn', input_blocks, weighted, preferred_element_type=jnp.float32)
    return (cumulative, y_inner, states)

def chain_blocks(states, totals):

    def advance(held_state, block_item):
        block_state, block_log = block_item
        return (held_state * jnp.exp(block_log)[..., None, None] + block_state, held_state)
    return lax.scan(advance, jnp.zeros_like(states[0]), (states, totals))

def carried_output(cquery_blocks, entering, cumulative):
    return jnp.einsum('blgn,bgrpn->blgrp', cquery_blocks.astype(jnp.float32), entering, precision=lax.Precision.HIGHEST) * jnp.exp(cumulative)[..., None]

def gating_rescaled_output(y_total, gate_act, gain_slice, groups):
    length = y_total.shape[0]
    group_width = y_total.shape[2] * y_total.shape[3]
    gated_out = y_total.reshape(length, groups, group_width) * jax.nn.silu(gate_act.astype(jnp.float32)).reshape(length, groups, group_width)
    scaled = gated_out * lax.rsqrt(lax.optimization_barrier(jnp.mean(gated_out * gated_out, axis=-1, keepdims=True)) + EPS)
    return (scaled.reshape(length, groups * group_width) * gain_slice).astype(jnp.bfloat16)

def mixer_branch(normed, gate_act, input_act, input_projection_after_silu, cquery_act, w_step, conv_weight, decay_rate, offset_seq, ssd_gain):
    length = normed.shape[0]
    blocks = length // BLOCK
    head_ratio = SSD_HEADS // SSD_GROUPS
    step_size = jax.nn.softplus(jnp.dot(normed, w_step, preferred_element_type=jnp.float32))
    log_decay = offset_seq - decay_rate * step_size
    input_conv = short_conv(jnp.zeros((CONV - 1, SSD_INNER), jnp.bfloat16), input_act, conv_weight[:, 0:SSD_INNER])
    bkey_conv = short_conv(jnp.zeros((CONV - 1, GROUP_WIDTH), jnp.bfloat16), input_projection_after_silu, conv_weight[:, SSD_INNER:SSD_INNER + GROUP_WIDTH])
    cquery_conv = short_conv(jnp.zeros((CONV - 1, GROUP_WIDTH), jnp.bfloat16), cquery_act, conv_weight[:, SSD_INNER + GROUP_WIDTH:])
    input_blocks = input_conv.reshape(blocks, BLOCK, SSD_GROUPS, head_ratio, HEAD_DIM)
    bkey_blocks = bkey_conv.reshape(blocks, BLOCK, SSD_GROUPS, STATE)
    cquery_blocks = cquery_conv.reshape(blocks, BLOCK, SSD_GROUPS, STATE)
    step_blocks = step_size.reshape(blocks, BLOCK, SSD_GROUPS, head_ratio)
    decay_blocks = log_decay.reshape(blocks, BLOCK, SSD_GROUPS, head_ratio)
    cumulative, y_inner, states = block_terms(input_blocks, bkey_blocks, cquery_blocks, step_blocks, decay_blocks)
    final_state, entering = chain_blocks(states, cumulative[:, -1])
    y_total = y_inner + carried_output(cquery_blocks, entering, cumulative)
    return gating_rescaled_output(y_total.reshape(length, SSD_GROUPS, head_ratio, HEAD_DIM), gate_act, ssd_gain, SSD_GROUPS)

def stick_branch(queries, key_act, value_act, stick_bias):
    length = queries.shape[0]
    query_heads = queries.reshape(length, SB_HEADS, SB_DIM).transpose(1, 0, 2)
    key_heads = key_act.reshape(length, SB_HEADS, SB_DIM).transpose(1, 0, 2)
    value_heads = value_act.reshape(length, SB_HEADS, SB_DIM).transpose(1, 0, 2)
    key_pos = jnp.arange(length, dtype=jnp.int32)
    score_scale = SB_DIM ** (-0.5)

    def one_head(head_args):
        head_query, head_key, head_value, head_bias = head_args

        def one_block(block_start):
            block_query = lax.dynamic_slice_in_dim(head_query, block_start, TOK_DEV, 0)
            logits = jnp.dot(block_query, head_key.T, preferred_element_type=jnp.float32) * score_scale + head_bias
            query_pos = block_start + jnp.arange(TOK_DEV, dtype=jnp.int32)
            before = key_pos[None, :] < query_pos[:, None]
            log_keep = jax.nn.log_sigmoid(logits)
            log_pass = jnp.where(before, jax.nn.log_sigmoid(-logits), 0.0)
            tail_sum = lax.cumsum(log_pass, axis=1, reverse=True) - log_pass
            weights = jnp.where(before, jnp.exp(log_keep + tail_sum), 0.0).astype(jnp.bfloat16)
            return jnp.dot(weights, head_value, preferred_element_type=jnp.float32)
        starts = jnp.arange(length // TOK_DEV, dtype=jnp.int32) * TOK_DEV
        return lax.map(one_block, starts).reshape(length, SB_DIM)
    outcome = lax.map(one_head, (query_heads, key_heads, value_heads, stick_bias))
    return outcome.transpose(1, 0, 2).reshape(length, SB_INNER).astype(jnp.bfloat16)

def reference(inputs, norm_gain, w_gate, w_input, w_bkey, w_cquery, w_step, conv_weight, decay_rate, decay_offset, ssd_gain, w_query, w_key, w_value, stick_bias, out_mixer, out_attend):

    def one_sequence(seq_args):
        tokens, offset_seq = seq_args
        widened = tokens.astype(jnp.float32)
        normed = (widened * lax.rsqrt(lax.optimization_barrier(jnp.mean(widened * widened, axis=-1, keepdims=True)) + EPS) * norm_gain).astype(jnp.bfloat16)
        projected = [jnp.dot(normed, weight_tensor, preferred_element_type=jnp.float32).astype(jnp.bfloat16) for weight_tensor in (w_gate, w_input, w_bkey, w_cquery, w_query, w_key, w_value)]
        gate_act, input_act, input_projection_after_silu, cquery_act, queries, key_act, value_act = projected
        y_mixer = mixer_branch(normed, gate_act, input_act, input_projection_after_silu, cquery_act, w_step, conv_weight, decay_rate, offset_seq, ssd_gain)
        y_attend = stick_branch(queries, key_act, value_act, stick_bias)
        mixer_share = SSD_INNER // N_TP
        attend_share = SB_INNER // N_TP
        summed = jnp.zeros((tokens.shape[0], D), jnp.float32)
        for shard_index in range(N_TP):
            first_part = jnp.dot(y_mixer[:, shard_index * mixer_share:(shard_index + 1) * mixer_share], out_mixer[shard_index * mixer_share:(shard_index + 1) * mixer_share], preferred_element_type=jnp.float32)
            second_part = jnp.dot(y_attend[:, shard_index * attend_share:(shard_index + 1) * attend_share], out_attend[shard_index * attend_share:(shard_index + 1) * attend_share], preferred_element_type=jnp.float32)
            rounded = lax.optimization_barrier((first_part + second_part).astype(jnp.bfloat16))
            summed = summed + rounded.astype(jnp.float32)
        return summed.astype(jnp.bfloat16)
    return lax.map(one_sequence, (inputs, decay_offset))
```

```python
import jax
import jax.numpy as jnp
from jax import lax
from jax.experimental import pallas as pl
from jax.experimental.pallas import tpu as pltpu
from jax.sharding import PartitionSpec as P

BLOCK = 128
CONV = 4
EPS = 1e-06
HALO = 16
F32 = jnp.float32
BF16 = jnp.bfloat16
HIGH = lax.Precision.HIGHEST
NT = (((1,), (1,)), ((), ()))
TN = (((0,), (0,)), ((), ()))


def vmem(limit=48):
    return pltpu.CompilerParams(vmem_limit_bytes=limit * 1024 * 1024)


def iota(shape, dim):
    return lax.broadcasted_iota(jnp.int32, shape, dim)


def softplus(x):
    return jnp.maximum(x, 0.0) + jnp.log1p(jnp.exp(-jnp.abs(x)))


def silu(x):
    return x / (1.0 + jnp.exp(-x))


def norm_kernel(x_ref, gain_ref, ws_ref, xs_ref, step_ref):
    x = x_ref[0].astype(F32)
    scale = lax.rsqrt(jnp.mean(x * x, axis=-1, keepdims=True) + EPS)
    normed = (x * scale * gain_ref[...]).astype(BF16)
    step_ref[...] = softplus(lax.dot_general(ws_ref[...], normed, NT, preferred_element_type=F32))
    wide = normed.astype(F32)
    lane = iota((x.shape[0], 128), 1) // 32
    for f in range(4):
        for g in range(4):
            out = None
            for k in range(4):
                at = (4 * g + k) * 128
                piece = wide[:, at : at + 128]
                shift = ((k - f) * 32) % 128
                if shift:
                    piece = pltpu.roll(piece, shift, 1)
                out = piece if out is None else jnp.where(lane == k, piece, out)
            xs_ref[f, :, g * 128 : (g + 1) * 128] = out.astype(BF16)


def norm_call(inputs, gain, w_step_t):
    rows, width = inputs.shape[1:]
    return pl.pallas_call(
        norm_kernel,
        out_shape=(
            jax.ShapeDtypeStruct((4, rows, width // 4), BF16),
            jax.ShapeDtypeStruct((w_step_t.shape[0], rows), F32),
        ),
        compiler_params=vmem(),
        name="norm",
    )(inputs, gain.reshape(1, -1), w_step_t)


def pack_kernel(g, i, b, c, q, k, v, om, oa, first, second):
    at = 0
    for r in (k, v):
        first[:, at : at + r.shape[1]] = r[...]
        at += r.shape[1]
    at = 0
    for r in (g, i, b, c, q, om, oa):
        second[:, at : at + r.shape[1]] = r[...]
        at += r.shape[1]


def pack_call(g, i, b, c, q, k, v, om, oa):
    rows = g.shape[0]
    w1 = k.shape[1] + v.shape[1]
    w2 = sum(a.shape[1] for a in (g, i, b, c, q, om, oa))
    return pl.pallas_call(
        pack_kernel,
        out_shape=(
            jax.ShapeDtypeStruct((rows, w1), BF16),
            jax.ShapeDtypeStruct((rows, w2), BF16),
        ),
        compiler_params=vmem(),
        name="pack",
    )(g, i, b, c, q, k, v, om, oa)


def local_kernel(
    ids, rate, act_ref, step_ref, off_ref, ci_ref, cb_ref, cc_ref,
    yin_ref, gate_ref, cq_ref, cum_ref, send_ref, wide_ref,
):
    tensor = ids[1]
    total = act_ref[0, :, 0:768].astype(F32)
    for j in range(1, 4):
        total = total + act_ref[j, :, 0:768].astype(F32)
    act = total.astype(BF16).astype(F32)
    gate_ref[...] = act[HALO:, 0:256]
    wide_ref[...] = act[:, 256:768]
    taps = jnp.concatenate([ci_ref[...], cb_ref[...], cc_ref[...]], axis=1)
    summed = None
    for i in range(CONV):
        part = taps[i : i + 1] * wide_ref[HALO - CONV + 1 + i : HALO - CONV + 1 + i + BLOCK, :]
        summed = part if summed is None else summed + part
    conv = silu(summed).astype(BF16)
    xin, bkey, cquery = conv[:, 0:256], conv[:, 256:384], conv[:, 384:512]
    cq_ref[...] = cquery
    row = iota((BLOCK, BLOCK), 0)
    col = iota((BLOCK, BLOCK), 1)
    lower = row >= col
    step = jnp.concatenate(
        [step_ref[pl.ds(4 * tensor + h, 1), :] for h in range(4)], axis=0
    )
    rates = jnp.concatenate(
        [jnp.full((1, BLOCK), rate[4 * tensor + h], F32) for h in range(4)], axis=0
    )
    decay = off_ref[...] - rates * step
    pad = jnp.zeros((4, BLOCK), F32)
    decay8 = jnp.concatenate([decay, pad], axis=0)
    upper = (row <= col).astype(F32)
    cum = jnp.dot(decay8, upper, precision=HIGH, preferred_element_type=F32)
    last = jnp.sum(decay, axis=1, keepdims=True)
    to_end = jnp.exp(last - cum[0:4]) * step
    eye = (row == col).astype(F32)
    rows = jnp.concatenate([cum[0:4], to_end], axis=0)
    cols = lax.dot_general(eye, rows, NT, precision=HIGH, preferred_element_type=F32)
    cum_ref[...] = cols
    inner = lax.dot_general(cquery, bkey, NT, preferred_element_type=F32)
    wide_key = bkey.astype(F32)
    ys = []
    for h in range(4):
        spread = cols[:, h : h + 1] - cum[h : h + 1]
        decayed = jnp.exp(jnp.where(lower, spread, 0.0))
        mix = jnp.where(lower, inner * decayed * step[h : h + 1], 0.0).astype(BF16)
        xh = xin[:, h * 64 : (h + 1) * 64]
        ys.append(jnp.dot(mix, xh, preferred_element_type=F32))
        wk = (wide_key * cols[:, 4 + h : 5 + h]).astype(BF16)
        state = lax.dot_general(xh, wk, TN, preferred_element_type=F32).astype(BF16)
        log = jnp.broadcast_to(last[h : h + 1], (8, BLOCK))
        high = log.astype(BF16).astype(F32)
        logs = jnp.concatenate([high, log - high], axis=0).astype(BF16)
        for j in range(4):
            send_ref[4 * h + j, 0:16, :] = state[16 * j : 16 * (j + 1), :]
            send_ref[4 * h + j, 16:32, :] = logs
    yin_ref[...] = jnp.concatenate(ys, axis=1)


def local_call(ids, rate, act, step, offset, conv_weight):
    full = lambda *shape: pl.BlockSpec(shape, lambda i, ids, rate: (0,) * len(shape))
    return pl.pallas_call(
        local_kernel,
        grid_spec=pltpu.PrefetchScalarGridSpec(
            num_scalar_prefetch=2,
            grid=(1,),
            in_specs=[
                full(*act.shape),
                full(*step.shape),
                full(*offset.shape),
                pl.BlockSpec((CONV, 256), lambda i, ids, rate: (0, ids[1])),
                pl.BlockSpec((CONV, 128), lambda i, ids, rate: (0, 16 + ids[1])),
                pl.BlockSpec((CONV, 128), lambda i, ids, rate: (0, 24 + ids[1])),
            ],
            out_specs=[
                full(BLOCK, 256), full(BLOCK, 256), full(BLOCK, 128), full(BLOCK, 8),
                full(16, 32, 128),
            ],
            scratch_shapes=[pltpu.VMEM((BLOCK + HALO, 512), F32)],
        ),
        out_shape=(
            jax.ShapeDtypeStruct((BLOCK, 256), F32),
            jax.ShapeDtypeStruct((BLOCK, 256), F32),
            jax.ShapeDtypeStruct((BLOCK, 128), BF16),
            jax.ShapeDtypeStruct((BLOCK, 8), F32),
            jax.ShapeDtypeStruct((16, 32, 128), BF16),
        ),
        compiler_params=vmem(),
        name="ssd_local",
    )(ids, rate, act, step, offset, conv_weight, conv_weight, conv_weight)


def scan_kernel(got_ref, out_ref):
    held = jnp.zeros((16, 128), F32)
    for k in range(16):
        out_ref[k] = held.astype(BF16)
        logs = got_ref[k, 16:32, :].astype(F32)
        decay = jnp.exp(logs[0:8] + logs[8:16])
        held = held * jnp.concatenate([decay, decay], axis=0) + got_ref[k, 0:16, :].astype(F32)


def scan_call(got):
    return pl.pallas_call(
        scan_kernel,
        out_shape=jax.ShapeDtypeStruct((16, 16, 128), BF16),
        name="state_scan",
    )(got)


def carry_kernel(ids, enter_ref, yin_ref, gate_ref, cq_ref, cum_ref, gain_ref, out_ref):
    cquery = cq_ref[...]
    ys = []
    for h in range(4):
        enter = enter_ref[64 * h : 64 * (h + 1), :]
        moved = lax.dot_general(cquery, enter, NT, preferred_element_type=F32)
        ys.append(moved * jnp.exp(cum_ref[:, h : h + 1]))
    total = yin_ref[...] + jnp.concatenate(ys, axis=1)
    gated = total * silu(gate_ref[...])
    scale = lax.rsqrt(jnp.mean(gated * gated, axis=-1, keepdims=True) + EPS)
    out_ref[...] = (gated * scale * gain_ref[...]).astype(BF16)


def carry_call(ids, enter, yin, gate, cq, cum, gain):
    full = lambda *shape: pl.BlockSpec(shape, lambda i, ids: (0,) * len(shape))
    return pl.pallas_call(
        carry_kernel,
        grid_spec=pltpu.PrefetchScalarGridSpec(
            num_scalar_prefetch=1,
            grid=(1,),
            in_specs=[
                full(256, 128), full(BLOCK, 256), full(BLOCK, 256), full(BLOCK, 128),
                full(BLOCK, 8), pl.BlockSpec((1, 256), lambda i, ids: (0, ids[1])),
            ],
            out_specs=full(BLOCK, 256),
        ),
        out_shape=jax.ShapeDtypeStruct((BLOCK, 256), BF16),
        compiler_params=vmem(),
        name="ssd_carry",
    )(ids, enter, yin, gate, cq, cum, gain.reshape(1, -1))


KEYS = 256


def attend_kernel(ids, bias, qp_ref, kv_ref, mix_ref, w0, w1, w2, w3, out_ref, w_ref, acc_ref, late_ref, sems):
    block = ids[0]
    mine = ids[2]
    copies = [
        pltpu.make_async_copy(w, w_ref.at[(mine + 4 - r) % 4], sems.at[r])
        for r, w in enumerate((w0, w1, w2, w3))
    ]
    for copy in copies:
        copy.start()
    queries = qp_ref[0, HALO:, :].astype(F32)
    for j in range(1, 4):
        queries = queries + qp_ref[j, HALO:, :].astype(F32)
    queries = queries.astype(BF16)
    acc_ref[...] = jnp.zeros_like(acc_ref)
    late_ref[...] = jnp.zeros_like(late_ref)
    after = (iota((KEYS, KEYS), 0) > iota((KEYS, KEYS), 1)).astype(BF16)
    ones = jnp.ones((KEYS, 128), BF16)
    spot = block * BLOCK + iota((BLOCK, KEYS), 0)
    for at in range(kv_ref.shape[0] - KEYS, -1, -KEYS):

        @pl.when(at <= block * BLOCK)
        def _(at=at):
            before = (at + iota((BLOCK, KEYS), 1)) < spot
            for h in range(2):
                key = kv_ref[at : at + KEYS, h * 128 : (h + 1) * 128]
                value = kv_ref[at : at + KEYS, 256 + h * 128 : 256 + (h + 1) * 128]
                query = queries[:, h * 128 : (h + 1) * 128]
                logits = lax.dot_general(query, key, NT, preferred_element_type=F32)
                logits = logits * (128 ** -0.5) + bias[2 * ids[1] + h]
                soft = jnp.maximum(logits, 0.0) + jnp.log1p(jnp.exp(-jnp.abs(logits)))
                passed = jnp.where(before, -soft, 0.0)
                high = passed.astype(BF16)
                low = (passed - high.astype(F32)).astype(BF16)
                tail = jnp.dot(high, after, preferred_element_type=F32) + jnp.dot(
                    low, after, preferred_element_type=F32
                )
                whole = jnp.dot(high, ones, preferred_element_type=F32) + jnp.dot(
                    low, ones, preferred_element_type=F32
                )
                late = late_ref[h]
                late2 = jnp.concatenate([late] * (KEYS // 128), axis=1)
                weight = jnp.where(before, jnp.exp(logits - soft + tail + late2), 0.0)
                acc_ref[h] += jnp.dot(weight.astype(BF16), value, preferred_element_type=F32)
                late_ref[h] = late + whole

    both = jnp.concatenate(
        [mix_ref[...], acc_ref[0].astype(BF16), acc_ref[1].astype(BF16)], axis=1
    )
    for copy in copies:
        copy.wait()
    for s in range(16):
        piece = jnp.concatenate([w_ref[f, 32 * s : 32 * (s + 1), :] for f in range(4)], axis=0)
        out_ref[:, 128 * s : 128 * (s + 1)] = lax.dot_general(
            both, piece, NT, preferred_element_type=F32
        ).astype(BF16)


def attend_call(ids, bias, act, kv, mix, w):
    full = lambda *shape: pl.BlockSpec(shape, lambda i, ids, bias: (0,) * len(shape))
    hbm = pl.BlockSpec(memory_space=pl.ANY)
    return pl.pallas_call(
        attend_kernel,
        grid_spec=pltpu.PrefetchScalarGridSpec(
            num_scalar_prefetch=2,
            grid=(1,),
            in_specs=[
                pl.BlockSpec((4, BLOCK + HALO, 256), lambda i, ids, bias: (0, 0, 3)),
                full(*kv.shape), full(BLOCK, 256), hbm, hbm, hbm, hbm,
            ],
            out_specs=full(BLOCK, 2048),
            scratch_shapes=[
                pltpu.VMEM((4, 512, 512), BF16),
                pltpu.VMEM((2, BLOCK, 128), F32),
                pltpu.VMEM((2, BLOCK, 128), F32),
                pltpu.SemaphoreType.DMA((4,)),
            ],
        ),
        out_shape=jax.ShapeDtypeStruct((BLOCK, 2048), BF16),
        compiler_params=vmem(),
        name="attend",
    )(ids, bias, act, kv, mix, *w)


def rotated(shard, axis, by):
    length = lax.axis_size(axis)
    return lax.ppermute(shard, axis, [(i, (i + by) % length) for i in range(length)])


def body(
    inputs, norm_gain, w_gate, w_input, w_bkey, w_cquery, w_step, conv_weight, decay_rate,
    decay_offset, ssd_gain, w_query, w_key, w_value, stick_bias, out_mixer, out_attend,
):
    tensor = lax.axis_index("tp")
    seq = lax.axis_index("sp")
    part = lax.axis_index("fs")
    ids = jnp.stack([seq, tensor, part]).astype(jnp.int32)
    first, second = pack_call(
        w_gate, w_input, w_bkey, w_cquery, w_query, w_key, w_value, out_mixer.T, out_attend.T
    )
    rest = lax.all_gather(second, "sp", axis=0, tiled=True)
    split, step = norm_call(inputs, norm_gain, w_step.T)
    length = lax.axis_size("sp")
    halo = lax.ppermute(
        split[:, BLOCK - HALO :], "sp", [(i, i + 1) for i in range(length - 1)]
    )
    tokens = lax.all_to_all(jnp.concatenate([halo, split], axis=1), "fs", 0, 0, tiled=True)
    flat = tokens.reshape(-1, 512)
    w_kv = lax.all_gather(first, "sp", axis=0, tiled=True)
    kv_part = jnp.dot(flat, w_kv, preferred_element_type=F32).astype(BF16)
    kv_part = lax.all_to_all(kv_part.reshape(4, -1, 512), "fs", 0, 0, tiled=True)
    kv_own = jnp.sum(kv_part[:, HALO:].astype(F32), axis=0).astype(BF16)
    kv = lax.all_gather(kv_own, "sp", axis=0, tiled=True)
    w_out = rest[:, 1024:]
    outs = [w_out] + [rotated(w_out, "fs", by) for by in (1, 2, 3)]
    act = jnp.dot(flat, rest[:, :1024], preferred_element_type=F32).astype(BF16)
    act = lax.all_to_all(act.reshape(4, -1, 1024), "fs", 0, 0, tiled=True)
    yin, gate, cq, cum, send = local_call(
        ids, decay_rate, act, step, decay_offset[0].T, conv_weight
    )
    got = lax.all_to_all(send, "sp", 0, 0, tiled=True)
    enter = lax.all_to_all(scan_call(got), "sp", 0, 0, tiled=True).reshape(256, 128)
    mix = carry_call(ids, enter, yin, gate, cq, cum, ssd_gain)
    partial = attend_call(ids, stick_bias, act, kv, mix, outs)
    parts = lax.all_to_all(partial.reshape(8, 16, 2048), "tp", 0, 0, tiled=True)
    return jnp.sum(parts.astype(F32), axis=0).astype(BF16)[None]


def solution(mesh):
    shard = P(("sp", "fs"), "tp")
    return jax.shard_map(
        body,
        mesh=mesh,
        in_specs=(
            P("fs", "sp", None), P(), shard, shard, shard, shard, P(), P(), P(),
            P("fs", "sp", "tp"), P(), shard, shard, shard, P(),
            P("tp", ("sp", "fs")), P("tp", ("sp", "fs")),
        ),
        out_specs=P("fs", ("sp", "tp"), None),
        check_vma=False,
    )
```

```python
import jax
import jax.numpy as jnp
from jax import lax
from jax.experimental import pallas as pl
from jax.experimental.pallas import tpu as pltpu
from jax.sharding import PartitionSpec as P

BLOCK = 128
CONV = 4
EPS = 1e-06
HALO = 16
F32 = jnp.float32
BF16 = jnp.bfloat16
HIGH = lax.Precision.HIGHEST
NT = (((1,), (1,)), ((), ()))
TN = (((0,), (0,)), ((), ()))


def vmem(limit=48):
    return pltpu.CompilerParams(vmem_limit_bytes=limit * 1024 * 1024)


def iota(shape, dim):
    return lax.broadcasted_iota(jnp.int32, shape, dim)


def softplus(x):
    return jnp.maximum(x, 0.0) + jnp.log1p(jnp.exp(-jnp.abs(x)))


def silu(x):
    return x / (1.0 + jnp.exp(-x))


def pull(pairs, sems):
    copies = [pltpu.make_async_copy(src, dst, sems.at[i]) for i, (src, dst) in enumerate(pairs)]
    for copy in copies:
        copy.start()
    return copies


def norm_kernel(x_hbm, halo_hbm, gain_hbm, ws_hbm, xs_ref, step_ref, x_ref, gain_ref, ws_ref, sems):
    copies = pull(
        (
            (x_hbm.at[0], x_ref.at[pl.ds(HALO, BLOCK)]),
            (halo_hbm, x_ref.at[pl.ds(0, HALO)]),
            (gain_hbm, gain_ref),
            (ws_hbm, ws_ref),
        ),
        sems,
    )
    for copy in copies:
        copy.wait()
    x = x_ref[...].astype(F32)
    scale = lax.rsqrt(jnp.mean(x * x, axis=-1, keepdims=True) + EPS)
    normed = (x * scale * gain_ref[...]).astype(BF16)
    step_ref[...] = softplus(
        lax.dot_general(ws_ref[...], normed[HALO:], NT, preferred_element_type=F32)
    )
    wide = normed.astype(F32)
    lane = iota((x.shape[0], 128), 1) // 32
    for f in range(4):
        for g in range(4):
            out = None
            for k in range(4):
                at = (4 * g + k) * 128
                piece = wide[:, at : at + 128]
                shift = ((k - f) * 32) % 128
                if shift:
                    piece = pltpu.roll(piece, shift, 1)
                out = piece if out is None else jnp.where(lane == k, piece, out)
            xs_ref[f, :, g * 128 : (g + 1) * 128] = out.astype(BF16)


def norm_call(inputs, halo, gain, w_step_t):
    rows, width = inputs.shape[1:]
    heads = w_step_t.shape[0]
    hbm = pl.BlockSpec(memory_space=pltpu.HBM)
    return pl.pallas_call(
        norm_kernel,
        in_specs=[hbm] * 4,
        out_shape=(
            jax.ShapeDtypeStruct((4, rows + HALO, width // 4), BF16),
            jax.ShapeDtypeStruct((heads, rows), F32),
        ),
        scratch_shapes=[
            pltpu.VMEM((rows + HALO, width), BF16),
            pltpu.VMEM((1, width), F32),
            pltpu.VMEM((heads, width), BF16),
            pltpu.SemaphoreType.DMA((4,)),
        ],
        compiler_params=vmem(),
        name="norm",
    )(inputs, halo, gain.reshape(1, -1), w_step_t)


def pack_kernel(*refs):
    sources, outs, sems = refs[:9], refs[9:12], refs[12]
    pairs = []
    at, which = 0, 0
    for n, src in enumerate(sources):
        if n in (4, 7):
            at, which = 0, which + 1
        width = src.shape[1]
        pairs.append((src, outs[which].at[:, pl.ds(at, width)]))
        at += width
    for copy in pull(pairs, sems):
        copy.wait()


def pack_call(*arrays):
    rows = arrays[0].shape[0]
    widths = [sum(a.shape[1] for a in group) for group in (arrays[:4], arrays[4:7], arrays[7:])]
    hbm = pl.BlockSpec(memory_space=pltpu.HBM)
    return pl.pallas_call(
        pack_kernel,
        in_specs=[hbm] * len(arrays),
        out_specs=[hbm] * 3,
        out_shape=[jax.ShapeDtypeStruct((rows, w), BF16) for w in widths],
        scratch_shapes=[pltpu.SemaphoreType.DMA((len(arrays),))],
        name="pack",
    )(*arrays)


def added(ref, at, width):
    total = ref[0, :, at : at + width].astype(F32)
    for j in range(1, 4):
        total = total + ref[j, :, at : at + width].astype(F32)
    return total.astype(BF16)


def convolved(wide_ref, taps):
    summed = None
    for i in range(CONV):
        at = HALO - CONV + 1 + i
        part = taps[i : i + 1] * wide_ref[at : at + BLOCK, :]
        summed = part if summed is None else summed + part
    return silu(summed).astype(BF16)


def local_kernel(
    ids, rate, act_ref, step_ref, off_ref, ci_ref, cb_ref,
    send_ref, xin_ref, bkey_ref, rows_ref, cols_ref, wide_ref,
):
    tensor = ids[1]
    send_ref[0:BLOCK, :] = added(act_ref, 0, 512)[HALO:]
    wide_ref[...] = added(act_ref, 512, 384).astype(F32)
    conv = convolved(wide_ref, jnp.concatenate([ci_ref[...], cb_ref[...]], axis=1))
    xin, bkey = conv[:, 0:256], conv[:, 256:384]
    xin_ref[...] = xin
    bkey_ref[...] = bkey
    row = iota((BLOCK, BLOCK), 0)
    col = iota((BLOCK, BLOCK), 1)
    step = jnp.concatenate([step_ref[pl.ds(4 * tensor + h, 1), :] for h in range(4)], axis=0)
    rates = jnp.concatenate(
        [jnp.full((1, BLOCK), rate[4 * tensor + h], F32) for h in range(4)], axis=0
    )
    decay = off_ref[...] - rates * step
    decay8 = jnp.concatenate([decay, jnp.zeros((4, BLOCK), F32)], axis=0)
    upper = (row <= col).astype(F32)
    cum = jnp.dot(decay8, upper, precision=HIGH, preferred_element_type=F32)
    last = jnp.sum(decay, axis=1, keepdims=True)
    to_end = jnp.exp(last - cum[0:4]) * step
    eye = (row == col).astype(F32)
    cols = lax.dot_general(
        eye, jnp.concatenate([cum[0:4], to_end], axis=0), NT, precision=HIGH,
        preferred_element_type=F32,
    )
    rows_ref[...] = jnp.concatenate([cum[0:4], step], axis=0)
    cols_ref[...] = cols
    wide_key = bkey.astype(F32)
    for h in range(4):
        wk = (wide_key * cols[:, 4 + h : 5 + h]).astype(BF16)
        state = lax.dot_general(
            xin[:, h * 64 : (h + 1) * 64], wk, TN, preferred_element_type=F32
        )
        log = jnp.broadcast_to(last[h : h + 1], (8, BLOCK))
        high = log.astype(BF16).astype(F32)
        logs = jnp.concatenate([high, log - high], axis=0).astype(BF16)
        send_ref[BLOCK : BLOCK + 64, h * 128 : (h + 1) * 128] = state.astype(BF16)
        send_ref[BLOCK + 64 : BLOCK + 80, h * 128 : (h + 1) * 128] = logs


def local_call(ids, rate, act, step, offset, conv_weight):
    full = lambda *shape: pl.BlockSpec(shape, lambda i, ids, rate: (0,) * len(shape))
    return pl.pallas_call(
        local_kernel,
        grid_spec=pltpu.PrefetchScalarGridSpec(
            num_scalar_prefetch=2,
            grid=(1,),
            in_specs=[
                full(*act.shape),
                full(*step.shape),
                full(*offset.shape),
                pl.BlockSpec((CONV, 256), lambda i, ids, rate: (0, ids[1])),
                pl.BlockSpec((CONV, 128), lambda i, ids, rate: (0, 16 + ids[1])),
            ],
            out_specs=[
                full(SENT, 512), full(BLOCK, 256), full(BLOCK, 128), full(8, BLOCK),
                full(BLOCK, 8),
            ],
            scratch_shapes=[pltpu.VMEM((BLOCK + HALO, 384), F32)],
        ),
        out_shape=(
            jax.ShapeDtypeStruct((SENT, 512), BF16),
            jax.ShapeDtypeStruct((BLOCK, 256), BF16),
            jax.ShapeDtypeStruct((BLOCK, 128), BF16),
            jax.ShapeDtypeStruct((8, BLOCK), F32),
            jax.ShapeDtypeStruct((BLOCK, 8), F32),
        ),
        compiler_params=vmem(),
        name="ssd_local",
    )(ids, rate, act, step, offset, conv_weight, conv_weight)


def inner_kernel(
    ids, act_ref, cc_ref, xin_ref, bkey_ref, rows_ref, cols_ref,
    yin_ref, gate_ref, cq_ref, q_ref, wide_ref,
):
    gate_ref[...] = silu(added(act_ref, 0, 256)[HALO:].astype(F32))
    q_ref[...] = added(act_ref, 384, 256)[HALO:]
    wide_ref[...] = added(act_ref, 256, 128).astype(F32)
    cquery = convolved(wide_ref, cc_ref[...])
    cq_ref[...] = cquery
    lower = iota((BLOCK, BLOCK), 0) >= iota((BLOCK, BLOCK), 1)
    inner = lax.dot_general(cquery, bkey_ref[...], NT, preferred_element_type=F32)
    for h in range(4):
        spread = cols_ref[:, h : h + 1] - rows_ref[h : h + 1, :]
        decayed = jnp.exp(jnp.where(lower, spread, 0.0))
        mix = jnp.where(lower, inner * decayed * rows_ref[4 + h : 5 + h, :], 0.0).astype(BF16)
        yin_ref[:, h * 64 : (h + 1) * 64] = jnp.dot(
            mix, xin_ref[:, h * 64 : (h + 1) * 64], preferred_element_type=F32
        )


def inner_call(ids, act, conv_weight, xin, bkey, rows, cols):
    full = lambda *shape: pl.BlockSpec(shape, lambda i, ids: (0,) * len(shape))
    return pl.pallas_call(
        inner_kernel,
        grid_spec=pltpu.PrefetchScalarGridSpec(
            num_scalar_prefetch=1,
            grid=(1,),
            in_specs=[
                full(*act.shape),
                pl.BlockSpec((CONV, 128), lambda i, ids: (0, 24 + ids[1])),
                full(BLOCK, 256), full(BLOCK, 128), full(8, BLOCK), full(BLOCK, 8),
            ],
            out_specs=[full(BLOCK, 256), full(BLOCK, 256), full(BLOCK, 128), full(BLOCK, 256)],
            scratch_shapes=[pltpu.VMEM((BLOCK + HALO, 128), F32)],
        ),
        out_shape=(
            jax.ShapeDtypeStruct((BLOCK, 256), F32),
            jax.ShapeDtypeStruct((BLOCK, 256), F32),
            jax.ShapeDtypeStruct((BLOCK, 128), BF16),
            jax.ShapeDtypeStruct((BLOCK, 256), BF16),
        ),
        compiler_params=vmem(),
        name="ssd_inner",
    )(ids, act, conv_weight, xin, bkey, rows, cols)


SUB = 256
KEYS = 512
SENT = BLOCK + 80


def attend_kernel(
    ids, bias, q_ref, yin_ref, gate_ref, cq_ref, cols_ref, gain_ref, all_hbm, w0, w1, w2, w3,
    out_ref, kv_ref, st_ref, w_ref, acc_ref, late_ref, hold_ref, sems, wsems,
):
    block, tensor, mine = ids[0], ids[1], ids[2]
    per = KEYS // BLOCK

    def move(k):
        return pltpu.make_async_copy(
            all_hbm.at[k, pl.ds(0, BLOCK)], kv_ref.at[pl.ds(k * BLOCK, BLOCK)], sems.at[0, k]
        )

    def state_move(k):
        return pltpu.make_async_copy(
            all_hbm.at[k, pl.ds(BLOCK, SENT - BLOCK)], st_ref.at[k], sems.at[1, k]
        )

    count = all_hbm.shape[0]
    for chunk in range(count // per - 1, -1, -1):

        @pl.when(chunk * per <= block)
        def _(chunk=chunk):
            for k in range(chunk * per, (chunk + 1) * per):
                move(k).start()

    for k in range(count - 1):
        state_move(k).start()
    weights = [
        pltpu.make_async_copy(w, w_ref.at[(mine + 4 - r) % 4], wsems.at[r])
        for r, w in enumerate((w0, w1, w2, w3))
    ]
    for copy in weights:
        copy.start()
    acc_ref[...] = jnp.zeros_like(acc_ref)
    late_ref[...] = jnp.zeros_like(late_ref)
    hold_ref[...] = jnp.zeros_like(hold_ref)
    after = (iota((SUB, SUB), 0) > iota((SUB, SUB), 1)).astype(BF16)
    ones = jnp.ones((SUB, 128), BF16)
    for chunk in range(count // per - 1, -1, -1):

        @pl.when(chunk * per <= block)
        def _(chunk=chunk):
            for k in range(chunk * per, (chunk + 1) * per):
                move(k).wait()
            for h in range(2):
                late = late_ref[h]
                gained = acc_ref[h]
                query = q_ref[:, h * 128 : (h + 1) * 128]
                for sub in range(KEYS // SUB - 1, -1, -1):
                    at = chunk * KEYS + sub * SUB
                    before = at + iota((BLOCK, SUB), 1) < block * BLOCK + iota((BLOCK, SUB), 0)
                    key = kv_ref[at : at + SUB, h * 128 : (h + 1) * 128]
                    value = kv_ref[at : at + SUB, 256 + h * 128 : 256 + (h + 1) * 128]
                    logits = lax.dot_general(query, key, NT, preferred_element_type=F32)
                    logits = logits * (128 ** -0.5) + bias[2 * tensor + h]
                    soft = jnp.maximum(logits, 0.0) + jnp.log(1.0 + jnp.exp(-jnp.abs(logits)))
                    passed = jnp.where(before, -soft, 0.0)
                    high = passed.astype(BF16)
                    low = (passed - high.astype(F32)).astype(BF16)
                    tail = jnp.dot(high, after, preferred_element_type=F32) + jnp.dot(
                        low, after, preferred_element_type=F32
                    )
                    whole = jnp.dot(high, ones, preferred_element_type=F32) + jnp.dot(
                        low, ones, preferred_element_type=F32
                    )
                    later = jnp.concatenate([late] * (SUB // 128), axis=1)
                    weight = jnp.where(before, jnp.exp(logits - soft + (tail + later)), 0.0)
                    gained = gained + jnp.dot(
                        weight.astype(BF16), value, preferred_element_type=F32
                    )
                    late = late + whole
                late_ref[h] = late
                acc_ref[h] = gained

    for k in range(count - 1):
        state_move(k).wait()

        @pl.when(k < block)
        def _(k=k):
            logs = st_ref[k, 64:80, :].astype(F32)
            decay = jnp.exp(logs[0:8] + logs[8:16])
            hold_ref[...] = hold_ref[...] * jnp.concatenate([decay] * 8, axis=0) + st_ref[
                k, 0:64, :
            ].astype(F32)

    cquery = cq_ref[...]
    ys = []
    for h in range(4):
        enter = hold_ref[:, h * 128 : (h + 1) * 128].astype(BF16)
        moved = lax.dot_general(cquery, enter, NT, preferred_element_type=F32)
        ys.append(moved * jnp.exp(cols_ref[:, h : h + 1]))
    gated = (yin_ref[...] + jnp.concatenate(ys, axis=1)) * gate_ref[...]
    scale = lax.rsqrt(jnp.mean(gated * gated, axis=-1, keepdims=True) + EPS)
    mixed = (gated * scale * gain_ref[...]).astype(BF16)
    both = jnp.concatenate([mixed, acc_ref[0].astype(BF16), acc_ref[1].astype(BF16)], axis=1)
    for copy in weights:
        copy.wait()
    for s in range(16):
        piece = jnp.concatenate([w_ref[f, 32 * s : 32 * (s + 1), :] for f in range(4)], axis=0)
        out_ref[:, 128 * s : 128 * (s + 1)] = lax.dot_general(
            both, piece, NT, preferred_element_type=F32
        ).astype(BF16)


def attend_call(ids, bias, q, yin, gate, cq, cols, gain, gathered, w):
    full = lambda *shape: pl.BlockSpec(shape, lambda i, ids, bias: (0,) * len(shape))
    hbm = pl.BlockSpec(memory_space=pltpu.HBM)
    count = gathered.shape[0]
    return pl.pallas_call(
        attend_kernel,
        grid_spec=pltpu.PrefetchScalarGridSpec(
            num_scalar_prefetch=2,
            grid=(1,),
            in_specs=[
                full(BLOCK, 256), full(BLOCK, 256), full(BLOCK, 256), full(BLOCK, 128),
                full(BLOCK, 8), pl.BlockSpec((1, 256), lambda i, ids, bias: (0, ids[1])),
                hbm, hbm, hbm, hbm, hbm,
            ],
            out_specs=full(BLOCK, 2048),
            scratch_shapes=[
                pltpu.VMEM((count * BLOCK, 512), BF16),
                pltpu.VMEM((count, SENT - BLOCK, 512), BF16),
                pltpu.VMEM((4, 512, 512), BF16),
                pltpu.VMEM((2, BLOCK, 128), F32),
                pltpu.VMEM((2, BLOCK, 128), F32),
                pltpu.VMEM((64, 512), F32),
                pltpu.SemaphoreType.DMA((2, count)),
                pltpu.SemaphoreType.DMA((4,)),
            ],
        ),
        out_shape=jax.ShapeDtypeStruct((BLOCK, 2048), BF16),
        compiler_params=vmem(),
        name="attend",
    )(ids, bias, q, yin, gate, cq, cols, gain.reshape(1, -1), gathered, *w)


def rotated(shard, axis, by):
    length = lax.axis_size(axis)
    return lax.ppermute(shard, axis, [(i, (i + by) % length) for i in range(length)])


def body(
    inputs, norm_gain, w_gate, w_input, w_bkey, w_cquery, w_step, conv_weight, decay_rate,
    decay_offset, ssd_gain, w_query, w_key, w_value, stick_bias, out_mixer, out_attend,
):
    tensor = lax.axis_index("tp")
    seq = lax.axis_index("sp")
    part = lax.axis_index("fs")
    length = lax.axis_size("sp")
    ids = jnp.stack([seq, tensor, part]).astype(jnp.int32)
    halo = lax.ppermute(
        inputs[0, BLOCK - HALO :], "sp", [(i, i + 1) for i in range(length - 1)]
    )
    first, second, third = pack_call(
        w_key, w_value, w_input, w_bkey, w_gate, w_cquery, w_query, out_mixer.T, out_attend.T
    )
    split, step = norm_call(inputs, halo, norm_gain, w_step.T)
    tokens = lax.all_to_all(split, "fs", 0, 0, tiled=True).reshape(-1, 512)
    rows = BLOCK + HALO

    def projected(weights):
        whole = lax.all_gather(weights, "sp", axis=0, tiled=True)
        act = jnp.dot(tokens, whole, preferred_element_type=F32).astype(BF16)
        return lax.all_to_all(act.reshape(4, rows, -1), "fs", 0, 0, tiled=True)

    send, xin, bkey, srows, scols = local_call(
        ids, decay_rate, projected(first), step, decay_offset[0].T, conv_weight
    )
    gathered = lax.all_gather(send, "sp", axis=0)
    out_w = lax.all_to_all(
        jnp.broadcast_to(third[None], (length, *third.shape)), "sp", 0, 0, tiled=True
    ).reshape(-1, 512)
    outs = [out_w] + [rotated(out_w, "fs", by) for by in (1, 2, 3)]
    yin, gate, cq, q = inner_call(ids, projected(second), conv_weight, xin, bkey, srows, scols)
    partial = attend_call(ids, stick_bias, q, yin, gate, cq, scols, ssd_gain, gathered, outs)
    parts = lax.all_to_all(partial.reshape(8, 16, 2048), "tp", 0, 0, tiled=True)
    return jnp.sum(parts.astype(F32), axis=0).astype(BF16)[None]


def solution(mesh):
    shard = P(("sp", "fs"), "tp")
    return jax.shard_map(
        body,
        mesh=mesh,
        in_specs=(
            P("fs", "sp", None), P(), shard, shard, shard, shard, P(), P(), P(),
            P("fs", "sp", "tp"), P(), shard, shard, shard, P(),
            P("tp", ("sp", "fs")), P("tp", ("sp", "fs")),
        ),
        out_specs=P("fs", ("sp", "tp"), None),
        check_vma=False,
    )
```

```python
import jax
import jax.numpy as jnp
from jax import lax
from jax.experimental import pallas as pl
from jax.experimental.pallas import tpu as pltpu
from jax.sharding import PartitionSpec as P

BLOCK = 128
CONV = 4
EPS = 1e-06
HALO = 16
ROWS = BLOCK + HALO
F32 = jnp.float32
BF16 = jnp.bfloat16
HIGH = lax.Precision.HIGHEST
NT = (((1,), (1,)), ((), ()))
TN = (((0,), (0,)), ((), ()))


def vmem(limit=48):
    return pltpu.CompilerParams(vmem_limit_bytes=limit * 1024 * 1024)


def iota(shape, dim):
    return lax.broadcasted_iota(jnp.int32, shape, dim)


def softplus(x):
    return jnp.maximum(x, 0.0) + jnp.log1p(jnp.exp(-jnp.abs(x)))


def silu(x):
    return x / (1.0 + jnp.exp(-x))


def pull(pairs, sems):
    copies = [pltpu.make_async_copy(src, dst, sems.at[i]) for i, (src, dst) in enumerate(pairs)]
    for copy in copies:
        copy.start()
    return copies


def shuffled(normed, f, g):
    lane = iota((normed.shape[0], 128), 1) // 32
    out = None
    for k in range(4):
        at = (4 * g + k) * 128
        piece = normed[:, at : at + 128]
        shift = ((k - f) * 32) % 128
        if shift:
            piece = pltpu.roll(piece, shift, 1)
        out = piece if out is None else jnp.where(lane == k, piece, out)
    return out.astype(BF16)


def normalised(x, gain):
    wide = x.astype(F32)
    scale = lax.rsqrt(jnp.mean(wide * wide, axis=-1, keepdims=True) + EPS)
    return (wide * scale * gain).astype(BF16)


def prep_kernel(*refs):
    x_hbm, gain_hbm, ws_hbm = refs[:3]
    sources = refs[3:12]
    xs_ref, step_ref, first_ref, second_ref = refs[12:16]
    x_ref, gain_ref, ws_ref, third_ref, sems, wsems = refs[16:]
    early = pull(((x_hbm.at[0], x_ref), (gain_hbm, gain_ref), (ws_hbm, ws_ref)), sems)
    pairs = []
    outs = (first_ref, second_ref, third_ref)
    at, which = 0, 0
    for n, src in enumerate(sources):
        if n in (4, 7):
            at, which = 0, which + 1
        pairs.append((src, outs[which].at[:, pl.ds(at, src.shape[1])]))
        at += src.shape[1]
    later = pull(pairs, wsems)
    for copy in early:
        copy.wait()
    normed = normalised(x_ref[...], gain_ref[...])
    step_ref[...] = softplus(
        lax.dot_general(ws_ref[...], normed, NT, preferred_element_type=F32)
    )
    wide = normed.astype(F32)
    for f in range(4):
        for g in range(4):
            xs_ref[f, HALO:ROWS, g * 128 : (g + 1) * 128] = shuffled(wide, f, g)
    for copy in later:
        copy.wait()
    for f in range(4):
        xs_ref[f, ROWS:, :] = third_ref[...]


def prep_call(inputs, gain, w_step_t, *arrays):
    rows, width = inputs.shape[1:]
    heads = w_step_t.shape[0]
    part = arrays[0].shape[0]
    widths = [sum(a.shape[1] for a in group) for group in (arrays[:4], arrays[4:7], arrays[7:])]
    hbm = pl.BlockSpec(memory_space=pltpu.HBM)
    return pl.pallas_call(
        prep_kernel,
        in_specs=[hbm] * 12,
        out_shape=(
            jax.ShapeDtypeStruct((4, ROWS + part, width // 4), BF16),
            jax.ShapeDtypeStruct((heads, rows), F32),
            jax.ShapeDtypeStruct((part, widths[0]), BF16),
            jax.ShapeDtypeStruct((part, widths[1]), BF16),
        ),
        scratch_shapes=[
            pltpu.VMEM((rows, width), BF16),
            pltpu.VMEM((1, width), F32),
            pltpu.VMEM((heads, width), BF16),
            pltpu.VMEM((part, widths[2]), BF16),
            pltpu.SemaphoreType.DMA((3,)),
            pltpu.SemaphoreType.DMA((9,)),
        ],
        name="prep",
    )(inputs, gain.reshape(1, -1), w_step_t, *arrays)


def halo_kernel(xs_in, halo_ref, gain_ref, xs_out, rim_ref, sem):
    wide = normalised(halo_ref[...], gain_ref[...]).astype(F32)
    for f in range(4):
        for g in range(4):
            rim_ref[f, :, g * 128 : (g + 1) * 128] = shuffled(wide, f, g)
    copy = pltpu.make_async_copy(rim_ref, xs_out.at[:, pl.ds(0, HALO)], sem)
    copy.start()
    copy.wait()


def halo_call(xs, halo, gain):
    anywhere = pl.BlockSpec(memory_space=pl.ANY)
    whole = pl.BlockSpec(memory_space=pltpu.VMEM)
    return pl.pallas_call(
        halo_kernel,
        in_specs=[anywhere, whole, whole],
        out_specs=anywhere,
        out_shape=jax.ShapeDtypeStruct(xs.shape, BF16),
        input_output_aliases={0: 0},
        scratch_shapes=[pltpu.VMEM((4, HALO, xs.shape[2]), BF16), pltpu.SemaphoreType.DMA],
        name="halo",
    )(xs, halo, gain.reshape(1, -1))


def project_kernel(x_ref, w_ref, out_ref):
    for f in range(4):
        out_ref[f] = jnp.dot(
            x_ref[f, 0:ROWS, :], w_ref[...], preferred_element_type=F32
        ).astype(BF16)


def project_call(x, w):
    return pl.pallas_call(
        project_kernel,
        out_shape=jax.ShapeDtypeStruct((4, ROWS, w.shape[1]), BF16),
        compiler_params=vmem(),
        name="project",
    )(x, w)


def added(ref, at, width):
    total = ref[0, :, at : at + width].astype(F32)
    for j in range(1, 4):
        total = total + ref[j, :, at : at + width].astype(F32)
    return total.astype(BF16)


def convolved(wide_ref, taps):
    summed = None
    for i in range(CONV):
        at = HALO - CONV + 1 + i
        part = taps[i : i + 1] * wide_ref[at : at + BLOCK, :]
        summed = part if summed is None else summed + part
    return silu(summed).astype(BF16)


def local_kernel(
    ids, rate, act_ref, step_ref, off_ref, ci_ref, cb_ref, buf_ref,
    send_ref, xin_ref, bkey_ref, rows_ref, cols_ref, wide_ref, sems,
):
    tensor = ids[1]
    moved = pull(
        [
            (buf_ref.at[f, pl.ds(ROWS, 32)], send_ref.at[pl.ds(KEPT + 32 * f, 32)])
            for f in range(4)
        ],
        sems,
    )
    send_ref[0:BLOCK, :] = added(act_ref, 0, 512)[HALO:]
    wide_ref[...] = added(act_ref, 512, 384).astype(F32)
    conv = convolved(wide_ref, jnp.concatenate([ci_ref[...], cb_ref[...]], axis=1))
    xin, bkey = conv[:, 0:256], conv[:, 256:384]
    xin_ref[...] = xin
    bkey_ref[...] = bkey
    row = iota((BLOCK, BLOCK), 0)
    col = iota((BLOCK, BLOCK), 1)
    step = jnp.concatenate([step_ref[pl.ds(4 * tensor + h, 1), :] for h in range(4)], axis=0)
    rates = jnp.concatenate(
        [jnp.full((1, BLOCK), rate[4 * tensor + h], F32) for h in range(4)], axis=0
    )
    decay = off_ref[...] - rates * step
    decay8 = jnp.concatenate([decay, jnp.zeros((4, BLOCK), F32)], axis=0)
    upper = (row <= col).astype(F32)
    cum = jnp.dot(decay8, upper, precision=HIGH, preferred_element_type=F32)
    last = jnp.sum(decay, axis=1, keepdims=True)
    to_end = jnp.exp(last - cum[0:4]) * step
    eye = (row == col).astype(F32)
    cols = lax.dot_general(
        eye, jnp.concatenate([cum[0:4], to_end], axis=0), NT, precision=HIGH,
        preferred_element_type=F32,
    )
    rows_ref[...] = jnp.concatenate([cum[0:4], step], axis=0)
    cols_ref[...] = cols
    wide_key = bkey.astype(F32)
    for h in range(4):
        wk = (wide_key * cols[:, 4 + h : 5 + h]).astype(BF16)
        state = lax.dot_general(
            xin[:, h * 64 : (h + 1) * 64], wk, TN, preferred_element_type=F32
        )
        log = jnp.broadcast_to(last[h : h + 1], (8, BLOCK))
        high = log.astype(BF16).astype(F32)
        logs = jnp.concatenate([high, log - high], axis=0).astype(BF16)
        send_ref[BLOCK : BLOCK + 64, h * 128 : (h + 1) * 128] = state.astype(BF16)
        send_ref[BLOCK + 64 : KEPT, h * 128 : (h + 1) * 128] = logs
    for copy in moved:
        copy.wait()


def local_call(ids, rate, act, step, offset, conv_weight, buf):
    full = lambda *shape: pl.BlockSpec(shape, lambda i, ids, rate: (0,) * len(shape))
    return pl.pallas_call(
        local_kernel,
        grid_spec=pltpu.PrefetchScalarGridSpec(
            num_scalar_prefetch=2,
            grid=(1,),
            in_specs=[
                full(*act.shape),
                full(*step.shape),
                full(*offset.shape),
                pl.BlockSpec((CONV, 256), lambda i, ids, rate: (0, ids[1])),
                pl.BlockSpec((CONV, 128), lambda i, ids, rate: (0, 16 + ids[1])),
                pl.BlockSpec(memory_space=pl.ANY),
            ],
            out_specs=[
                full(SENT, 512), full(BLOCK, 256), full(BLOCK, 128), full(8, BLOCK),
                full(BLOCK, 8),
            ],
            scratch_shapes=[pltpu.VMEM((ROWS, 384), F32), pltpu.SemaphoreType.DMA((4,))],
        ),
        out_shape=(
            jax.ShapeDtypeStruct((SENT, 512), BF16),
            jax.ShapeDtypeStruct((BLOCK, 256), BF16),
            jax.ShapeDtypeStruct((BLOCK, 128), BF16),
            jax.ShapeDtypeStruct((8, BLOCK), F32),
            jax.ShapeDtypeStruct((BLOCK, 8), F32),
        ),
        compiler_params=vmem(),
        name="ssd_local",
    )(ids, rate, act, step, offset, conv_weight, conv_weight, buf)


def inner_kernel(
    ids, act_ref, cc_ref, xin_ref, bkey_ref, rows_ref, cols_ref,
    yin_ref, gate_ref, cq_ref, q_ref, wide_ref,
):
    gate_ref[...] = silu(added(act_ref, 0, 256)[HALO:].astype(F32))
    q_ref[...] = added(act_ref, 384, 256)[HALO:]
    wide_ref[...] = added(act_ref, 256, 128).astype(F32)
    cquery = convolved(wide_ref, cc_ref[...])
    cq_ref[...] = cquery
    lower = iota((BLOCK, BLOCK), 0) >= iota((BLOCK, BLOCK), 1)
    inner = lax.dot_general(cquery, bkey_ref[...], NT, preferred_element_type=F32)
    for h in range(4):
        spread = cols_ref[:, h : h + 1] - rows_ref[h : h + 1, :]
        decayed = jnp.exp(jnp.where(lower, spread, 0.0))
        mix = jnp.where(lower, inner * decayed * rows_ref[4 + h : 5 + h, :], 0.0).astype(BF16)
        yin_ref[:, h * 64 : (h + 1) * 64] = jnp.dot(
            mix, xin_ref[:, h * 64 : (h + 1) * 64], preferred_element_type=F32
        )


def inner_call(ids, act, conv_weight, xin, bkey, rows, cols):
    full = lambda *shape: pl.BlockSpec(shape, lambda i, ids: (0,) * len(shape))
    return pl.pallas_call(
        inner_kernel,
        grid_spec=pltpu.PrefetchScalarGridSpec(
            num_scalar_prefetch=1,
            grid=(1,),
            in_specs=[
                full(*act.shape),
                pl.BlockSpec((CONV, 128), lambda i, ids: (0, 24 + ids[1])),
                full(BLOCK, 256), full(BLOCK, 128), full(8, BLOCK), full(BLOCK, 8),
            ],
            out_specs=[full(BLOCK, 256), full(BLOCK, 256), full(BLOCK, 128), full(BLOCK, 256)],
            scratch_shapes=[pltpu.VMEM((BLOCK + HALO, 128), F32)],
        ),
        out_shape=(
            jax.ShapeDtypeStruct((BLOCK, 256), F32),
            jax.ShapeDtypeStruct((BLOCK, 256), F32),
            jax.ShapeDtypeStruct((BLOCK, 128), BF16),
            jax.ShapeDtypeStruct((BLOCK, 256), BF16),
        ),
        compiler_params=vmem(),
        name="ssd_inner",
    )(ids, act, conv_weight, xin, bkey, rows, cols)


SUB = 256
KEYS = 512
KEPT = BLOCK + 80
SENT = KEPT + BLOCK


def attend_kernel(
    ids, bias, q_ref, yin_ref, gate_ref, cq_ref, cols_ref, gain_ref, all_hbm,
    out_ref, kv_ref, st_ref, w_ref, acc_ref, late_ref, hold_ref, sems, ksems,
):
    block, tensor = ids[0], ids[1]
    per = KEYS // BLOCK
    count = all_hbm.shape[0]
    chunks = range(count // per - 1, -1, -1)

    def move(chunk):
        picked = pl.ds(chunk * per, per)
        return pltpu.make_async_copy(
            all_hbm.at[picked, pl.ds(0, BLOCK)], kv_ref.at[picked], ksems.at[chunk]
        )

    states = pltpu.make_async_copy(all_hbm.at[:, pl.ds(BLOCK, 80)], st_ref, sems.at[0])
    states.start()
    for chunk in chunks:

        @pl.when(chunk * per <= block)
        def _(chunk=chunk):
            move(chunk).start()

    weights = pltpu.make_async_copy(all_hbm.at[:, pl.ds(KEPT, BLOCK)], w_ref, sems.at[1])
    weights.start()
    acc_ref[...] = jnp.zeros_like(acc_ref)
    late_ref[...] = jnp.zeros_like(late_ref)
    hold_ref[...] = jnp.zeros_like(hold_ref)
    states.wait()

    def advance(k, carry):
        logs = st_ref[k, 64:80, :].astype(F32)
        decay = jnp.exp(logs[0:8] + logs[8:16])
        hold_ref[...] = hold_ref[...] * jnp.concatenate([decay] * 8, axis=0) + st_ref[
            k, 0:64, :
        ].astype(F32)
        return carry

    lax.fori_loop(0, block, advance, 0)
    cquery = cq_ref[...]
    ys = []
    for h in range(4):
        enter = hold_ref[:, h * 128 : (h + 1) * 128].astype(BF16)
        moved = lax.dot_general(cquery, enter, NT, preferred_element_type=F32)
        ys.append(moved * jnp.exp(cols_ref[:, h : h + 1]))
    gated = (yin_ref[...] + jnp.concatenate(ys, axis=1)) * gate_ref[...]
    scale = lax.rsqrt(jnp.mean(gated * gated, axis=-1, keepdims=True) + EPS)
    mixed = (gated * scale * gain_ref[...]).astype(BF16)
    after = (iota((SUB, SUB), 0) > iota((SUB, SUB), 1)).astype(BF16)
    ones = jnp.ones((SUB, 128), BF16)
    for chunk in chunks:

        @pl.when(chunk * per <= block)
        def _(chunk=chunk):
            move(chunk).wait()
            for h in range(2):
                late = late_ref[h]
                gained = acc_ref[h]
                query = q_ref[:, h * 128 : (h + 1) * 128]
                for sub in range(KEYS // SUB - 1, -1, -1):
                    at = chunk * KEYS + sub * SUB
                    first = at // BLOCK
                    before = at + iota((BLOCK, SUB), 1) < block * BLOCK + iota((BLOCK, SUB), 0)
                    key = kv_ref[first : first + 2, :, h * 128 : (h + 1) * 128]
                    value = kv_ref[first : first + 2, :, 256 + h * 128 : 256 + (h + 1) * 128]
                    logits = lax.dot_general(
                        query, key.reshape(SUB, 128), NT, preferred_element_type=F32
                    )
                    logits = logits * (128 ** -0.5) + bias[2 * tensor + h]
                    soft = jnp.maximum(logits, 0.0) + jnp.log(1.0 + jnp.exp(-jnp.abs(logits)))
                    passed = jnp.where(before, -soft, 0.0)
                    high = passed.astype(BF16)
                    low = (passed - high.astype(F32)).astype(BF16)
                    tail = jnp.dot(high, after, preferred_element_type=F32) + jnp.dot(
                        low, after, preferred_element_type=F32
                    )
                    whole = jnp.dot(high, ones, preferred_element_type=F32) + jnp.dot(
                        low, ones, preferred_element_type=F32
                    )
                    later = jnp.concatenate([late] * (SUB // 128), axis=1)
                    weight = jnp.where(before, jnp.exp(logits - soft + (tail + later)), 0.0)
                    gained = gained + jnp.dot(
                        weight.astype(BF16), value.reshape(SUB, 128), preferred_element_type=F32
                    )
                    late = late + whole
                late_ref[h] = late
                acc_ref[h] = gained

    both = jnp.concatenate([mixed, acc_ref[0].astype(BF16), acc_ref[1].astype(BF16)], axis=1)
    weights.wait()
    for s in range(count):
        out_ref[:, 128 * s : 128 * (s + 1)] = lax.dot_general(
            both, w_ref[s], NT, preferred_element_type=F32
        ).astype(BF16)


def attend_call(ids, bias, q, yin, gate, cq, cols, gain, gathered):
    full = lambda *shape: pl.BlockSpec(shape, lambda i, ids, bias: (0,) * len(shape))
    count = gathered.shape[0]
    return pl.pallas_call(
        attend_kernel,
        grid_spec=pltpu.PrefetchScalarGridSpec(
            num_scalar_prefetch=2,
            grid=(1,),
            in_specs=[
                full(BLOCK, 256), full(BLOCK, 256), full(BLOCK, 256), full(BLOCK, 128),
                full(BLOCK, 8), pl.BlockSpec((1, 256), lambda i, ids, bias: (0, ids[1])),
                pl.BlockSpec(memory_space=pltpu.HBM),
            ],
            out_specs=full(BLOCK, 2048),
            scratch_shapes=[
                pltpu.VMEM((count, BLOCK, 512), BF16),
                pltpu.VMEM((count, 80, 512), BF16),
                pltpu.VMEM((count, BLOCK, 512), BF16),
                pltpu.VMEM((2, BLOCK, 128), F32),
                pltpu.VMEM((2, BLOCK, 128), F32),
                pltpu.VMEM((64, 512), F32),
                pltpu.SemaphoreType.DMA((2,)),
                pltpu.SemaphoreType.DMA((count * BLOCK // KEYS,)),
            ],
        ),
        out_shape=jax.ShapeDtypeStruct((BLOCK, 2048), BF16),
        compiler_params=vmem(),
        name="attend",
    )(ids, bias, q, yin, gate, cq, cols, gain.reshape(1, -1), gathered)


def body(
    inputs, norm_gain, w_gate, w_input, w_bkey, w_cquery, w_step, conv_weight, decay_rate,
    decay_offset, ssd_gain, w_query, w_key, w_value, stick_bias, out_mixer, out_attend,
):
    length = lax.axis_size("sp")
    ids = jnp.stack([lax.axis_index("sp"), lax.axis_index("tp")]).astype(jnp.int32)
    halo = lax.ppermute(
        inputs[0, BLOCK - HALO :], "sp", [(i, i + 1) for i in range(length - 1)]
    )
    split, step, first, second = prep_call(
        inputs, norm_gain, w_step.T, w_key, w_value, w_input, w_bkey, w_gate, w_cquery, w_query,
        out_mixer.T, out_attend.T,
    )
    split = halo_call(split, halo, norm_gain)
    tokens = lax.all_to_all(split, "fs", 0, 0, tiled=True)

    def projected(weights):
        whole = lax.all_gather(weights, "sp", axis=0, tiled=True)
        return lax.all_to_all(project_call(tokens, whole), "fs", 0, 0, tiled=True)

    send, xin, bkey, srows, scols = local_call(
        ids, decay_rate, projected(first), step, decay_offset[0].T, conv_weight, tokens
    )
    gathered = lax.all_gather(send, "sp", axis=0)
    yin, gate, cq, q = inner_call(ids, projected(second), conv_weight, xin, bkey, srows, scols)
    partial = attend_call(ids, stick_bias, q, yin, gate, cq, scols, ssd_gain, gathered)
    parts = lax.all_to_all(partial.reshape(8, 16, 2048), "tp", 0, 0, tiled=True)
    return jnp.sum(parts.astype(F32), axis=0).astype(BF16)[None]


def solution(mesh):
    shard = P(("sp", "fs"), "tp")
    return jax.shard_map(
        body,
        mesh=mesh,
        in_specs=(
            P("fs", "sp", None), P(), shard, shard, shard, shard, P(), P(), P(),
            P("fs", "sp", "tp"), P(), shard, shard, shard, P(),
            P("tp", ("sp", "fs")), P("tp", ("sp", "fs")),
        ),
        out_specs=P("fs", ("sp", "tp"), None),
        check_vma=False,
    )
```

```python
import jax
import jax.numpy as jnp
from jax import lax
from jax.experimental import pallas as pl
from jax.experimental.pallas import tpu as pltpu
from jax.sharding import PartitionSpec as P

BLOCK = 128
CONV = 4
EPS = 1e-06
HALO = 16
ROWS = BLOCK + HALO
F32 = jnp.float32
BF16 = jnp.bfloat16
HIGH = lax.Precision.HIGHEST
NT = (((1,), (1,)), ((), ()))
TN = (((0,), (0,)), ((), ()))


def vmem(limit=48):
    return pltpu.CompilerParams(vmem_limit_bytes=limit * 1024 * 1024)


def iota(shape, dim):
    return lax.broadcasted_iota(jnp.int32, shape, dim)


def softplus(x):
    return jnp.maximum(x, 0.0) + jnp.log1p(jnp.exp(-jnp.abs(x)))


def silu(x):
    return x / (1.0 + jnp.exp(-x))


def pull(pairs, sems):
    copies = [pltpu.make_async_copy(src, dst, sems.at[i]) for i, (src, dst) in enumerate(pairs)]
    for copy in copies:
        copy.start()
    return copies


def shuffled(normed, f, g):
    lane = iota((normed.shape[0], 128), 1) // 32
    out = None
    for k in range(4):
        at = (4 * g + k) * 128
        piece = normed[:, at : at + 128]
        shift = ((k - f) * 32) % 128
        if shift:
            piece = pltpu.roll(piece, shift, 1)
        out = piece if out is None else jnp.where(lane == k, piece, out)
    return out.astype(BF16)


def normalised(x, gain):
    wide = x.astype(F32)
    scale = lax.rsqrt(jnp.mean(wide * wide, axis=-1, keepdims=True) + EPS)
    return (wide * scale * gain).astype(BF16)


def prep_kernel(*refs):
    x_hbm, gain_hbm, ws_hbm = refs[:3]
    sources = refs[3:12]
    xs_ref, step_ref, first_ref, second_ref = refs[12:16]
    x_ref, gain_ref, ws_ref, third_ref, sems, wsems = refs[16:]
    early = pull(((x_hbm.at[0], x_ref), (gain_hbm, gain_ref), (ws_hbm, ws_ref)), sems)
    pairs = []
    outs = (first_ref, second_ref, third_ref)
    at, which = 0, 0
    for n, src in enumerate(sources):
        if n in (4, 8):
            at, which = 0, which + 1
        pairs.append((src, outs[which].at[:, pl.ds(at, src.shape[1])]))
        at += src.shape[1]
    later = pull(pairs, wsems)
    for copy in early:
        copy.wait()
    normed = normalised(x_ref[...], gain_ref[...])
    step_ref[...] = softplus(
        lax.dot_general(ws_ref[...], normed, NT, preferred_element_type=F32)
    )
    wide = normed.astype(F32)
    for f in range(4):
        for g in range(4):
            xs_ref[f, HALO:ROWS, g * 128 : (g + 1) * 128] = shuffled(wide, f, g)
    for copy in later:
        copy.wait()
    for f in range(4):
        xs_ref[f, ROWS:, 0:256] = third_ref[0:16, :]
        xs_ref[f, ROWS:, 256:512] = third_ref[16:32, :]


def prep_call(inputs, gain, w_step_t, *arrays):
    rows, width = inputs.shape[1:]
    heads = w_step_t.shape[0]
    part = arrays[0].shape[0]
    widths = [sum(a.shape[1] for a in group) for group in (arrays[:4], arrays[4:8], arrays[8:])]
    hbm = pl.BlockSpec(memory_space=pltpu.HBM)
    return pl.pallas_call(
        prep_kernel,
        in_specs=[hbm] * 12,
        out_shape=(
            jax.ShapeDtypeStruct((4, ROWS + HALO, width // 4), BF16),
            jax.ShapeDtypeStruct((heads, rows), F32),
            jax.ShapeDtypeStruct((part, widths[0]), BF16),
            jax.ShapeDtypeStruct((part, widths[1]), BF16),
        ),
        scratch_shapes=[
            pltpu.VMEM((rows, width), BF16),
            pltpu.VMEM((1, width), F32),
            pltpu.VMEM((heads, width), BF16),
            pltpu.VMEM((part, widths[2]), BF16),
            pltpu.SemaphoreType.DMA((3,)),
            pltpu.SemaphoreType.DMA((9,)),
        ],
        name="prep",
    )(inputs, gain.reshape(1, -1), w_step_t, *arrays)


def halo_kernel(xs_in, halo_ref, gain_ref, xs_out, rim_ref, sem):
    wide = normalised(halo_ref[...], gain_ref[...]).astype(F32)
    for f in range(4):
        for g in range(4):
            rim_ref[f, :, g * 128 : (g + 1) * 128] = shuffled(wide, f, g)
    copy = pltpu.make_async_copy(rim_ref, xs_out.at[:, pl.ds(0, HALO)], sem)
    copy.start()
    copy.wait()


def halo_call(xs, halo, gain):
    anywhere = pl.BlockSpec(memory_space=pl.ANY)
    whole = pl.BlockSpec(memory_space=pltpu.VMEM)
    return pl.pallas_call(
        halo_kernel,
        in_specs=[anywhere, whole, whole],
        out_specs=anywhere,
        out_shape=jax.ShapeDtypeStruct(xs.shape, BF16),
        input_output_aliases={0: 0},
        scratch_shapes=[pltpu.VMEM((4, HALO, xs.shape[2]), BF16), pltpu.SemaphoreType.DMA],
        name="halo",
    )(xs, halo, gain.reshape(1, -1))


def project_kernel(x_ref, w_ref, out_ref, *kept):
    width = out_ref.shape[2]
    for f in range(4):
        out_ref[f] = jnp.dot(
            x_ref[f, 0:ROWS, :], w_ref[:, 0:width], preferred_element_type=F32
        ).astype(BF16)
    for ref in kept:
        ref[...] = w_ref[:, width:]


def project_call(x, w, width):
    outs = [jax.ShapeDtypeStruct((4, ROWS, width), BF16)]
    if w.shape[1] > width:
        outs.append(jax.ShapeDtypeStruct((w.shape[0], w.shape[1] - width), BF16))
    return pl.pallas_call(
        project_kernel,
        out_shape=outs,
        compiler_params=vmem(),
        name="project",
    )(x, w)


def added(ref, at, width):
    total = ref[0, :, at : at + width].astype(F32)
    for j in range(1, 4):
        total = total + ref[j, :, at : at + width].astype(F32)
    return total.astype(BF16)


def convolved(wide_ref, taps):
    summed = None
    for i in range(CONV):
        at = HALO - CONV + 1 + i
        part = taps[i : i + 1] * wide_ref[at : at + BLOCK, :]
        summed = part if summed is None else summed + part
    return silu(summed).astype(BF16)


def local_kernel(
    ids, rate, act_ref, step_ref, off_ref, ci_ref, cb_ref, buf_ref,
    send_ref, xin_ref, bkey_ref, rows_ref, cols_ref, wide_ref, sems,
):
    tensor = ids[1]
    moved = pull(
        [
            (buf_ref.at[f, pl.ds(ROWS, HALO)], send_ref.at[pl.ds(KEPT + HALO * f, HALO)])
            for f in range(4)
        ],
        sems,
    )
    send_ref[0:BLOCK, :] = added(act_ref, 0, 512)[HALO:]
    wide_ref[...] = added(act_ref, 512, 384).astype(F32)
    conv = convolved(wide_ref, jnp.concatenate([ci_ref[...], cb_ref[...]], axis=1))
    xin, bkey = conv[:, 0:256], conv[:, 256:384]
    xin_ref[...] = xin
    bkey_ref[...] = bkey
    row = iota((BLOCK, BLOCK), 0)
    col = iota((BLOCK, BLOCK), 1)
    step = jnp.concatenate([step_ref[pl.ds(4 * tensor + h, 1), :] for h in range(4)], axis=0)
    rates = jnp.concatenate(
        [jnp.full((1, BLOCK), rate[4 * tensor + h], F32) for h in range(4)], axis=0
    )
    decay = off_ref[...] - rates * step
    decay8 = jnp.concatenate([decay, jnp.zeros((4, BLOCK), F32)], axis=0)
    upper = (row <= col).astype(F32)
    cum = jnp.dot(decay8, upper, precision=HIGH, preferred_element_type=F32)
    last = jnp.sum(decay, axis=1, keepdims=True)
    to_end = jnp.exp(last - cum[0:4]) * step
    eye = (row == col).astype(F32)
    cols = lax.dot_general(
        eye, jnp.concatenate([cum[0:4], to_end], axis=0), NT, precision=HIGH,
        preferred_element_type=F32,
    )
    rows_ref[...] = jnp.concatenate([cum[0:4], step], axis=0)
    cols_ref[...] = cols
    wide_key = bkey.astype(F32)
    for h in range(4):
        wk = (wide_key * cols[:, 4 + h : 5 + h]).astype(BF16)
        state = lax.dot_general(
            xin[:, h * 64 : (h + 1) * 64], wk, TN, preferred_element_type=F32
        )
        log = jnp.broadcast_to(last[h : h + 1], (8, BLOCK))
        high = log.astype(BF16).astype(F32)
        logs = jnp.concatenate([high, log - high], axis=0).astype(BF16)
        send_ref[BLOCK : BLOCK + 64, h * 128 : (h + 1) * 128] = state.astype(BF16)
        send_ref[BLOCK + 64 : KEPT, h * 128 : (h + 1) * 128] = logs
    for copy in moved:
        copy.wait()


def local_call(ids, rate, act, step, offset, conv_weight, buf):
    full = lambda *shape: pl.BlockSpec(shape, lambda i, ids, rate: (0,) * len(shape))
    return pl.pallas_call(
        local_kernel,
        grid_spec=pltpu.PrefetchScalarGridSpec(
            num_scalar_prefetch=2,
            grid=(1,),
            in_specs=[
                full(*act.shape),
                full(*step.shape),
                full(*offset.shape),
                pl.BlockSpec((CONV, 256), lambda i, ids, rate: (0, ids[1])),
                pl.BlockSpec((CONV, 128), lambda i, ids, rate: (0, 16 + ids[1])),
                pl.BlockSpec(memory_space=pl.ANY),
            ],
            out_specs=[
                full(SENT, 512), full(BLOCK, 256), full(BLOCK, 128), full(8, BLOCK),
                full(BLOCK, 8),
            ],
            scratch_shapes=[pltpu.VMEM((ROWS, 384), F32), pltpu.SemaphoreType.DMA((4,))],
        ),
        out_shape=(
            jax.ShapeDtypeStruct((SENT, 512), BF16),
            jax.ShapeDtypeStruct((BLOCK, 256), BF16),
            jax.ShapeDtypeStruct((BLOCK, 128), BF16),
            jax.ShapeDtypeStruct((8, BLOCK), F32),
            jax.ShapeDtypeStruct((BLOCK, 8), F32),
        ),
        compiler_params=vmem(),
        name="ssd_local",
    )(ids, rate, act, step, offset, conv_weight, conv_weight, buf)


def inner_kernel(
    ids, act_ref, cc_ref, xin_ref, bkey_ref, rows_ref, cols_ref,
    yin_ref, gate_ref, cq_ref, q_ref, wide_ref,
):
    gate_ref[...] = silu(added(act_ref, 0, 256)[HALO:].astype(F32))
    q_ref[...] = added(act_ref, 384, 256)[HALO:]
    wide_ref[...] = added(act_ref, 256, 128).astype(F32)
    cquery = convolved(wide_ref, cc_ref[...])
    cq_ref[...] = cquery
    lower = iota((BLOCK, BLOCK), 0) >= iota((BLOCK, BLOCK), 1)
    inner = lax.dot_general(cquery, bkey_ref[...], NT, preferred_element_type=F32)
    for h in range(4):
        spread = cols_ref[:, h : h + 1] - rows_ref[h : h + 1, :]
        decayed = jnp.exp(jnp.where(lower, spread, 0.0))
        mix = jnp.where(lower, inner * decayed * rows_ref[4 + h : 5 + h, :], 0.0).astype(BF16)
        yin_ref[:, h * 64 : (h + 1) * 64] = jnp.dot(
            mix, xin_ref[:, h * 64 : (h + 1) * 64], preferred_element_type=F32
        )


def inner_call(ids, act, conv_weight, xin, bkey, rows, cols):
    full = lambda *shape: pl.BlockSpec(shape, lambda i, ids: (0,) * len(shape))
    return pl.pallas_call(
        inner_kernel,
        grid_spec=pltpu.PrefetchScalarGridSpec(
            num_scalar_prefetch=1,
            grid=(1,),
            in_specs=[
                full(*act.shape),
                pl.BlockSpec((CONV, 128), lambda i, ids: (0, 24 + ids[1])),
                full(BLOCK, 256), full(BLOCK, 128), full(8, BLOCK), full(BLOCK, 8),
            ],
            out_specs=[full(BLOCK, 256), full(BLOCK, 256), full(BLOCK, 128), full(BLOCK, 256)],
            scratch_shapes=[pltpu.VMEM((BLOCK + HALO, 128), F32)],
        ),
        out_shape=(
            jax.ShapeDtypeStruct((BLOCK, 256), F32),
            jax.ShapeDtypeStruct((BLOCK, 256), F32),
            jax.ShapeDtypeStruct((BLOCK, 128), BF16),
            jax.ShapeDtypeStruct((BLOCK, 256), BF16),
        ),
        compiler_params=vmem(),
        name="ssd_inner",
    )(ids, act, conv_weight, xin, bkey, rows, cols)


SUB = 256
KEYS = 512
KEPT = BLOCK + 80
SENT = KEPT + 64
LOG2E = 1.4426950408889634


def attend_kernel(
    ids, bias, q_ref, yin_ref, gate_ref, cq_ref, cols_ref, gain_ref, all_hbm, a0, a1, a2, a3,
    out_ref, kv_ref, st_ref, wm_ref, wa_ref, acc_ref, late_ref, hold_ref, sems, ksems,
):
    block, tensor, mine = ids[0], ids[1], ids[2]
    per = KEYS // BLOCK
    count = all_hbm.shape[0]
    chunks = range(count // per - 1, -1, -1)
    last = block // per

    def move(chunk):
        picked = pl.ds(chunk * per, per)
        return pltpu.make_async_copy(
            all_hbm.at[picked, pl.ds(0, BLOCK)], kv_ref.at[picked], ksems.at[chunk]
        )

    states = pltpu.make_async_copy(all_hbm.at[:, pl.ds(BLOCK, 80)], st_ref, sems.at[0])
    states.start()
    for chunk in chunks:

        @pl.when(chunk <= last)
        def _(chunk=chunk):
            move(chunk).start()

    weights = [pltpu.make_async_copy(all_hbm.at[:, pl.ds(KEPT, 64)], wm_ref, sems.at[1])]
    weights += [
        pltpu.make_async_copy(w, wa_ref.at[(mine + 4 - r) % 4], sems.at[2 + r])
        for r, w in enumerate((a0, a1, a2, a3))
    ]
    for copy in weights:
        copy.start()
    acc_ref[...] = jnp.zeros_like(acc_ref)
    late_ref[...] = jnp.zeros_like(late_ref)
    hold_ref[...] = jnp.zeros_like(hold_ref)
    states.wait()

    def advance(k, carry):
        logs = st_ref[k, 64:80, :].astype(F32)
        decay = jnp.exp(logs[0:8] + logs[8:16])
        hold_ref[...] = hold_ref[...] * jnp.concatenate([decay] * 8, axis=0) + st_ref[
            k, 0:64, :
        ].astype(F32)
        return carry

    lax.fori_loop(0, block, advance, 0)
    cquery = cq_ref[...]
    ys = []
    for h in range(4):
        enter = hold_ref[:, h * 128 : (h + 1) * 128].astype(BF16)
        moved = lax.dot_general(cquery, enter, NT, preferred_element_type=F32)
        ys.append(moved * jnp.exp(cols_ref[:, h : h + 1]))
    gated = (yin_ref[...] + jnp.concatenate(ys, axis=1)) * gate_ref[...]
    scale = lax.rsqrt(jnp.mean(gated * gated, axis=-1, keepdims=True) + EPS)
    mixed = (gated * scale * gain_ref[...]).astype(BF16)
    onward = (iota((2 * SUB, SUB), 0) % SUB > iota((2 * SUB, SUB), 1)).astype(BF16)

    def piece(chunk, masked):
        move(chunk).wait()
        for h in range(2):
            late = late_ref[h]
            gained = acc_ref[h]
            query = q_ref[:, h * 128 : (h + 1) * 128]
            offset = bias[2 * tensor + h] * LOG2E
            for sub in range(KEYS // SUB - 1, -1, -1):
                at = chunk * KEYS + sub * SUB
                first = at // BLOCK
                key = kv_ref[first : first + 2, :, h * 128 : (h + 1) * 128]
                value = kv_ref[first : first + 2, :, 256 + h * 128 : 256 + (h + 1) * 128]
                logits = lax.dot_general(
                    query, key.reshape(SUB, 128), NT, preferred_element_type=F32
                )
                logits = logits * (128 ** -0.5 * LOG2E) + offset
                soft = jnp.maximum(logits, 0.0) + LOG2E * jnp.log(
                    1.0 + jnp.exp2(-jnp.abs(logits))
                )
                taken = logits - soft
                if masked:
                    before = at + iota((BLOCK, SUB), 1) < block * BLOCK + iota((BLOCK, SUB), 0)
                    soft = jnp.where(before, soft, 0.0)
                high = soft.astype(BF16)
                low = (soft - high.astype(F32)).astype(BF16)
                tail = jnp.dot(
                    jnp.concatenate([high, low], axis=1), onward, preferred_element_type=F32
                )
                later = jnp.concatenate([late] * (SUB // 128), axis=1)
                weight = jnp.exp2(taken - (tail + later))
                if masked:
                    weight = jnp.where(before, weight, 0.0)
                gained = gained + jnp.dot(
                    weight.astype(BF16), value.reshape(SUB, 128), preferred_element_type=F32
                )
                late = late + jnp.broadcast_to(tail[:, 0:1] + soft[:, 0:1], (BLOCK, 128))
            late_ref[h] = late
            acc_ref[h] = gained

    for chunk in chunks:
        pl.when(chunk == last)(lambda chunk=chunk: piece(chunk, True))
        pl.when(chunk < last)(lambda chunk=chunk: piece(chunk, False))

    attended = jnp.concatenate([acc_ref[0].astype(BF16), acc_ref[1].astype(BF16)], axis=1)
    for copy in weights:
        copy.wait()
    for s in range(count):
        halves = []
        for f in range(4):
            for half in range(2):
                halves.append(
                    wm_ref[s, 16 * f : 16 * (f + 1), 256 * half : 256 * (half + 1)]
                )
        rows_m = jnp.concatenate(halves, axis=0)
        rows_a = jnp.concatenate(
            [wa_ref[f, 32 * s : 32 * (s + 1), :] for f in range(4)], axis=0
        )
        out_ref[:, 128 * s : 128 * (s + 1)] = (
            lax.dot_general(mixed, rows_m, NT, preferred_element_type=F32)
            + lax.dot_general(attended, rows_a, NT, preferred_element_type=F32)
        ).astype(BF16)


def attend_call(ids, bias, q, yin, gate, cq, cols, gain, gathered, rows):
    full = lambda *shape: pl.BlockSpec(shape, lambda i, ids, bias: (0,) * len(shape))
    count = gathered.shape[0]
    hbm = pl.BlockSpec(memory_space=pl.ANY)
    return pl.pallas_call(
        attend_kernel,
        grid_spec=pltpu.PrefetchScalarGridSpec(
            num_scalar_prefetch=2,
            grid=(1,),
            in_specs=[
                full(BLOCK, 256), full(BLOCK, 256), full(BLOCK, 256), full(BLOCK, 128),
                full(BLOCK, 8), pl.BlockSpec((1, 256), lambda i, ids, bias: (0, ids[1])),
                pl.BlockSpec(memory_space=pltpu.HBM), hbm, hbm, hbm, hbm,
            ],
            out_specs=full(BLOCK, 2048),
            scratch_shapes=[
                pltpu.VMEM((count, BLOCK, 512), BF16),
                pltpu.VMEM((count, 80, 512), BF16),
                pltpu.VMEM((count, 64, 512), BF16),
                pltpu.VMEM((4, 512, 256), BF16),
                pltpu.VMEM((2, BLOCK, 128), F32),
                pltpu.VMEM((2, BLOCK, 128), F32),
                pltpu.VMEM((64, 512), F32),
                pltpu.SemaphoreType.DMA((6,)),
                pltpu.SemaphoreType.DMA((count * BLOCK // KEYS,)),
            ],
        ),
        out_shape=jax.ShapeDtypeStruct((BLOCK, 2048), BF16),
        compiler_params=vmem(),
        name="attend",
    )(ids, bias, q, yin, gate, cq, cols, gain.reshape(1, -1), gathered, *rows)


def rotated(shard, axis, by):
    length = lax.axis_size(axis)
    return lax.ppermute(shard, axis, [(i, (i + by) % length) for i in range(length)])


def body(
    inputs, norm_gain, w_gate, w_input, w_bkey, w_cquery, w_step, conv_weight, decay_rate,
    decay_offset, ssd_gain, w_query, w_key, w_value, stick_bias, out_mixer, out_attend,
):
    length = lax.axis_size("sp")
    ids = jnp.stack([lax.axis_index(name) for name in ("sp", "tp", "fs")]).astype(jnp.int32)
    halo = lax.ppermute(
        inputs[0, BLOCK - HALO :], "sp", [(i, i + 1) for i in range(length - 1)]
    )
    split, step, first, second = prep_call(
        inputs, norm_gain, w_step.T, w_key, w_value, w_input, w_bkey, w_gate, w_cquery, w_query,
        out_attend.T, out_mixer.T,
    )
    split = halo_call(split, halo, norm_gain)
    tokens = lax.all_to_all(split, "fs", 0, 0, tiled=True)

    def projected(weights, width):
        whole = lax.all_gather(weights, "sp", axis=0, tiled=True)
        act, *kept = project_call(tokens, whole, width)
        return lax.all_to_all(act, "fs", 0, 0, tiled=True), *kept

    (act,) = projected(first, 896)
    send, xin, bkey, srows, scols = local_call(
        ids, decay_rate, act, step, decay_offset[0].T, conv_weight, tokens
    )
    gathered = lax.all_gather(send, "sp", axis=0)
    act, kept = projected(second, 640)
    rows = [kept] + [rotated(kept, "fs", by) for by in (1, 2, 3)]
    yin, gate, cq, q = inner_call(ids, act, conv_weight, xin, bkey, srows, scols)
    partial = attend_call(ids, stick_bias, q, yin, gate, cq, scols, ssd_gain, gathered, rows)
    parts = lax.all_to_all(partial.reshape(8, 16, 2048), "tp", 0, 0, tiled=True)
    return jnp.sum(parts.astype(F32), axis=0).astype(BF16)[None]


def solution(mesh):
    shard = P(("sp", "fs"), "tp")
    return jax.shard_map(
        body,
        mesh=mesh,
        in_specs=(
            P("fs", "sp", None), P(), shard, shard, shard, shard, P(), P(), P(),
            P("fs", "sp", "tp"), P(), shard, shard, shard, P(),
            P("tp", ("sp", "fs")), P("tp", ("sp", "fs")),
        ),
        out_specs=P("fs", ("sp", "tp"), None),
        check_vma=False,
    )
```

```python
import jax
import jax.numpy as jnp
from jax import lax
from jax.experimental import pallas as pl
from jax.experimental.pallas import tpu as pltpu
from jax.sharding import PartitionSpec as P

BLOCK = 128
CONV = 4
EPS = 1e-06
HALO = 16
ROWS = BLOCK + HALO
F32 = jnp.float32
BF16 = jnp.bfloat16
HIGH = lax.Precision.HIGHEST
NT = (((1,), (1,)), ((), ()))
TN = (((0,), (0,)), ((), ()))


def vmem(limit=48):
    return pltpu.CompilerParams(vmem_limit_bytes=limit * 1024 * 1024)


def iota(shape, dim):
    return lax.broadcasted_iota(jnp.int32, shape, dim)


def softplus(x):
    return jnp.maximum(x, 0.0) + jnp.log1p(jnp.exp(-jnp.abs(x)))


def silu(x):
    return x / (1.0 + jnp.exp(-x))


def pull(pairs, sems):
    copies = [pltpu.make_async_copy(src, dst, sems.at[i]) for i, (src, dst) in enumerate(pairs)]
    for copy in copies:
        copy.start()
    return copies


def shuffled(normed, f, g):
    lane = iota((normed.shape[0], 128), 1) // 32
    out = None
    for k in range(4):
        at = (4 * g + k) * 128
        piece = normed[:, at : at + 128]
        shift = ((k - f) * 32) % 128
        if shift:
            piece = pltpu.roll(piece, shift, 1)
        out = piece if out is None else jnp.where(lane == k, piece, out)
    return out.astype(BF16)


def normalised(x, gain):
    wide = x.astype(F32)
    scale = lax.rsqrt(jnp.mean(wide * wide, axis=-1, keepdims=True) + EPS)
    return (wide * scale * gain).astype(BF16)


def prep_kernel(*refs):
    x_hbm, gain_hbm, ws_hbm = refs[:3]
    sources = refs[3:12]
    xs_ref, step_ref, first_ref, second_ref = refs[12:16]
    x_ref, gain_ref, ws_ref, third_ref, sems, wsems = refs[16:]
    early = pull(((x_hbm.at[0], x_ref), (gain_hbm, gain_ref), (ws_hbm, ws_ref)), sems)
    pairs = []
    outs = (first_ref, second_ref, third_ref)
    at, which = 0, 0
    for n, src in enumerate(sources):
        if n in (4, 8):
            at, which = 0, which + 1
        pairs.append((src, outs[which].at[:, pl.ds(at, src.shape[1])]))
        at += src.shape[1]
    later = pull(pairs, wsems)
    for copy in early:
        copy.wait()
    normed = normalised(x_ref[...], gain_ref[...])
    step_ref[...] = softplus(
        lax.dot_general(ws_ref[...], normed, NT, preferred_element_type=F32)
    )
    wide = normed.astype(F32)
    for f in range(4):
        for g in range(4):
            xs_ref[f, 0:BLOCK, g * 128 : (g + 1) * 128] = shuffled(wide, f, g)
    for copy in later:
        copy.wait()
    for f in range(4):
        xs_ref[f, BLOCK:, 0:256] = third_ref[0:16, :]
        xs_ref[f, BLOCK:, 256:512] = third_ref[16:32, :]


def prep_call(inputs, gain, w_step_t, *arrays):
    rows, width = inputs.shape[1:]
    heads = w_step_t.shape[0]
    part = arrays[0].shape[0]
    widths = [sum(a.shape[1] for a in group) for group in (arrays[:4], arrays[4:8], arrays[8:])]
    hbm = pl.BlockSpec(memory_space=pltpu.HBM)
    return pl.pallas_call(
        prep_kernel,
        in_specs=[hbm] * 12,
        out_shape=(
            jax.ShapeDtypeStruct((4, rows + HALO, width // 4), BF16),
            jax.ShapeDtypeStruct((heads, rows), F32),
            jax.ShapeDtypeStruct((part, widths[0]), BF16),
            jax.ShapeDtypeStruct((part, widths[1]), BF16),
        ),
        scratch_shapes=[
            pltpu.VMEM((rows, width), BF16),
            pltpu.VMEM((1, width), F32),
            pltpu.VMEM((heads, width), BF16),
            pltpu.VMEM((part, widths[2]), BF16),
            pltpu.SemaphoreType.DMA((3,)),
            pltpu.SemaphoreType.DMA((9,)),
        ],
        name="prep",
    )(inputs, gain.reshape(1, -1), w_step_t, *arrays)


def project_kernel(x_ref, rim_ref, w_ref, out_hbm, *rest):
    kept, (out_ref, sems) = rest[:-2], rest[-2:]
    width = out_hbm.shape[2]
    weights = w_ref[:, 0:width]
    copies = []
    for f in range(4):
        rows = jnp.concatenate([rim_ref[f], x_ref[f, 0:BLOCK, :]], axis=0)
        out_ref[f] = jnp.dot(rows, weights, preferred_element_type=F32).astype(BF16)
        copies.append(pltpu.make_async_copy(out_ref.at[f], out_hbm.at[f], sems.at[f]))
        copies[-1].start()
    for ref in kept:
        ref[...] = w_ref[:, width:]
    for copy in copies:
        copy.wait()


def project_call(x, rim, w, width):
    whole = pl.BlockSpec(memory_space=pltpu.VMEM)
    outs = [jax.ShapeDtypeStruct((4, ROWS, width), BF16)]
    specs = [pl.BlockSpec(memory_space=pltpu.HBM)]
    if w.shape[1] > width:
        outs.append(jax.ShapeDtypeStruct((w.shape[0], w.shape[1] - width), BF16))
        specs.append(whole)
    return pl.pallas_call(
        project_kernel,
        in_specs=[whole] * 3,
        out_specs=specs,
        out_shape=outs,
        scratch_shapes=[pltpu.VMEM((4, ROWS, width), BF16), pltpu.SemaphoreType.DMA((4,))],
        compiler_params=vmem(),
        name="project",
    )(x, rim, w)


def added(ref, at, width):
    total = ref[0, :, at : at + width].astype(F32)
    for j in range(1, 4):
        total = total + ref[j, :, at : at + width].astype(F32)
    return total.astype(BF16)


def convolved(wide_ref, taps):
    summed = None
    for i in range(CONV):
        at = HALO - CONV + 1 + i
        part = taps[i : i + 1] * wide_ref[at : at + BLOCK, :]
        summed = part if summed is None else summed + part
    return silu(summed).astype(BF16)


def local_kernel(
    ids, rate, act_ref, step_ref, off_ref, ci_ref, cb_ref, buf_ref,
    send_ref, xin_ref, bkey_ref, rows_ref, cols_ref, wide_ref, sems,
):
    tensor = ids[1]
    moved = pull(
        [
            (buf_ref.at[f, pl.ds(BLOCK, HALO)], send_ref.at[pl.ds(KEPT + HALO * f, HALO)])
            for f in range(4)
        ],
        sems,
    )
    send_ref[0:BLOCK, :] = added(act_ref, 0, 512)[HALO:]
    wide_ref[...] = added(act_ref, 512, 384).astype(F32)
    conv = convolved(wide_ref, jnp.concatenate([ci_ref[...], cb_ref[...]], axis=1))
    xin, bkey = conv[:, 0:256], conv[:, 256:384]
    xin_ref[...] = xin
    bkey_ref[...] = bkey
    row = iota((BLOCK, BLOCK), 0)
    col = iota((BLOCK, BLOCK), 1)
    step = jnp.concatenate([step_ref[pl.ds(4 * tensor + h, 1), :] for h in range(4)], axis=0)
    rates = jnp.concatenate(
        [jnp.full((1, BLOCK), rate[4 * tensor + h], F32) for h in range(4)], axis=0
    )
    decay = off_ref[...] - rates * step
    decay8 = jnp.concatenate([decay, jnp.zeros((4, BLOCK), F32)], axis=0)
    upper = (row <= col).astype(F32)
    cum = jnp.dot(decay8, upper, precision=HIGH, preferred_element_type=F32)
    last = jnp.sum(decay, axis=1, keepdims=True)
    to_end = jnp.exp(last - cum[0:4]) * step
    eye = (row == col).astype(F32)
    cols = lax.dot_general(
        eye, jnp.concatenate([cum[0:4], to_end], axis=0), NT, precision=HIGH,
        preferred_element_type=F32,
    )
    rows_ref[...] = jnp.concatenate([cum[0:4], step], axis=0)
    cols_ref[...] = cols
    wide_key = bkey.astype(F32)
    for h in range(4):
        wk = (wide_key * cols[:, 4 + h : 5 + h]).astype(BF16)
        state = lax.dot_general(
            xin[:, h * 64 : (h + 1) * 64], wk, TN, preferred_element_type=F32
        )
        log = jnp.broadcast_to(last[h : h + 1], (8, BLOCK))
        high = log.astype(BF16).astype(F32)
        logs = jnp.concatenate([high, log - high], axis=0).astype(BF16)
        send_ref[BLOCK : BLOCK + 64, h * 128 : (h + 1) * 128] = state.astype(BF16)
        send_ref[BLOCK + 64 : KEPT, h * 128 : (h + 1) * 128] = logs
    for copy in moved:
        copy.wait()


def local_call(ids, rate, act, step, offset, conv_weight, buf):
    full = lambda *shape: pl.BlockSpec(shape, lambda i, ids, rate: (0,) * len(shape))
    return pl.pallas_call(
        local_kernel,
        grid_spec=pltpu.PrefetchScalarGridSpec(
            num_scalar_prefetch=2,
            grid=(1,),
            in_specs=[
                full(*act.shape),
                full(*step.shape),
                full(*offset.shape),
                pl.BlockSpec((CONV, 256), lambda i, ids, rate: (0, ids[1])),
                pl.BlockSpec((CONV, 128), lambda i, ids, rate: (0, 16 + ids[1])),
                pl.BlockSpec(memory_space=pl.ANY),
            ],
            out_specs=[
                full(SENT, 512), full(BLOCK, 256), full(BLOCK, 128), full(8, BLOCK),
                full(BLOCK, 8),
            ],
            scratch_shapes=[pltpu.VMEM((ROWS, 384), F32), pltpu.SemaphoreType.DMA((4,))],
        ),
        out_shape=(
            jax.ShapeDtypeStruct((SENT, 512), BF16),
            jax.ShapeDtypeStruct((BLOCK, 256), BF16),
            jax.ShapeDtypeStruct((BLOCK, 128), BF16),
            jax.ShapeDtypeStruct((8, BLOCK), F32),
            jax.ShapeDtypeStruct((BLOCK, 8), F32),
        ),
        compiler_params=vmem(),
        name="ssd_local",
    )(ids, rate, act, step, offset, conv_weight, conv_weight, buf)


def inner_kernel(
    ids, act_ref, cc_ref, xin_ref, bkey_ref, rows_ref, cols_ref,
    yin_ref, gate_ref, cq_ref, q_ref, wide_ref,
):
    gate_ref[...] = silu(added(act_ref, 0, 256)[HALO:].astype(F32))
    q_ref[...] = added(act_ref, 384, 256)[HALO:]
    wide_ref[...] = added(act_ref, 256, 128).astype(F32)
    cquery = convolved(wide_ref, cc_ref[...])
    cq_ref[...] = cquery
    lower = iota((BLOCK, BLOCK), 0) >= iota((BLOCK, BLOCK), 1)
    inner = lax.dot_general(cquery, bkey_ref[...], NT, preferred_element_type=F32)
    for h in range(4):
        spread = cols_ref[:, h : h + 1] - rows_ref[h : h + 1, :]
        decayed = jnp.exp(jnp.where(lower, spread, 0.0))
        mix = jnp.where(lower, inner * decayed * rows_ref[4 + h : 5 + h, :], 0.0).astype(BF16)
        yin_ref[:, h * 64 : (h + 1) * 64] = jnp.dot(
            mix, xin_ref[:, h * 64 : (h + 1) * 64], preferred_element_type=F32
        )


def inner_call(ids, act, conv_weight, xin, bkey, rows, cols):
    full = lambda *shape: pl.BlockSpec(shape, lambda i, ids: (0,) * len(shape))
    return pl.pallas_call(
        inner_kernel,
        grid_spec=pltpu.PrefetchScalarGridSpec(
            num_scalar_prefetch=1,
            grid=(1,),
            in_specs=[
                full(*act.shape),
                pl.BlockSpec((CONV, 128), lambda i, ids: (0, 24 + ids[1])),
                full(BLOCK, 256), full(BLOCK, 128), full(8, BLOCK), full(BLOCK, 8),
            ],
            out_specs=[full(BLOCK, 256), full(BLOCK, 256), full(BLOCK, 128), full(BLOCK, 256)],
            scratch_shapes=[pltpu.VMEM((BLOCK + HALO, 128), F32)],
        ),
        out_shape=(
            jax.ShapeDtypeStruct((BLOCK, 256), F32),
            jax.ShapeDtypeStruct((BLOCK, 256), F32),
            jax.ShapeDtypeStruct((BLOCK, 128), BF16),
            jax.ShapeDtypeStruct((BLOCK, 256), BF16),
        ),
        compiler_params=vmem(),
        name="ssd_inner",
    )(ids, act, conv_weight, xin, bkey, rows, cols)


SUB = 256
KEYS = 512
KEPT = BLOCK + 80
SENT = KEPT + 64
LOG2E = 1.4426950408889634


def attend_kernel(
    ids, bias, q_ref, yin_ref, gate_ref, cq_ref, cols_ref, gain_ref, all_hbm, a0, a1, a2, a3,
    out_ref, kv_ref, st_ref, wm_ref, wa_ref, acc_ref, late_ref, hold_ref, sems, ksems,
):
    block, tensor, mine = ids[0], ids[1], ids[2]
    per = KEYS // BLOCK
    count = all_hbm.shape[0]
    chunks = range(count // per - 1, -1, -1)
    last = block // per

    def move(chunk):
        picked = pl.ds(chunk * per, per)
        return pltpu.make_async_copy(
            all_hbm.at[picked, pl.ds(0, BLOCK)], kv_ref.at[picked], ksems.at[chunk]
        )

    states = pltpu.make_async_copy(all_hbm.at[:, pl.ds(BLOCK, 80)], st_ref, sems.at[0])
    weights = [pltpu.make_async_copy(all_hbm.at[:, pl.ds(KEPT, 64)], wm_ref, sems.at[1])]
    weights += [
        pltpu.make_async_copy(w, wa_ref.at[(mine + 4 - r) % 4], sems.at[2 + r])
        for r, w in enumerate((a0, a1, a2, a3))
    ]
    for chunk in chunks:
        pl.when((chunk <= last) & (chunk >= last - 1))(lambda chunk=chunk: move(chunk).start())
    acc_ref[...] = jnp.zeros_like(acc_ref)
    late_ref[...] = jnp.zeros_like(late_ref)
    hold_ref[...] = jnp.zeros_like(hold_ref)
    onward = (iota((2 * SUB, SUB), 0) % SUB > iota((2 * SUB, SUB), 1)).astype(BF16)

    def piece(chunk, masked):
        move(chunk).wait()
        if chunk > 1:
            move(chunk - 2).start()
        for h in range(2):
            late = late_ref[h]
            gained = acc_ref[h]
            query = q_ref[:, h * 128 : (h + 1) * 128]
            offset = bias[2 * tensor + h] * LOG2E
            for sub in range(KEYS // SUB - 1, -1, -1):
                at = chunk * KEYS + sub * SUB
                first = at // BLOCK
                key = kv_ref[first : first + 2, :, h * 128 : (h + 1) * 128]
                value = kv_ref[first : first + 2, :, 256 + h * 128 : 256 + (h + 1) * 128]
                logits = lax.dot_general(
                    query, key.reshape(SUB, 128), NT, preferred_element_type=F32
                )
                logits = logits * (128 ** -0.5 * LOG2E) + offset
                soft = jnp.maximum(logits, 0.0) + LOG2E * jnp.log(
                    1.0 + jnp.exp2(-jnp.abs(logits))
                )
                taken = logits - soft
                if masked:
                    before = at + iota((BLOCK, SUB), 1) < block * BLOCK + iota((BLOCK, SUB), 0)
                    soft = jnp.where(before, soft, 0.0)
                high = soft.astype(BF16)
                low = (soft - high.astype(F32)).astype(BF16)
                tail = jnp.dot(
                    jnp.concatenate([high, low], axis=1), onward, preferred_element_type=F32
                )
                later = jnp.concatenate([late] * (SUB // 128), axis=1)
                weight = jnp.exp2(taken - (tail + later))
                if masked:
                    weight = jnp.where(before, weight, 0.0)
                gained = gained + jnp.dot(
                    weight.astype(BF16), value.reshape(SUB, 128), preferred_element_type=F32
                )
                late = late + jnp.broadcast_to(tail[:, 0:1] + soft[:, 0:1], (BLOCK, 128))
            late_ref[h] = late
            acc_ref[h] = gained

    for chunk in chunks:
        if chunk == 1:
            states.start()
            for copy in weights:
                copy.start()
        pl.when(chunk == last)(lambda chunk=chunk: piece(chunk, True))
        pl.when(chunk < last)(lambda chunk=chunk: piece(chunk, False))

    states.wait()

    def advance(k, carry):
        logs = st_ref[k, 64:80, :].astype(F32)
        decay = jnp.exp(logs[0:8] + logs[8:16])
        hold_ref[...] = hold_ref[...] * jnp.concatenate([decay] * 8, axis=0) + st_ref[
            k, 0:64, :
        ].astype(F32)
        return carry

    lax.fori_loop(0, block, advance, 0)
    cquery = cq_ref[...]
    ys = []
    for h in range(4):
        enter = hold_ref[:, h * 128 : (h + 1) * 128].astype(BF16)
        moved = lax.dot_general(cquery, enter, NT, preferred_element_type=F32)
        ys.append(moved * jnp.exp(cols_ref[:, h : h + 1]))
    gated = (yin_ref[...] + jnp.concatenate(ys, axis=1)) * gate_ref[...]
    scale = lax.rsqrt(jnp.mean(gated * gated, axis=-1, keepdims=True) + EPS)
    mixed = (gated * scale * gain_ref[...]).astype(BF16)
    attended = jnp.concatenate([acc_ref[0].astype(BF16), acc_ref[1].astype(BF16)], axis=1)
    for copy in weights:
        copy.wait()
    for s in range(count):
        halves = []
        for f in range(4):
            for half in range(2):
                halves.append(
                    wm_ref[s, 16 * f : 16 * (f + 1), 256 * half : 256 * (half + 1)]
                )
        rows_m = jnp.concatenate(halves, axis=0)
        rows_a = jnp.concatenate(
            [wa_ref[f, 32 * s : 32 * (s + 1), :] for f in range(4)], axis=0
        )
        out_ref[:, 128 * s : 128 * (s + 1)] = (
            lax.dot_general(mixed, rows_m, NT, preferred_element_type=F32)
            + lax.dot_general(attended, rows_a, NT, preferred_element_type=F32)
        ).astype(BF16)


def attend_call(ids, bias, q, yin, gate, cq, cols, gain, gathered, rows):
    full = lambda *shape: pl.BlockSpec(shape, lambda i, ids, bias: (0,) * len(shape))
    count = gathered.shape[0]
    hbm = pl.BlockSpec(memory_space=pl.ANY)
    return pl.pallas_call(
        attend_kernel,
        grid_spec=pltpu.PrefetchScalarGridSpec(
            num_scalar_prefetch=2,
            grid=(1,),
            in_specs=[
                full(BLOCK, 256), full(BLOCK, 256), full(BLOCK, 256), full(BLOCK, 128),
                full(BLOCK, 8), pl.BlockSpec((1, 256), lambda i, ids, bias: (0, ids[1])),
                pl.BlockSpec(memory_space=pltpu.HBM), hbm, hbm, hbm, hbm,
            ],
            out_specs=full(BLOCK, 2048),
            scratch_shapes=[
                pltpu.VMEM((count, BLOCK, 512), BF16),
                pltpu.VMEM((count, 80, 512), BF16),
                pltpu.VMEM((count, 64, 512), BF16),
                pltpu.VMEM((4, 512, 256), BF16),
                pltpu.VMEM((2, BLOCK, 128), F32),
                pltpu.VMEM((2, BLOCK, 128), F32),
                pltpu.VMEM((64, 512), F32),
                pltpu.SemaphoreType.DMA((6,)),
                pltpu.SemaphoreType.DMA((count * BLOCK // KEYS,)),
            ],
        ),
        out_shape=jax.ShapeDtypeStruct((BLOCK, 2048), BF16),
        compiler_params=vmem(),
        name="attend",
    )(ids, bias, q, yin, gate, cq, cols, gain.reshape(1, -1), gathered, *rows)


def rotated(shard, axis, by):
    length = lax.axis_size(axis)
    return lax.ppermute(shard, axis, [(i, (i + by) % length) for i in range(length)])


def body(
    inputs, norm_gain, w_gate, w_input, w_bkey, w_cquery, w_step, conv_weight, decay_rate,
    decay_offset, ssd_gain, w_query, w_key, w_value, stick_bias, out_mixer, out_attend,
):
    length = lax.axis_size("sp")
    ids = jnp.stack([lax.axis_index(name) for name in ("sp", "tp", "fs")]).astype(jnp.int32)
    split, step, first, second = prep_call(
        inputs, norm_gain, w_step.T, w_key, w_value, w_input, w_bkey, w_gate, w_cquery, w_query,
        out_attend.T, out_mixer.T,
    )
    tokens = lax.all_to_all(split, "fs", 0, 0, tiled=True)
    early = lax.all_gather(first, "sp", axis=0, tiled=True)
    tokens, early = lax.optimization_barrier((tokens, early))
    rim = lax.ppermute(
        tokens[:, BLOCK - HALO : BLOCK], "sp", [(i, i + 1) for i in range(length - 1)]
    )

    def projected(whole, width):
        act, *kept = project_call(tokens, rim, whole, width)
        return lax.all_to_all(act, "fs", 0, 0, tiled=True), *kept

    (act,) = projected(early, 896)
    send, xin, bkey, srows, scols = local_call(
        ids, decay_rate, act, step, decay_offset[0].T, conv_weight, tokens
    )
    gathered = lax.all_gather(send, "sp", axis=0)
    act, kept = projected(lax.all_gather(second, "sp", axis=0, tiled=True), 640)
    rows = [kept] + [rotated(kept, "fs", by) for by in (1, 2, 3)]
    yin, gate, cq, q = inner_call(ids, act, conv_weight, xin, bkey, srows, scols)
    partial = attend_call(ids, stick_bias, q, yin, gate, cq, scols, ssd_gain, gathered, rows)
    parts = lax.all_to_all(partial.reshape(8, 16, 2048), "tp", 0, 0, tiled=True)
    return jnp.sum(parts.astype(F32), axis=0).astype(BF16)[None]


def solution(mesh):
    shard = P(("sp", "fs"), "tp")
    return jax.shard_map(
        body,
        mesh=mesh,
        in_specs=(
            P("fs", "sp", None), P(), shard, shard, shard, shard, P(), P(), P(),
            P("fs", "sp", "tp"), P(), shard, shard, shard, P(),
            P("tp", ("sp", "fs")), P("tp", ("sp", "fs")),
        ),
        out_specs=P("fs", ("sp", "tp"), None),
        check_vma=False,
    )
```

```python
import jax
import jax.numpy as jnp
from jax import lax
from jax.experimental import pallas as pl
from jax.experimental.pallas import tpu as pltpu
from jax.sharding import PartitionSpec as P

BLOCK = 128
CONV = 4
EPS = 1e-06
HALO = 16
ROWS = BLOCK + HALO
F32 = jnp.float32
BF16 = jnp.bfloat16
HIGH = lax.Precision.HIGHEST
NT = (((1,), (1,)), ((), ()))
TN = (((0,), (0,)), ((), ()))


def vmem(limit=48):
    return pltpu.CompilerParams(vmem_limit_bytes=limit * 1024 * 1024)


def iota(shape, dim):
    return lax.broadcasted_iota(jnp.int32, shape, dim)


def softplus(x):
    return jnp.maximum(x, 0.0) + jnp.log1p(jnp.exp(-jnp.abs(x)))


def silu(x):
    return x / (1.0 + jnp.exp(-x))


def pull(pairs, sems):
    copies = [pltpu.make_async_copy(src, dst, sems.at[i]) for i, (src, dst) in enumerate(pairs)]
    for copy in copies:
        copy.start()
    return copies


def shuffled(normed, f, g):
    lane = iota((normed.shape[0], 128), 1) // 32
    out = None
    for k in range(4):
        at = (4 * g + k) * 128
        piece = pltpu.roll(normed[:, at : at + 128], (k + 4 - f) * 32 % 128, 1)
        out = piece if out is None else jnp.where(lane == k, piece, out)
    return out.astype(BF16)


def normalised(x, gain):
    wide = x.astype(F32)
    scale = lax.rsqrt(jnp.mean(wide * wide, axis=-1, keepdims=True) + EPS)
    return (wide * scale * gain).astype(BF16)


def prep_kernel(*refs):
    x_hbm, gain_hbm, ws_hbm = refs[:3]
    sources = refs[3:12]
    xs_ref, step_ref, first_ref, second_ref = refs[12:16]
    x_ref, gain_ref, ws_ref, third_ref, wide_ref, sems, wsems = refs[16:]
    early = pull(((x_hbm.at[0], x_ref), (gain_hbm, gain_ref), (ws_hbm, ws_ref)), sems)
    pairs = []
    outs = (first_ref, second_ref, third_ref)
    at, which = 0, 0
    for n, src in enumerate(sources):
        if n in (4, 8):
            at, which = 0, which + 1
        pairs.append((src, outs[which].at[:, pl.ds(at, src.shape[1])]))
        at += src.shape[1]
    later = pull(pairs, wsems)
    for copy in early:
        copy.wait()
    normed = normalised(x_ref[...], gain_ref[...])
    step_ref[...] = softplus(
        lax.dot_general(ws_ref[...], normed, NT, preferred_element_type=F32)
    )
    wide = normed.astype(F32)
    wide_ref[...] = wide

    def each(f, carry):
        for g in range(4):
            xs_ref[f, 0:BLOCK, g * 128 : (g + 1) * 128] = shuffled(wide_ref, f, g)
        return carry

    lax.fori_loop(0, 4, each, 0)
    for copy in later:
        copy.wait()
    for f in range(4):
        xs_ref[f, BLOCK:, 0:256] = third_ref[0:16, :]
        xs_ref[f, BLOCK:, 256:512] = third_ref[16:32, :]


def prep_call(inputs, gain, w_step_t, *arrays):
    rows, width = inputs.shape[1:]
    heads = w_step_t.shape[0]
    part = arrays[0].shape[0]
    widths = [sum(a.shape[1] for a in group) for group in (arrays[:4], arrays[4:8], arrays[8:])]
    hbm = pl.BlockSpec(memory_space=pltpu.HBM)
    return pl.pallas_call(
        prep_kernel,
        in_specs=[hbm] * 12,
        out_shape=(
            jax.ShapeDtypeStruct((4, rows + HALO, width // 4), BF16),
            jax.ShapeDtypeStruct((heads, rows), F32),
            jax.ShapeDtypeStruct((part, widths[0]), BF16),
            jax.ShapeDtypeStruct((part, widths[1]), BF16),
        ),
        scratch_shapes=[
            pltpu.VMEM((rows, width), BF16),
            pltpu.VMEM((1, width), F32),
            pltpu.VMEM((heads, width), BF16),
            pltpu.VMEM((part, widths[2]), BF16),
            pltpu.VMEM((rows, width), F32),
            pltpu.SemaphoreType.DMA((3,)),
            pltpu.SemaphoreType.DMA((9,)),
        ],
        name="prep",
    )(inputs, gain.reshape(1, -1), w_step_t, *arrays)


def project_kernel(x_ref, rim_ref, w_ref, out_hbm, *rest):
    kept, (out_ref, sems) = rest[:-2], rest[-2:]
    width = out_hbm.shape[2]
    weights = w_ref[:, 0:width]

    def copy(f):
        return pltpu.make_async_copy(out_ref.at[f], out_hbm.at[f], sems.at[f])

    def each(f, carry):
        rows = jnp.concatenate([rim_ref[f], x_ref[f, 0:BLOCK, :]], axis=0)
        out_ref[f] = jnp.dot(rows, weights, preferred_element_type=F32).astype(BF16)
        copy(f).start()
        return carry

    lax.fori_loop(0, 4, each, 0)
    for ref in kept:
        ref[...] = w_ref[:, width:]
    for f in range(4):
        copy(f).wait()


def project_call(x, rim, w, width):
    whole = pl.BlockSpec(memory_space=pltpu.VMEM)
    outs = [jax.ShapeDtypeStruct((4, ROWS, width), BF16)]
    specs = [pl.BlockSpec(memory_space=pltpu.HBM)]
    if w.shape[1] > width:
        outs.append(jax.ShapeDtypeStruct((w.shape[0], w.shape[1] - width), BF16))
        specs.append(whole)
    return pl.pallas_call(
        project_kernel,
        in_specs=[whole] * 3,
        out_specs=specs,
        out_shape=outs,
        scratch_shapes=[pltpu.VMEM((4, ROWS, width), BF16), pltpu.SemaphoreType.DMA((4,))],
        compiler_params=vmem(),
        name="project",
    )(x, rim, w)


def added(ref, at, width):
    total = ref[0, :, at : at + width].astype(F32)
    for j in range(1, 4):
        total = total + ref[j, :, at : at + width].astype(F32)
    return total.astype(BF16)


def convolved(wide_ref, taps):
    summed = None
    for i in range(CONV):
        at = HALO - CONV + 1 + i
        part = taps[i : i + 1] * wide_ref[at : at + BLOCK, :]
        summed = part if summed is None else summed + part
    return silu(summed).astype(BF16)


def local_kernel(
    ids, rate, act_ref, step_ref, off_ref, ci_ref, cb_ref, buf_ref,
    send_ref, xin_ref, bkey_ref, rows_ref, cols_ref, wide_ref, sems,
):
    tensor = ids[1]
    moved = pull(
        [
            (buf_ref.at[f, pl.ds(BLOCK, HALO)], send_ref.at[pl.ds(KEPT + HALO * f, HALO)])
            for f in range(4)
        ],
        sems,
    )
    send_ref[0:BLOCK, :] = added(act_ref, 0, 512)[HALO:]
    wide_ref[...] = added(act_ref, 512, 384).astype(F32)
    conv = convolved(wide_ref, jnp.concatenate([ci_ref[...], cb_ref[...]], axis=1))
    xin, bkey = conv[:, 0:256], conv[:, 256:384]
    xin_ref[...] = xin
    bkey_ref[...] = bkey
    row = iota((BLOCK, BLOCK), 0)
    col = iota((BLOCK, BLOCK), 1)
    step = jnp.concatenate([step_ref[pl.ds(4 * tensor + h, 1), :] for h in range(4)], axis=0)
    rates = jnp.concatenate(
        [jnp.full((1, BLOCK), rate[4 * tensor + h], F32) for h in range(4)], axis=0
    )
    decay = off_ref[...] - rates * step
    decay8 = jnp.concatenate([decay, jnp.zeros((4, BLOCK), F32)], axis=0)
    upper = (row <= col).astype(F32)
    cum = jnp.dot(decay8, upper, precision=HIGH, preferred_element_type=F32)
    last = jnp.sum(decay, axis=1, keepdims=True)
    to_end = jnp.exp(last - cum[0:4]) * step
    eye = (row == col).astype(F32)
    cols = lax.dot_general(
        eye, jnp.concatenate([cum[0:4], to_end], axis=0), NT, precision=HIGH,
        preferred_element_type=F32,
    )
    rows_ref[...] = jnp.concatenate([cum[0:4], step], axis=0)
    cols_ref[...] = cols
    wide_key = bkey.astype(F32)
    for h in range(4):
        wk = (wide_key * cols[:, 4 + h : 5 + h]).astype(BF16)
        state = lax.dot_general(
            xin[:, h * 64 : (h + 1) * 64], wk, TN, preferred_element_type=F32
        )
        log = jnp.broadcast_to(last[h : h + 1], (8, BLOCK))
        high = log.astype(BF16).astype(F32)
        logs = jnp.concatenate([high, log - high], axis=0).astype(BF16)
        send_ref[BLOCK : BLOCK + 64, h * 128 : (h + 1) * 128] = state.astype(BF16)
        send_ref[BLOCK + 64 : KEPT, h * 128 : (h + 1) * 128] = logs
    for copy in moved:
        copy.wait()


def local_call(ids, rate, act, step, offset, conv_weight, buf):
    full = lambda *shape: pl.BlockSpec(shape, lambda i, ids, rate: (0,) * len(shape))
    return pl.pallas_call(
        local_kernel,
        grid_spec=pltpu.PrefetchScalarGridSpec(
            num_scalar_prefetch=2,
            grid=(1,),
            in_specs=[
                full(*act.shape),
                full(*step.shape),
                full(*offset.shape),
                pl.BlockSpec((CONV, 256), lambda i, ids, rate: (0, ids[1])),
                pl.BlockSpec((CONV, 128), lambda i, ids, rate: (0, 16 + ids[1])),
                pl.BlockSpec(memory_space=pl.ANY),
            ],
            out_specs=[
                full(SENT, 512), full(BLOCK, 256), full(BLOCK, 128), full(8, BLOCK),
                full(BLOCK, 8),
            ],
            scratch_shapes=[pltpu.VMEM((ROWS, 384), F32), pltpu.SemaphoreType.DMA((4,))],
        ),
        out_shape=(
            jax.ShapeDtypeStruct((SENT, 512), BF16),
            jax.ShapeDtypeStruct((BLOCK, 256), BF16),
            jax.ShapeDtypeStruct((BLOCK, 128), BF16),
            jax.ShapeDtypeStruct((8, BLOCK), F32),
            jax.ShapeDtypeStruct((BLOCK, 8), F32),
        ),
        compiler_params=vmem(),
        name="ssd_local",
    )(ids, rate, act, step, offset, conv_weight, conv_weight, buf)


def inner_kernel(
    ids, act_ref, cc_ref, xin_ref, bkey_ref, rows_ref, cols_ref,
    yin_ref, gate_ref, cq_ref, q_ref, wide_ref,
):
    gate_ref[...] = silu(added(act_ref, 0, 256)[HALO:].astype(F32))
    q_ref[...] = added(act_ref, 384, 256)[HALO:]
    wide_ref[...] = added(act_ref, 256, 128).astype(F32)
    cquery = convolved(wide_ref, cc_ref[...])
    cq_ref[...] = cquery
    lower = iota((BLOCK, BLOCK), 0) >= iota((BLOCK, BLOCK), 1)
    inner = lax.dot_general(cquery, bkey_ref[...], NT, preferred_element_type=F32)
    for h in range(4):
        spread = cols_ref[:, h : h + 1] - rows_ref[h : h + 1, :]
        decayed = jnp.exp(jnp.where(lower, spread, 0.0))
        mix = jnp.where(lower, inner * decayed * rows_ref[4 + h : 5 + h, :], 0.0).astype(BF16)
        yin_ref[:, h * 64 : (h + 1) * 64] = jnp.dot(
            mix, xin_ref[:, h * 64 : (h + 1) * 64], preferred_element_type=F32
        )


def inner_call(ids, act, conv_weight, xin, bkey, rows, cols):
    full = lambda *shape: pl.BlockSpec(shape, lambda i, ids: (0,) * len(shape))
    return pl.pallas_call(
        inner_kernel,
        grid_spec=pltpu.PrefetchScalarGridSpec(
            num_scalar_prefetch=1,
            grid=(1,),
            in_specs=[
                full(*act.shape),
                pl.BlockSpec((CONV, 128), lambda i, ids: (0, 24 + ids[1])),
                full(BLOCK, 256), full(BLOCK, 128), full(8, BLOCK), full(BLOCK, 8),
            ],
            out_specs=[full(BLOCK, 256), full(BLOCK, 256), full(BLOCK, 128), full(BLOCK, 256)],
            scratch_shapes=[pltpu.VMEM((BLOCK + HALO, 128), F32)],
        ),
        out_shape=(
            jax.ShapeDtypeStruct((BLOCK, 256), F32),
            jax.ShapeDtypeStruct((BLOCK, 256), F32),
            jax.ShapeDtypeStruct((BLOCK, 128), BF16),
            jax.ShapeDtypeStruct((BLOCK, 256), BF16),
        ),
        compiler_params=vmem(),
        name="ssd_inner",
    )(ids, act, conv_weight, xin, bkey, rows, cols)


SUB = 256
KEYS = 512
KEPT = BLOCK + 80
SENT = KEPT + 64
LOG2E = 1.4426950408889634


def attend_kernel(
    ids, bias, q_ref, yin_ref, gate_ref, cq_ref, cols_ref, gain_ref, all_hbm, a0, a1, a2, a3,
    out_ref, kv_ref, st_ref, wm_ref, wa_ref, acc_ref, late_ref, hold_ref, sems, ksems,
):
    block, tensor, mine = ids[0], ids[1], ids[2]
    per = KEYS // BLOCK
    count = all_hbm.shape[0]
    chunks = range(count // per - 1, -1, -1)
    last = block // per

    def move(chunk):
        picked = pl.ds(chunk * per, per)
        return pltpu.make_async_copy(
            all_hbm.at[picked, pl.ds(0, BLOCK)], kv_ref.at[picked], ksems.at[chunk]
        )

    states = pltpu.make_async_copy(all_hbm.at[:, pl.ds(BLOCK, 80)], st_ref, sems.at[0])
    weights = [pltpu.make_async_copy(all_hbm.at[:, pl.ds(KEPT, 64)], wm_ref, sems.at[1])]
    weights += [
        pltpu.make_async_copy(w, wa_ref.at[(mine + 4 - r) % 4], sems.at[2 + r])
        for r, w in enumerate((a0, a1, a2, a3))
    ]
    for chunk in chunks:
        pl.when((chunk <= last) & (chunk >= last - 1))(lambda chunk=chunk: move(chunk).start())
    acc_ref[...] = jnp.zeros_like(acc_ref)
    late_ref[...] = jnp.zeros_like(late_ref)
    hold_ref[...] = jnp.zeros_like(hold_ref)
    onward = (iota((2 * SUB, SUB), 0) % SUB > iota((2 * SUB, SUB), 1)).astype(BF16)

    def piece(turn, carry):
        chunk = last - turn
        move(chunk).wait()
        pl.when(chunk > 1)(lambda: move(chunk - 2).start())

        @pl.when(turn == jnp.minimum(last, 1))
        def _():
            states.start()
            for copy in weights:
                copy.start()

        for h in range(2):
            late = late_ref[h]
            gained = acc_ref[h]
            query = q_ref[:, h * 128 : (h + 1) * 128]
            offset = bias[2 * tensor + h] * LOG2E
            for sub in range(KEYS // SUB - 1, -1, -1):
                at = chunk * KEYS + sub * SUB
                picked = pl.ds(chunk * per + sub * (SUB // BLOCK), SUB // BLOCK)
                key = kv_ref[picked, :, h * 128 : (h + 1) * 128]
                value = kv_ref[picked, :, 256 + h * 128 : 256 + (h + 1) * 128]
                logits = lax.dot_general(
                    query, key.reshape(SUB, 128), NT, preferred_element_type=F32
                )
                logits = logits * (128 ** -0.5 * LOG2E) + offset
                soft = jnp.maximum(logits, 0.0) + LOG2E * jnp.log(
                    1.0 + jnp.exp2(-jnp.abs(logits))
                )
                taken = logits - soft
                before = at + iota((BLOCK, SUB), 1) < block * BLOCK + iota((BLOCK, SUB), 0)
                soft = jnp.where(before, soft, 0.0)
                high = soft.astype(BF16)
                low = (soft - high.astype(F32)).astype(BF16)
                tail = jnp.dot(
                    jnp.concatenate([high, low], axis=1), onward, preferred_element_type=F32
                )
                later = jnp.concatenate([late] * (SUB // 128), axis=1)
                weight = jnp.where(before, jnp.exp2(taken - (tail + later)), 0.0)
                gained = gained + jnp.dot(
                    weight.astype(BF16), value.reshape(SUB, 128), preferred_element_type=F32
                )
                late = late + jnp.broadcast_to(tail[:, 0:1] + soft[:, 0:1], (BLOCK, 128))
            late_ref[h] = late
            acc_ref[h] = gained
        return carry

    lax.fori_loop(0, last + 1, piece, 0)
    states.wait()

    def advance(k, carry):
        logs = st_ref[k, 64:80, :].astype(F32)
        decay = jnp.exp(logs[0:8] + logs[8:16])
        hold_ref[...] = hold_ref[...] * jnp.concatenate([decay] * 8, axis=0) + st_ref[
            k, 0:64, :
        ].astype(F32)
        return carry

    lax.fori_loop(0, block, advance, 0)
    cquery = cq_ref[...]
    ys = []
    for h in range(4):
        enter = hold_ref[:, h * 128 : (h + 1) * 128].astype(BF16)
        moved = lax.dot_general(cquery, enter, NT, preferred_element_type=F32)
        ys.append(moved * jnp.exp(cols_ref[:, h : h + 1]))
    gated = (yin_ref[...] + jnp.concatenate(ys, axis=1)) * gate_ref[...]
    scale = lax.rsqrt(jnp.mean(gated * gated, axis=-1, keepdims=True) + EPS)
    mixed = (gated * scale * gain_ref[...]).astype(BF16)
    attended = jnp.concatenate([acc_ref[0].astype(BF16), acc_ref[1].astype(BF16)], axis=1)
    for copy in weights:
        copy.wait()
    for s in range(count):
        halves = []
        for f in range(4):
            for half in range(2):
                halves.append(
                    wm_ref[s, 16 * f : 16 * (f + 1), 256 * half : 256 * (half + 1)]
                )
        rows_m = jnp.concatenate(halves, axis=0)
        rows_a = jnp.concatenate(
            [wa_ref[f, 32 * s : 32 * (s + 1), :] for f in range(4)], axis=0
        )
        out_ref[:, 128 * s : 128 * (s + 1)] = (
            lax.dot_general(mixed, rows_m, NT, preferred_element_type=F32)
            + lax.dot_general(attended, rows_a, NT, preferred_element_type=F32)
        ).astype(BF16)


def attend_call(ids, bias, q, yin, gate, cq, cols, gain, gathered, rows):
    full = lambda *shape: pl.BlockSpec(shape, lambda i, ids, bias: (0,) * len(shape))
    count = gathered.shape[0]
    hbm = pl.BlockSpec(memory_space=pl.ANY)
    return pl.pallas_call(
        attend_kernel,
        grid_spec=pltpu.PrefetchScalarGridSpec(
            num_scalar_prefetch=2,
            grid=(1,),
            in_specs=[
                full(BLOCK, 256), full(BLOCK, 256), full(BLOCK, 256), full(BLOCK, 128),
                full(BLOCK, 8), pl.BlockSpec((1, 256), lambda i, ids, bias: (0, ids[1])),
                pl.BlockSpec(memory_space=pltpu.HBM), hbm, hbm, hbm, hbm,
            ],
            out_specs=full(BLOCK, 2048),
            scratch_shapes=[
                pltpu.VMEM((count, BLOCK, 512), BF16),
                pltpu.VMEM((count, 80, 512), BF16),
                pltpu.VMEM((count, 64, 512), BF16),
                pltpu.VMEM((4, 512, 256), BF16),
                pltpu.VMEM((2, BLOCK, 128), F32),
                pltpu.VMEM((2, BLOCK, 128), F32),
                pltpu.VMEM((64, 512), F32),
                pltpu.SemaphoreType.DMA((6,)),
                pltpu.SemaphoreType.DMA((count * BLOCK // KEYS,)),
            ],
        ),
        out_shape=jax.ShapeDtypeStruct((BLOCK, 2048), BF16),
        compiler_params=vmem(),
        name="attend",
    )(ids, bias, q, yin, gate, cq, cols, gain.reshape(1, -1), gathered, *rows)


def rotated(shard, axis, by):
    length = lax.axis_size(axis)
    return lax.ppermute(shard, axis, [(i, (i + by) % length) for i in range(length)])


def body(
    inputs, norm_gain, w_gate, w_input, w_bkey, w_cquery, w_step, conv_weight, decay_rate,
    decay_offset, ssd_gain, w_query, w_key, w_value, stick_bias, out_mixer, out_attend,
):
    length = lax.axis_size("sp")
    ids = jnp.stack([lax.axis_index(name) for name in ("sp", "tp", "fs")]).astype(jnp.int32)
    split, step, first, second = prep_call(
        inputs, norm_gain, w_step.T, w_key, w_value, w_input, w_bkey, w_gate, w_cquery, w_query,
        out_attend.T, out_mixer.T,
    )
    tokens = lax.all_to_all(split, "fs", 0, 0, tiled=True)
    early = lax.all_gather(first, "sp", axis=0, tiled=True)
    tokens, early = lax.optimization_barrier((tokens, early))
    rim = lax.ppermute(
        tokens[:, BLOCK - HALO : BLOCK], "sp", [(i, i + 1) for i in range(length - 1)]
    )

    def projected(whole, width):
        act, *kept = project_call(tokens, rim, whole, width)
        return lax.all_to_all(act, "fs", 0, 0, tiled=True), *kept

    (act,) = projected(early, 896)
    send, xin, bkey, srows, scols = local_call(
        ids, decay_rate, act, step, decay_offset[0].T, conv_weight, tokens
    )
    gathered = lax.all_gather(send, "sp", axis=0)
    act, kept = projected(lax.all_gather(second, "sp", axis=0, tiled=True), 640)
    rows = [kept] + [rotated(kept, "fs", by) for by in (1, 2, 3)]
    yin, gate, cq, q = inner_call(ids, act, conv_weight, xin, bkey, srows, scols)
    partial = attend_call(ids, stick_bias, q, yin, gate, cq, scols, ssd_gain, gathered, rows)
    parts = lax.all_to_all(partial.reshape(8, 16, 2048), "tp", 0, 0, tiled=True)
    return jnp.sum(parts.astype(F32), axis=0).astype(BF16)[None]


def solution(mesh):
    shard = P(("sp", "fs"), "tp")
    return jax.shard_map(
        body,
        mesh=mesh,
        in_specs=(
            P("fs", "sp", None), P(), shard, shard, shard, shard, P(), P(), P(),
            P("fs", "sp", "tp"), P(), shard, shard, shard, P(),
            P("tp", ("sp", "fs")), P("tp", ("sp", "fs")),
        ),
        out_specs=P("fs", ("sp", "tp"), None),
        check_vma=False,
    )
```

```python
import jax
import jax.numpy as jnp
from jax import lax
from jax.experimental import pallas as pl
from jax.experimental.pallas import tpu as pltpu
from jax.sharding import PartitionSpec as P

BLOCK = 128
CONV = 4
EPS = 1e-06
HALO = 16
ROWS = BLOCK + HALO
F32 = jnp.float32
BF16 = jnp.bfloat16
HIGH = lax.Precision.HIGHEST
NT = (((1,), (1,)), ((), ()))
TN = (((0,), (0,)), ((), ()))


def vmem(limit=48):
    return pltpu.CompilerParams(vmem_limit_bytes=limit * 1024 * 1024)


def iota(shape, dim):
    return lax.broadcasted_iota(jnp.int32, shape, dim)


def softplus(x):
    return jnp.maximum(x, 0.0) + jnp.log1p(jnp.exp(-jnp.abs(x)))


def silu(x):
    return x / (1.0 + jnp.exp(-x))


def pull(pairs, sems):
    copies = [pltpu.make_async_copy(src, dst, sems.at[i]) for i, (src, dst) in enumerate(pairs)]
    for copy in copies:
        copy.start()
    return copies


def normalised(x, gain):
    wide = x.astype(F32)
    scale = lax.rsqrt(jnp.mean(wide * wide, axis=-1, keepdims=True) + EPS)
    return (wide * scale * gain).astype(BF16)


def turned(tile, by):
    return pltpu.roll(tile, by % 128, 1) if by % 128 else tile


def prep_kernel(*refs):
    x_hbm, gain_hbm, ws_hbm = refs[:3]
    sources = refs[3:12]
    xs_ref, step_ref, cut_ref = refs[12:15]
    x_ref, gain_ref, ws_ref, all_ref, sems, wsems = refs[15:]
    early = pull(((x_hbm.at[0], x_ref), (gain_hbm, gain_ref), (ws_hbm, ws_ref)), sems)
    pairs, starts, at = [], [], 0
    for src in sources:
        pairs.append((src, all_ref.at[:, pl.ds(at, src.shape[1])]))
        starts.append(at)
        at += src.shape[1]
    later = pull(pairs, wsems)
    for copy in early:
        copy.wait()
    normed = normalised(x_ref[...], gain_ref[...])
    xs_ref[HALO:, :] = normed
    step_ref[...] = softplus(
        lax.dot_general(ws_ref[...], normed, NT, preferred_element_type=F32)
    )
    for copy in later:
        copy.wait()
    rows = all_ref.shape[0]
    lane = iota((rows, 128), 1)
    key, value, entry, gate, query, bkey, cquery, outs = starts[:8]

    def tile(at):
        return all_ref[:, at : at + 128].astype(F32)

    for f in range(4):
        side, half = 64 * (f % 2), 128 * (f // 2)
        pair = lambda a, b: jnp.where(
            lane < 64, turned(tile(a + half), -side), turned(tile(b + half), 64 - side)
        ).astype(BF16)
        cut_ref[f, :, 0:128] = pair(key, value)
        cut_ref[f, :, 128:256] = jnp.where(
            lane < 64, turned(tile(entry + half), -side), turned(tile(bkey), 64 - 32 * f)
        ).astype(BF16)
        cut_ref[f, :, 256:384] = pair(gate, query)
        cut_ref[f, :, 384:512] = turned(tile(cquery), -32 * f).astype(BF16)
        cut_ref[f, :, 512:] = all_ref[:, outs : outs + 512]


def prep_call(inputs, gain, w_step_t, *arrays):
    rows, width = inputs.shape[1:]
    heads = w_step_t.shape[0]
    part = arrays[0].shape[0]
    hbm = pl.BlockSpec(memory_space=pltpu.HBM)
    return pl.pallas_call(
        prep_kernel,
        in_specs=[hbm] * 12,
        out_shape=(
            jax.ShapeDtypeStruct((rows + HALO, width), BF16),
            jax.ShapeDtypeStruct((heads, rows), F32),
            jax.ShapeDtypeStruct((4, part, 1024), BF16),
        ),
        scratch_shapes=[
            pltpu.VMEM((rows, width), BF16),
            pltpu.VMEM((1, width), F32),
            pltpu.VMEM((heads, width), BF16),
            pltpu.VMEM((part, sum(a.shape[1] for a in arrays)), BF16),
            pltpu.SemaphoreType.DMA((3,)),
            pltpu.SemaphoreType.DMA((9,)),
        ],
        name="prep",
    )(inputs, gain.reshape(1, -1), w_step_t, *arrays)


def halo_kernel(xs_in, halo_ref, gain_ref, xs_out, rim_ref, sem):
    rim_ref[...] = normalised(halo_ref[...], gain_ref[...])
    copy = pltpu.make_async_copy(rim_ref, xs_out.at[pl.ds(0, HALO)], sem)
    copy.start()
    copy.wait()


def halo_call(xs, halo, gain):
    anywhere = pl.BlockSpec(memory_space=pl.ANY)
    whole = pl.BlockSpec(memory_space=pltpu.VMEM)
    return pl.pallas_call(
        halo_kernel,
        in_specs=[anywhere, whole, whole],
        out_specs=anywhere,
        out_shape=jax.ShapeDtypeStruct(xs.shape, BF16),
        input_output_aliases={0: 0},
        scratch_shapes=[pltpu.VMEM((HALO, xs.shape[1]), BF16), pltpu.SemaphoreType.DMA],
        name="halo",
    )(xs, halo, gain.reshape(1, -1))


def project_kernel(x_ref, w_ref, out_ref):
    act = jnp.dot(x_ref[0], w_ref[...], preferred_element_type=F32).astype(BF16)
    width = act.shape[1]
    out_ref[0, :, 0:width] = act
    out_ref[0, :, width:] = jnp.zeros((act.shape[0], out_ref.shape[2] - width), BF16)


def project_call(x, w):
    count, rows, depth = x.shape
    return pl.pallas_call(
        project_kernel,
        grid=(count,),
        in_specs=[
            pl.BlockSpec((1, rows, depth), lambda i: (i, 0, 0)),
            pl.BlockSpec(w.shape, lambda i: (0, 0)),
        ],
        out_specs=pl.BlockSpec((1, rows, 256), lambda i: (i, 0, 0)),
        out_shape=jax.ShapeDtypeStruct((count, rows, 256), BF16),
        name="project",
    )(x, w)


def joined(ref, rows, swap):
    lane = iota((rows, 128), 1) < 64
    tiles = []
    for j in range(2):
        left = ref[2 * j, ref.shape[1] - rows :, 0:128].astype(F32)
        right = ref[2 * j + 1, ref.shape[1] - rows :, 0:128].astype(F32)
        if swap:
            tiles.append(jnp.where(lane, turned(left, 64), right))
        else:
            tiles.append(jnp.where(lane, left, turned(right, 64)))
    return tiles


def quarters(ref, at):
    lane = iota((ROWS, 128), 1) // 32
    out = None
    for f in range(4):
        tile = turned(ref[f, :, 128:256].astype(F32), 32 * f - at)
        out = tile if out is None else jnp.where(lane == f, tile, out)
    return out


def convolved(wide_ref, taps):
    summed = None
    for i in range(CONV):
        at = HALO - CONV + 1 + i
        part = taps[i : i + 1] * wide_ref[at : at + BLOCK, :]
        summed = part if summed is None else summed + part
    return silu(summed).astype(BF16)


def local_kernel(
    ids, rate, act_ref, step_ref, off_ref, ci_ref, cb_ref, buf_ref,
    send_ref, xin_ref, bkey_ref, rows_ref, cols_ref, wide_ref, sems,
):
    tensor = ids[1]
    moved = pull(
        [
            (buf_ref.at[f, :, pl.ds(512, 512)], send_ref.at[pl.ds(KEPT + 32 * f, 32)])
            for f in range(4)
        ],
        sems,
    )
    keys = joined(act_ref, BLOCK, False) + joined(act_ref, BLOCK, True)
    send_ref[0:BLOCK, :] = jnp.concatenate(keys, axis=1).astype(BF16)
    entry = [act_ref[f, :, 128:256].astype(F32) for f in range(4)]
    left = iota((ROWS, 128), 1) < 64
    wide_ref[:, 0:128] = jnp.where(left, entry[0], turned(entry[1], 64))
    wide_ref[:, 128:256] = jnp.where(left, entry[2], turned(entry[3], 64))
    wide_ref[:, 256:384] = quarters(act_ref, 64)
    conv = convolved(wide_ref, jnp.concatenate([ci_ref[...], cb_ref[...]], axis=1))
    xin, bkey = conv[:, 0:256], conv[:, 256:384]
    xin_ref[...] = xin
    bkey_ref[...] = bkey
    row = iota((BLOCK, BLOCK), 0)
    col = iota((BLOCK, BLOCK), 1)
    step = jnp.concatenate([step_ref[pl.ds(4 * tensor + h, 1), :] for h in range(4)], axis=0)
    rates = jnp.concatenate(
        [jnp.full((1, BLOCK), rate[4 * tensor + h], F32) for h in range(4)], axis=0
    )
    decay = off_ref[...] - rates * step
    decay8 = jnp.concatenate([decay, jnp.zeros((4, BLOCK), F32)], axis=0)
    upper = (row <= col).astype(F32)
    cum = jnp.dot(decay8, upper, precision=HIGH, preferred_element_type=F32)
    last = jnp.sum(decay, axis=1, keepdims=True)
    to_end = jnp.exp(last - cum[0:4]) * step
    eye = (row == col).astype(F32)
    cols = lax.dot_general(
        eye, jnp.concatenate([cum[0:4], to_end], axis=0), NT, precision=HIGH,
        preferred_element_type=F32,
    )
    rows_ref[...] = jnp.concatenate([cum[0:4], step], axis=0)
    cols_ref[...] = cols
    wide_key = bkey.astype(F32)
    for h in range(4):
        wk = (wide_key * cols[:, 4 + h : 5 + h]).astype(BF16)
        state = lax.dot_general(
            xin[:, h * 64 : (h + 1) * 64], wk, TN, preferred_element_type=F32
        )
        log = jnp.broadcast_to(last[h : h + 1], (8, BLOCK))
        high = log.astype(BF16).astype(F32)
        logs = jnp.concatenate([high, log - high], axis=0).astype(BF16)
        send_ref[BLOCK : BLOCK + 64, h * 128 : (h + 1) * 128] = state.astype(BF16)
        send_ref[BLOCK + 64 : KEPT, h * 128 : (h + 1) * 128] = logs
    for copy in moved:
        copy.wait()


def local_call(ids, rate, act, step, offset, conv_weight, buf):
    full = lambda *shape: pl.BlockSpec(shape, lambda i, ids, rate: (0,) * len(shape))
    return pl.pallas_call(
        local_kernel,
        grid_spec=pltpu.PrefetchScalarGridSpec(
            num_scalar_prefetch=2,
            grid=(1,),
            in_specs=[
                full(*act.shape),
                full(*step.shape),
                full(*offset.shape),
                pl.BlockSpec((CONV, 256), lambda i, ids, rate: (0, ids[1])),
                pl.BlockSpec((CONV, 128), lambda i, ids, rate: (0, 16 + ids[1])),
                pl.BlockSpec(memory_space=pl.ANY),
            ],
            out_specs=[
                full(SENT, 512), full(BLOCK, 256), full(BLOCK, 128), full(8, BLOCK),
                full(BLOCK, 8),
            ],
            scratch_shapes=[pltpu.VMEM((ROWS, 384), F32), pltpu.SemaphoreType.DMA((4,))],
        ),
        out_shape=(
            jax.ShapeDtypeStruct((SENT, 512), BF16),
            jax.ShapeDtypeStruct((BLOCK, 256), BF16),
            jax.ShapeDtypeStruct((BLOCK, 128), BF16),
            jax.ShapeDtypeStruct((8, BLOCK), F32),
            jax.ShapeDtypeStruct((BLOCK, 8), F32),
        ),
        name="ssd_local",
    )(ids, rate, act, step, offset, conv_weight, conv_weight, buf)


def inner_kernel(
    ids, act_ref, cc_ref, xin_ref, bkey_ref, rows_ref, cols_ref,
    yin_ref, gate_ref, cq_ref, q_ref, wide_ref,
):
    gate_ref[...] = silu(jnp.concatenate(joined(act_ref, BLOCK, False), axis=1))
    q_ref[...] = jnp.concatenate(joined(act_ref, BLOCK, True), axis=1).astype(BF16)
    wide_ref[...] = quarters(act_ref, 0)
    cquery = convolved(wide_ref, cc_ref[...])
    cq_ref[...] = cquery
    lower = iota((BLOCK, BLOCK), 0) >= iota((BLOCK, BLOCK), 1)
    inner = lax.dot_general(cquery, bkey_ref[...], NT, preferred_element_type=F32)
    for h in range(4):
        spread = cols_ref[:, h : h + 1] - rows_ref[h : h + 1, :]
        decayed = jnp.exp(jnp.where(lower, spread, 0.0))
        mix = jnp.where(lower, inner * decayed * rows_ref[4 + h : 5 + h, :], 0.0).astype(BF16)
        yin_ref[:, h * 64 : (h + 1) * 64] = jnp.dot(
            mix, xin_ref[:, h * 64 : (h + 1) * 64], preferred_element_type=F32
        )


def inner_call(ids, act, conv_weight, xin, bkey, rows, cols):
    full = lambda *shape: pl.BlockSpec(shape, lambda i, ids: (0,) * len(shape))
    return pl.pallas_call(
        inner_kernel,
        grid_spec=pltpu.PrefetchScalarGridSpec(
            num_scalar_prefetch=1,
            grid=(1,),
            in_specs=[
                full(*act.shape),
                pl.BlockSpec((CONV, 128), lambda i, ids: (0, 24 + ids[1])),
                full(BLOCK, 256), full(BLOCK, 128), full(8, BLOCK), full(BLOCK, 8),
            ],
            out_specs=[full(BLOCK, 256), full(BLOCK, 256), full(BLOCK, 128), full(BLOCK, 256)],
            scratch_shapes=[pltpu.VMEM((BLOCK + HALO, 128), F32)],
        ),
        out_shape=(
            jax.ShapeDtypeStruct((BLOCK, 256), F32),
            jax.ShapeDtypeStruct((BLOCK, 256), F32),
            jax.ShapeDtypeStruct((BLOCK, 128), BF16),
            jax.ShapeDtypeStruct((BLOCK, 256), BF16),
        ),
        compiler_params=vmem(),
        name="ssd_inner",
    )(ids, act, conv_weight, xin, bkey, rows, cols)


KEYS = 512
KEPT = BLOCK + 80
SENT = KEPT + BLOCK
LOG2E = 1.4426950408889634


def attend_kernel(
    ids, bias, q_ref, yin_ref, gate_ref, cq_ref, cols_ref, gain_ref, all_hbm,
    out_ref, kv_ref, st_ref, w_ref, acc_ref, late_ref, hold_ref, sems, ksems,
):
    block, tensor = ids[0], ids[1]
    per = KEYS // BLOCK
    count = all_hbm.shape[0]
    chunks = range(count // per - 1, -1, -1)
    last = block // per

    def move(chunk):
        picked = pl.ds(chunk * per, per)
        return pltpu.make_async_copy(
            all_hbm.at[picked, pl.ds(0, BLOCK)], kv_ref.at[picked], ksems.at[chunk]
        )

    states = pltpu.make_async_copy(all_hbm.at[:, pl.ds(BLOCK, 80)], st_ref, sems.at[0])
    weights = pltpu.make_async_copy(all_hbm.at[:, pl.ds(KEPT, BLOCK)], w_ref, sems.at[1])
    for chunk in chunks:
        pl.when((chunk <= last) & (chunk >= last - 1))(lambda chunk=chunk: move(chunk).start())
    acc_ref[...] = jnp.zeros_like(acc_ref)
    late_ref[...] = jnp.zeros_like(late_ref)
    hold_ref[...] = jnp.zeros_like(hold_ref)
    row = iota((256, 256), 0) % 128
    col = iota((256, 256), 1)
    onward = ((row > col) | (col >= 128)).astype(BF16)

    def piece(turn, carry):
        chunk = last - turn
        move(chunk).wait()
        pl.when(chunk > 1)(lambda: move(chunk - 2).start())

        @pl.when(turn == jnp.minimum(last, 1))
        def _():
            states.start()
            weights.start()

        picked = pl.ds(chunk * per, per)
        before = [
            chunk * KEYS + sub * BLOCK + iota((BLOCK, BLOCK), 1)
            < block * BLOCK + iota((BLOCK, BLOCK), 0)
            for sub in range(per)
        ]
        taken, parts = {}, []
        for h in range(2):
            query = q_ref[:, h * 128 : (h + 1) * 128]
            key = kv_ref[picked, :, h * 128 : (h + 1) * 128].reshape(KEYS, 128)
            logits = lax.dot_general(query, key, NT, preferred_element_type=F32)
            logits = logits * (128 ** -0.5 * LOG2E) + bias[2 * tensor + h] * LOG2E
            soft = jnp.maximum(logits, 0.0) + LOG2E * jnp.log(1.0 + jnp.exp2(-jnp.abs(logits)))
            for sub in range(per):
                at = slice(sub * BLOCK, (sub + 1) * BLOCK)
                taken[h, sub] = logits[:, at] - soft[:, at]
                kept = jnp.where(before[sub], soft[:, at], 0.0)
                high = kept.astype(BF16)
                low = (kept - high.astype(F32)).astype(BF16)
                parts.append(jnp.concatenate([high, low], axis=1))
        sums = jnp.dot(jnp.concatenate(parts, axis=0), onward, preferred_element_type=F32)
        for h in range(2):
            late = late_ref[h]
            weights_h = [None] * per
            for sub in range(per - 1, -1, -1):
                at = (h * per + sub) * BLOCK
                mine_sums = sums[at : at + BLOCK]
                weight = jnp.exp2(taken[h, sub] - (mine_sums[:, 0:128] + late))
                weights_h[sub] = jnp.where(before[sub], weight, 0.0).astype(BF16)
                late = late + mine_sums[:, 128:256]
            value = kv_ref[picked, :, 256 + h * 128 : 256 + (h + 1) * 128].reshape(KEYS, 128)
            acc_ref[h] += jnp.dot(
                jnp.concatenate(weights_h, axis=1), value, preferred_element_type=F32
            )
            late_ref[h] = late
        return carry

    lax.fori_loop(0, last + 1, piece, 0)
    states.wait()

    def advance(k, carry):
        logs = st_ref[k, 64:80, :].astype(F32)
        decay = jnp.exp(logs[0:8] + logs[8:16])
        hold_ref[...] = hold_ref[...] * jnp.concatenate([decay] * 8, axis=0) + st_ref[
            k, 0:64, :
        ].astype(F32)
        return carry

    lax.fori_loop(0, block, advance, 0)
    cquery = cq_ref[...]
    ys = []
    for h in range(4):
        enter = hold_ref[:, h * 128 : (h + 1) * 128].astype(BF16)
        moved = lax.dot_general(cquery, enter, NT, preferred_element_type=F32)
        ys.append(moved * jnp.exp(cols_ref[:, h : h + 1]))
    gated = (yin_ref[...] + jnp.concatenate(ys, axis=1)) * gate_ref[...]
    scale = lax.rsqrt(jnp.mean(gated * gated, axis=-1, keepdims=True) + EPS)
    mixed = (gated * scale * gain_ref[...]).astype(BF16)
    both = jnp.concatenate([mixed, acc_ref[0].astype(BF16), acc_ref[1].astype(BF16)], axis=1)
    weights.wait()
    for s in range(count):
        out_ref[:, 128 * s : 128 * (s + 1)] = lax.dot_general(
            both, w_ref[s], NT, preferred_element_type=F32
        ).astype(BF16)


def attend_call(ids, bias, q, yin, gate, cq, cols, gain, gathered):
    full = lambda *shape: pl.BlockSpec(shape, lambda i, ids, bias: (0,) * len(shape))
    count = gathered.shape[0]
    return pl.pallas_call(
        attend_kernel,
        grid_spec=pltpu.PrefetchScalarGridSpec(
            num_scalar_prefetch=2,
            grid=(1,),
            in_specs=[
                full(BLOCK, 256), full(BLOCK, 256), full(BLOCK, 256), full(BLOCK, 128),
                full(BLOCK, 8), pl.BlockSpec((1, 256), lambda i, ids, bias: (0, ids[1])),
                pl.BlockSpec(memory_space=pltpu.HBM),
            ],
            out_specs=full(BLOCK, 2048),
            scratch_shapes=[
                pltpu.VMEM((count, BLOCK, 512), BF16),
                pltpu.VMEM((count, 80, 512), BF16),
                pltpu.VMEM((count, BLOCK, 512), BF16),
                pltpu.VMEM((2, BLOCK, 128), F32),
                pltpu.VMEM((2, BLOCK, 128), F32),
                pltpu.VMEM((64, 512), F32),
                pltpu.SemaphoreType.DMA((2,)),
                pltpu.SemaphoreType.DMA((count * BLOCK // KEYS,)),
            ],
        ),
        out_shape=jax.ShapeDtypeStruct((BLOCK, 2048), BF16),
        compiler_params=vmem(),
        name="attend",
    )(ids, bias, q, yin, gate, cq, cols, gain.reshape(1, -1), gathered)


def body(
    inputs, norm_gain, w_gate, w_input, w_bkey, w_cquery, w_step, conv_weight, decay_rate,
    decay_offset, ssd_gain, w_query, w_key, w_value, stick_bias, out_mixer, out_attend,
):
    length = lax.axis_size("sp")
    ids = jnp.stack([lax.axis_index(name) for name in ("sp", "tp")]).astype(jnp.int32)
    halo = lax.ppermute(
        inputs[0, BLOCK - HALO :], "sp", [(i, i + 1) for i in range(length - 1)]
    )
    normed, step, cut = prep_call(
        inputs, norm_gain, w_step.T, w_key, w_value, w_input, w_gate, w_query, w_bkey, w_cquery,
        out_mixer.T, out_attend.T,
    )
    cut = lax.all_to_all(cut, "fs", 0, 0, tiled=True)
    tokens = lax.all_gather(halo_call(normed, halo, norm_gain), "fs", axis=0)

    def projected(at, width):
        part = cut[:, :, at : at + width].reshape(-1, width)
        act = project_call(tokens, lax.all_gather(part, "sp", axis=0, tiled=True))
        return lax.all_to_all(act, "fs", 0, 0, tiled=True)

    send, xin, bkey, srows, scols = local_call(
        ids, decay_rate, projected(0, 224), step, decay_offset[0].T, conv_weight, cut
    )
    gathered = lax.all_gather(send, "sp", axis=0)
    yin, gate, cq, q = inner_call(
        ids, projected(256, 160), conv_weight, xin, bkey, srows, scols
    )
    partial = attend_call(ids, stick_bias, q, yin, gate, cq, scols, ssd_gain, gathered)
    parts = lax.all_to_all(partial.reshape(8, 16, 2048), "tp", 0, 0, tiled=True)
    return jnp.sum(parts.astype(F32), axis=0).astype(BF16)[None]


def solution(mesh):
    shard = P(("sp", "fs"), "tp")
    return jax.shard_map(
        body,
        mesh=mesh,
        in_specs=(
            P("fs", "sp", None), P(), shard, shard, shard, shard, P(), P(), P(),
            P("fs", "sp", "tp"), P(), shard, shard, shard, P(),
            P("tp", ("sp", "fs")), P("tp", ("sp", "fs")),
        ),
        out_specs=P("fs", ("sp", "tp"), None),
        check_vma=False,
    )
```

```python
import jax
import jax.numpy as jnp
from jax import lax
from jax.experimental import pallas as pl
from jax.experimental.pallas import tpu as pltpu
from jax.sharding import PartitionSpec as P

BLOCK = 128
CONV = 4
EPS = 1e-06
HALO = 16
ROWS = BLOCK + HALO
F32 = jnp.float32
BF16 = jnp.bfloat16
HIGH = lax.Precision.HIGHEST
NT = (((1,), (1,)), ((), ()))
TN = (((0,), (0,)), ((), ()))


def vmem(limit=48):
    return pltpu.CompilerParams(vmem_limit_bytes=limit * 1024 * 1024)


def iota(shape, dim):
    return lax.broadcasted_iota(jnp.int32, shape, dim)


def softplus(x):
    return jnp.maximum(x, 0.0) + jnp.log1p(jnp.exp(-jnp.abs(x)))


def silu(x):
    return x / (1.0 + jnp.exp(-x))


def pull(pairs, sems):
    copies = [pltpu.make_async_copy(src, dst, sems.at[i]) for i, (src, dst) in enumerate(pairs)]
    for copy in copies:
        copy.start()
    return copies


def shuffled(normed, f, g):
    lane = iota((normed.shape[0], 128), 1) // 32
    out = None
    for k in range(4):
        at = (4 * g + k) * 128
        piece = normed[:, at : at + 128]
        shift = ((k - f) * 32) % 128
        if shift:
            piece = pltpu.roll(piece, shift, 1)
        out = piece if out is None else jnp.where(lane == k, piece, out)
    return out.astype(BF16)


def normalised(x, gain):
    wide = x.astype(F32)
    scale = lax.rsqrt(jnp.mean(wide * wide, axis=-1, keepdims=True) + EPS)
    return (wide * scale * gain).astype(BF16)


def prep_kernel(*refs):
    x_hbm, gain_hbm, ws_hbm = refs[:3]
    sources = refs[3:12]
    xs_hbm, step_ref, first_ref, second_ref = refs[12:16]
    x_ref, gain_ref, ws_ref, third_ref, xs_ref, sems, wsems, xsems = refs[16:]
    early = pull(((x_hbm.at[0], x_ref), (gain_hbm, gain_ref), (ws_hbm, ws_ref)), sems)
    pairs = []
    outs = (first_ref, second_ref, third_ref)
    at, which = 0, 0
    for n, src in enumerate(sources):
        if n in (4, 8):
            at, which = 0, which + 1
        pairs.append((src, outs[which].at[:, pl.ds(at, src.shape[1])]))
        at += src.shape[1]
    later = pull(pairs, wsems)
    for copy in early:
        copy.wait()
    normed = normalised(x_ref[...], gain_ref[...])
    step_ref[...] = softplus(
        lax.dot_general(ws_ref[...], normed, NT, preferred_element_type=F32)
    )
    wide = normed.astype(F32)
    for copy in later:
        copy.wait()
    writes = []
    for f in range(4):
        for g in range(4):
            xs_ref[f, 0:BLOCK, g * 128 : (g + 1) * 128] = shuffled(wide, f, g)
        xs_ref[f, BLOCK:, 0:256] = third_ref[0:16, :]
        xs_ref[f, BLOCK:, 256:512] = third_ref[16:32, :]
        writes.append(pltpu.make_async_copy(xs_ref.at[f], xs_hbm.at[f], xsems.at[f]))
        writes[-1].start()
    for copy in writes:
        copy.wait()


def prep_call(inputs, gain, w_step_t, *arrays):
    rows, width = inputs.shape[1:]
    heads = w_step_t.shape[0]
    part = arrays[0].shape[0]
    widths = [sum(a.shape[1] for a in group) for group in (arrays[:4], arrays[4:8], arrays[8:])]
    hbm = pl.BlockSpec(memory_space=pltpu.HBM)
    return pl.pallas_call(
        prep_kernel,
        in_specs=[hbm] * 12,
        out_specs=[hbm] + [pl.BlockSpec(memory_space=pltpu.VMEM)] * 3,
        out_shape=(
            jax.ShapeDtypeStruct((4, rows + HALO, width // 4), BF16),
            jax.ShapeDtypeStruct((heads, rows), F32),
            jax.ShapeDtypeStruct((part, widths[0]), BF16),
            jax.ShapeDtypeStruct((part, widths[1]), BF16),
        ),
        scratch_shapes=[
            pltpu.VMEM((rows, width), BF16),
            pltpu.VMEM((1, width), F32),
            pltpu.VMEM((heads, width), BF16),
            pltpu.VMEM((part, widths[2]), BF16),
            pltpu.VMEM((4, rows + HALO, width // 4), BF16),
            pltpu.SemaphoreType.DMA((3,)),
            pltpu.SemaphoreType.DMA((9,)),
            pltpu.SemaphoreType.DMA((4,)),
        ],
        name="prep",
    )(inputs, gain.reshape(1, -1), w_step_t, *arrays)


def project_kernel(x_ref, rim_ref, w_ref, out_hbm, *rest):
    kept, (out_ref, sems) = rest[:-2], rest[-2:]
    width = out_hbm.shape[2]
    weights = w_ref[:, 0:width]
    copies = []
    for f in range(4):
        rows = jnp.concatenate([rim_ref[f], x_ref[f, 0:BLOCK, :]], axis=0)
        out_ref[f] = jnp.dot(rows, weights, preferred_element_type=F32).astype(BF16)
        copies.append(pltpu.make_async_copy(out_ref.at[f], out_hbm.at[f], sems.at[f]))
        copies[-1].start()
    for ref in kept:
        ref[...] = w_ref[:, width:]
    for copy in copies:
        copy.wait()


def project_call(x, rim, w, width):
    whole = pl.BlockSpec(memory_space=pltpu.VMEM)
    outs = [jax.ShapeDtypeStruct((4, ROWS, width), BF16)]
    specs = [pl.BlockSpec(memory_space=pltpu.HBM)]
    if w.shape[1] > width:
        outs.append(jax.ShapeDtypeStruct((w.shape[0], w.shape[1] - width), BF16))
        specs.append(whole)
    return pl.pallas_call(
        project_kernel,
        in_specs=[whole] * 3,
        out_specs=specs,
        out_shape=outs,
        scratch_shapes=[pltpu.VMEM((4, ROWS, width), BF16), pltpu.SemaphoreType.DMA((4,))],
        compiler_params=vmem(),
        name="project",
    )(x, rim, w)


def added(ref, at, width):
    total = ref[0, :, at : at + width].astype(F32)
    for j in range(1, 4):
        total = total + ref[j, :, at : at + width].astype(F32)
    return total.astype(BF16)


def convolved(wide_ref, taps):
    summed = None
    for i in range(CONV):
        at = HALO - CONV + 1 + i
        part = taps[i : i + 1] * wide_ref[at : at + BLOCK, :]
        summed = part if summed is None else summed + part
    return silu(summed).astype(BF16)


def local_kernel(
    ids, rate, act_ref, step_ref, off_ref, ci_ref, cb_ref, buf_ref,
    send_hbm, xin_ref, bkey_ref, rows_ref, cols_ref, wide_ref, send_ref, sems,
):
    tensor = ids[1]
    moved = pull(
        [
            (buf_ref.at[f, pl.ds(BLOCK, HALO)], send_hbm.at[pl.ds(KEPT + HALO * f, HALO)])
            for f in range(4)
        ],
        sems,
    )
    send_ref[0:BLOCK, :] = added(act_ref, 0, 512)[HALO:]
    moved.append(
        pltpu.make_async_copy(
            send_ref.at[pl.ds(0, BLOCK)], send_hbm.at[pl.ds(0, BLOCK)], sems.at[4]
        )
    )
    moved[-1].start()
    wide_ref[...] = added(act_ref, 512, 384).astype(F32)
    conv = convolved(wide_ref, jnp.concatenate([ci_ref[...], cb_ref[...]], axis=1))
    xin, bkey = conv[:, 0:256], conv[:, 256:384]
    xin_ref[...] = xin
    bkey_ref[...] = bkey
    row = iota((BLOCK, BLOCK), 0)
    col = iota((BLOCK, BLOCK), 1)
    step = jnp.concatenate([step_ref[pl.ds(4 * tensor + h, 1), :] for h in range(4)], axis=0)
    rates = jnp.concatenate(
        [jnp.full((1, BLOCK), rate[4 * tensor + h], F32) for h in range(4)], axis=0
    )
    decay = off_ref[...] - rates * step
    decay8 = jnp.concatenate([decay, jnp.zeros((4, BLOCK), F32)], axis=0)
    upper = (row <= col).astype(F32)
    cum = jnp.dot(decay8, upper, precision=HIGH, preferred_element_type=F32)
    last = jnp.sum(decay, axis=1, keepdims=True)
    to_end = jnp.exp(last - cum[0:4]) * step
    eye = (row == col).astype(F32)
    cols = lax.dot_general(
        eye, jnp.concatenate([cum[0:4], to_end], axis=0), NT, precision=HIGH,
        preferred_element_type=F32,
    )
    rows_ref[...] = jnp.concatenate([cum[0:4], step], axis=0)
    cols_ref[...] = cols
    wide_key = bkey.astype(F32)
    for h in range(4):
        wk = (wide_key * cols[:, 4 + h : 5 + h]).astype(BF16)
        state = lax.dot_general(
            xin[:, h * 64 : (h + 1) * 64], wk, TN, preferred_element_type=F32
        )
        log = jnp.broadcast_to(last[h : h + 1], (8, BLOCK))
        high = log.astype(BF16).astype(F32)
        logs = jnp.concatenate([high, log - high], axis=0).astype(BF16)
        send_ref[BLOCK : BLOCK + 64, h * 128 : (h + 1) * 128] = state.astype(BF16)
        send_ref[BLOCK + 64 : KEPT, h * 128 : (h + 1) * 128] = logs
    kept = pl.ds(BLOCK, KEPT - BLOCK)
    moved.append(pltpu.make_async_copy(send_ref.at[kept], send_hbm.at[kept], sems.at[5]))
    moved[-1].start()
    for copy in moved:
        copy.wait()


def local_call(ids, rate, act, step, offset, conv_weight, buf):
    full = lambda *shape: pl.BlockSpec(shape, lambda i, ids, rate: (0,) * len(shape))
    return pl.pallas_call(
        local_kernel,
        grid_spec=pltpu.PrefetchScalarGridSpec(
            num_scalar_prefetch=2,
            grid=(1,),
            in_specs=[
                full(*act.shape),
                full(*step.shape),
                full(*offset.shape),
                pl.BlockSpec((CONV, 256), lambda i, ids, rate: (0, ids[1])),
                pl.BlockSpec((CONV, 128), lambda i, ids, rate: (0, 16 + ids[1])),
                pl.BlockSpec(memory_space=pl.ANY),
            ],
            out_specs=[
                pl.BlockSpec(memory_space=pltpu.HBM), full(BLOCK, 256), full(BLOCK, 128),
                full(8, BLOCK),
                full(BLOCK, 8),
            ],
            scratch_shapes=[
                pltpu.VMEM((ROWS, 384), F32),
                pltpu.VMEM((KEPT, 512), BF16),
                pltpu.SemaphoreType.DMA((6,)),
            ],
        ),
        out_shape=(
            jax.ShapeDtypeStruct((SENT, 512), BF16),
            jax.ShapeDtypeStruct((BLOCK, 256), BF16),
            jax.ShapeDtypeStruct((BLOCK, 128), BF16),
            jax.ShapeDtypeStruct((8, BLOCK), F32),
            jax.ShapeDtypeStruct((BLOCK, 8), F32),
        ),
        compiler_params=vmem(),
        name="ssd_local",
    )(ids, rate, act, step, offset, conv_weight, conv_weight, buf)


def inner_kernel(
    ids, act_ref, cc_ref, xin_ref, bkey_ref, rows_ref, cols_ref,
    yin_ref, gate_ref, cq_ref, q_ref, wide_ref,
):
    gate_ref[...] = silu(added(act_ref, 0, 256)[HALO:].astype(F32))
    q_ref[...] = added(act_ref, 384, 256)[HALO:]
    wide_ref[...] = added(act_ref, 256, 128).astype(F32)
    cquery = convolved(wide_ref, cc_ref[...])
    cq_ref[...] = cquery
    lower = iota((BLOCK, BLOCK), 0) >= iota((BLOCK, BLOCK), 1)
    inner = lax.dot_general(cquery, bkey_ref[...], NT, preferred_element_type=F32)
    for h in range(4):
        spread = cols_ref[:, h : h + 1] - rows_ref[h : h + 1, :]
        decayed = jnp.exp(jnp.where(lower, spread, 0.0))
        mix = jnp.where(lower, inner * decayed * rows_ref[4 + h : 5 + h, :], 0.0).astype(BF16)
        yin_ref[:, h * 64 : (h + 1) * 64] = jnp.dot(
            mix, xin_ref[:, h * 64 : (h + 1) * 64], preferred_element_type=F32
        )


def inner_call(ids, act, conv_weight, xin, bkey, rows, cols):
    full = lambda *shape: pl.BlockSpec(shape, lambda i, ids: (0,) * len(shape))
    return pl.pallas_call(
        inner_kernel,
        grid_spec=pltpu.PrefetchScalarGridSpec(
            num_scalar_prefetch=1,
            grid=(1,),
            in_specs=[
                full(*act.shape),
                pl.BlockSpec((CONV, 128), lambda i, ids: (0, 24 + ids[1])),
                full(BLOCK, 256), full(BLOCK, 128), full(8, BLOCK), full(BLOCK, 8),
            ],
            out_specs=[full(BLOCK, 256), full(BLOCK, 256), full(BLOCK, 128), full(BLOCK, 256)],
            scratch_shapes=[pltpu.VMEM((BLOCK + HALO, 128), F32)],
        ),
        out_shape=(
            jax.ShapeDtypeStruct((BLOCK, 256), F32),
            jax.ShapeDtypeStruct((BLOCK, 256), F32),
            jax.ShapeDtypeStruct((BLOCK, 128), BF16),
            jax.ShapeDtypeStruct((BLOCK, 256), BF16),
        ),
        compiler_params=vmem(),
        name="ssd_inner",
    )(ids, act, conv_weight, xin, bkey, rows, cols)


KEYS = 512
KEPT = BLOCK + 80
SENT = KEPT + 64
LOG2E = 1.4426950408889634


def attend_kernel(
    ids, bias, q_ref, yin_ref, gate_ref, cq_ref, cols_ref, gain_ref, all_hbm, a0, a1, a2, a3,
    out_ref, kv_ref, st_ref, wm_ref, wa_ref, acc_ref, late_ref, hold_ref, sems, ksems, gsems,
):
    block, tensor, mine = ids[0], ids[1], ids[2]
    per = KEYS // BLOCK
    count = all_hbm.shape[0]
    chunks = range(count // per - 1, -1, -1)
    last = block // per

    def move(chunk):
        picked = pl.ds(chunk * per, per)
        return pltpu.make_async_copy(
            all_hbm.at[picked, pl.ds(0, BLOCK)], kv_ref.at[picked], ksems.at[chunk]
        )

    def states(group):
        picked = pl.ds(group * per, per)
        return pltpu.make_async_copy(
            all_hbm.at[picked, pl.ds(BLOCK, 80)], st_ref.at[picked], gsems.at[group]
        )

    weights = [pltpu.make_async_copy(all_hbm.at[:, pl.ds(KEPT, 64)], wm_ref, sems.at[0])]
    weights += [
        pltpu.make_async_copy(w, wa_ref.at[(mine + 4 - r) % 4], sems.at[1 + r])
        for r, w in enumerate((a0, a1, a2, a3))
    ]
    for group in range(count // per):
        pl.when(group * per < block)(lambda group=group: states(group).start())
    for chunk in chunks:
        pl.when((chunk <= last) & (chunk >= last - 1))(lambda chunk=chunk: move(chunk).start())
    acc_ref[...] = jnp.zeros_like(acc_ref)
    late_ref[...] = jnp.zeros_like(late_ref)
    hold_ref[...] = jnp.zeros_like(hold_ref)
    for group in range(count // per):
        pl.when(group * per < block)(lambda group=group: states(group).wait())

    def advance(k, carry):
        logs = st_ref[k, 64:80, :].astype(F32)
        decay = jnp.exp(logs[0:8] + logs[8:16])
        hold_ref[...] = hold_ref[...] * jnp.concatenate([decay] * 8, axis=0) + st_ref[
            k, 0:64, :
        ].astype(F32)
        return carry

    lax.fori_loop(0, block, advance, 0)
    cquery = cq_ref[...]
    ys = []
    for h in range(4):
        enter = hold_ref[:, h * 128 : (h + 1) * 128].astype(BF16)
        moved = lax.dot_general(cquery, enter, NT, preferred_element_type=F32)
        ys.append(moved * jnp.exp(cols_ref[:, h : h + 1]))
    gated = (yin_ref[...] + jnp.concatenate(ys, axis=1)) * gate_ref[...]
    scale = lax.rsqrt(jnp.mean(gated * gated, axis=-1, keepdims=True) + EPS)
    mixed = (gated * scale * gain_ref[...]).astype(BF16)
    row = iota((256, 256), 0) % 128
    col = iota((256, 256), 1)
    onward = ((row > col) | (col >= 128)).astype(BF16)

    def piece(turn, carry):
        chunk = last - turn
        move(chunk).wait()
        pl.when(chunk > 1)(lambda: move(chunk - 2).start())

        @pl.when(turn == jnp.minimum(last, 1))
        def _():
            for copy in weights:
                copy.start()

        picked = pl.ds(chunk * per, per)
        before = [
            chunk * KEYS + sub * BLOCK + iota((BLOCK, BLOCK), 1)
            < block * BLOCK + iota((BLOCK, BLOCK), 0)
            for sub in range(per)
        ]
        taken, parts = {}, []
        for h in range(2):
            query = q_ref[:, h * 128 : (h + 1) * 128]
            key = kv_ref[picked, :, h * 128 : (h + 1) * 128].reshape(KEYS, 128)
            logits = lax.dot_general(query, key, NT, preferred_element_type=F32)
            logits = logits * (128 ** -0.5 * LOG2E) + bias[2 * tensor + h] * LOG2E
            soft = jnp.maximum(logits, 0.0) + LOG2E * jnp.log(1.0 + jnp.exp2(-jnp.abs(logits)))
            for sub in range(per):
                at = slice(sub * BLOCK, (sub + 1) * BLOCK)
                taken[h, sub] = logits[:, at] - soft[:, at]
                kept = jnp.where(before[sub], soft[:, at], 0.0)
                high = kept.astype(BF16)
                low = (kept - high.astype(F32)).astype(BF16)
                parts.append(jnp.concatenate([high, low], axis=1))
        sums = jnp.dot(jnp.concatenate(parts, axis=0), onward, preferred_element_type=F32)
        for h in range(2):
            late = late_ref[h]
            weights_h = [None] * per
            for sub in range(per - 1, -1, -1):
                at = (h * per + sub) * BLOCK
                mine_sums = sums[at : at + BLOCK]
                weight = jnp.exp2(taken[h, sub] - (mine_sums[:, 0:128] + late))
                weights_h[sub] = jnp.where(before[sub], weight, 0.0).astype(BF16)
                late = late + mine_sums[:, 128:256]
            value = kv_ref[picked, :, 256 + h * 128 : 256 + (h + 1) * 128].reshape(KEYS, 128)
            acc_ref[h] += jnp.dot(
                jnp.concatenate(weights_h, axis=1), value, preferred_element_type=F32
            )
            late_ref[h] = late
        return carry

    lax.fori_loop(0, last + 1, piece, 0)
    attended = jnp.concatenate([acc_ref[0].astype(BF16), acc_ref[1].astype(BF16)], axis=1)
    for copy in weights:
        copy.wait()
    for s in range(count):
        halves = []
        for f in range(4):
            for half in range(2):
                halves.append(
                    wm_ref[s, 16 * f : 16 * (f + 1), 256 * half : 256 * (half + 1)]
                )
        rows_m = jnp.concatenate(halves, axis=0)
        rows_a = jnp.concatenate(
            [wa_ref[f, 32 * s : 32 * (s + 1), :] for f in range(4)], axis=0
        )
        out_ref[:, 128 * s : 128 * (s + 1)] = (
            lax.dot_general(mixed, rows_m, NT, preferred_element_type=F32)
            + lax.dot_general(attended, rows_a, NT, preferred_element_type=F32)
        ).astype(BF16)


def attend_call(ids, bias, q, yin, gate, cq, cols, gain, gathered, rows):
    full = lambda *shape: pl.BlockSpec(shape, lambda i, ids, bias: (0,) * len(shape))
    count = gathered.shape[0]
    near = pl.BlockSpec(memory_space=pltpu.VMEM)
    return pl.pallas_call(
        attend_kernel,
        grid_spec=pltpu.PrefetchScalarGridSpec(
            num_scalar_prefetch=2,
            grid=(1,),
            in_specs=[
                full(BLOCK, 256), full(BLOCK, 256), full(BLOCK, 256), full(BLOCK, 128),
                full(BLOCK, 8), pl.BlockSpec((1, 256), lambda i, ids, bias: (0, ids[1])),
                pl.BlockSpec(memory_space=pltpu.HBM), near, near, near, near,
            ],
            out_specs=full(BLOCK, 2048),
            scratch_shapes=[
                pltpu.VMEM((count, BLOCK, 512), BF16),
                pltpu.VMEM((count, 80, 512), BF16),
                pltpu.VMEM((count, 64, 512), BF16),
                pltpu.VMEM((4, 512, 256), BF16),
                pltpu.VMEM((2, BLOCK, 128), F32),
                pltpu.VMEM((2, BLOCK, 128), F32),
                pltpu.VMEM((64, 512), F32),
                pltpu.SemaphoreType.DMA((5,)),
                pltpu.SemaphoreType.DMA((count * BLOCK // KEYS,)),
                pltpu.SemaphoreType.DMA((count * BLOCK // KEYS,)),
            ],
        ),
        out_shape=jax.ShapeDtypeStruct((BLOCK, 2048), BF16),
        compiler_params=vmem(),
        name="attend",
    )(ids, bias, q, yin, gate, cq, cols, gain.reshape(1, -1), gathered, *rows)


def rotated(shard, axis, by):
    length = lax.axis_size(axis)
    return lax.ppermute(shard, axis, [(i, (i + by) % length) for i in range(length)])


def body(
    inputs, norm_gain, w_gate, w_input, w_bkey, w_cquery, w_step, conv_weight, decay_rate,
    decay_offset, ssd_gain, w_query, w_key, w_value, stick_bias, out_mixer, out_attend,
):
    length = lax.axis_size("sp")
    ids = jnp.stack([lax.axis_index(name) for name in ("sp", "tp", "fs")]).astype(jnp.int32)
    split, step, first, second = prep_call(
        inputs, norm_gain, w_step.T, w_key, w_value, w_input, w_bkey, w_gate, w_cquery, w_query,
        out_attend.T, out_mixer.T,
    )
    tokens = lax.all_to_all(split, "fs", 0, 0, tiled=True)
    early = lax.all_gather(first, "sp", axis=0, tiled=True)
    tokens, early = lax.optimization_barrier((tokens, early))
    rim = lax.ppermute(
        tokens[:, BLOCK - HALO : BLOCK], "sp", [(i, i + 1) for i in range(length - 1)]
    )

    def projected(whole, width):
        act, *kept = project_call(tokens, rim, whole, width)
        return lax.all_to_all(act, "fs", 0, 0, tiled=True), *kept

    (act,) = projected(early, 896)
    send, xin, bkey, srows, scols = local_call(
        ids, decay_rate, act, step, decay_offset[0].T, conv_weight, tokens
    )
    gathered = lax.all_gather(send, "sp", axis=0)
    act, kept = projected(lax.all_gather(second, "sp", axis=0, tiled=True), 640)
    rows = [kept] + [rotated(kept, "fs", by) for by in (1, 2, 3)]
    yin, gate, cq, q = inner_call(ids, act, conv_weight, xin, bkey, srows, scols)
    partial = attend_call(ids, stick_bias, q, yin, gate, cq, scols, ssd_gain, gathered, rows)
    parts = lax.all_to_all(partial.reshape(8, 16, 2048), "tp", 0, 0, tiled=True)
    return jnp.sum(parts.astype(F32), axis=0).astype(BF16)[None]


def solution(mesh):
    shard = P(("sp", "fs"), "tp")
    return jax.shard_map(
        body,
        mesh=mesh,
        in_specs=(
            P("fs", "sp", None), P(), shard, shard, shard, shard, P(), P(), P(),
            P("fs", "sp", "tp"), P(), shard, shard, shard, P(),
            P("tp", ("sp", "fs")), P("tp", ("sp", "fs")),
        ),
        out_specs=P("fs", ("sp", "tp"), None),
        check_vma=False,
    )
```

```python
import functools

import jax
import jax.numpy as jnp
from jax import lax
from jax.experimental import pallas as pl
from jax.experimental.pallas import tpu as pltpu
from jax.sharding import PartitionSpec as P


BLOCK = 128
CONV = 4
EPS = 1e-06
HALO = 16
ROWS = BLOCK + HALO
F32 = jnp.float32
BF16 = jnp.bfloat16
HIGH = lax.Precision.HIGHEST
NT = (((1,), (1,)), ((), ()))
TN = (((0,), (0,)), ((), ()))


def vmem(limit=48):
    return pltpu.CompilerParams(vmem_limit_bytes=limit * 1024 * 1024)


def iota(shape, dim):
    return lax.broadcasted_iota(jnp.int32, shape, dim)


def softplus(x):
    return jnp.maximum(x, 0.0) + jnp.log1p(jnp.exp(-jnp.abs(x)))


def silu(x):
    return x / (1.0 + jnp.exp(-x))


def pull(pairs, sems):
    copies = [pltpu.make_async_copy(src, dst, sems.at[i]) for i, (src, dst) in enumerate(pairs)]
    for copy in copies:
        copy.start()
    return copies


def shuffled(normed, f, g):
    lane = iota((normed.shape[0], 128), 1) // 32
    out = None
    for k in range(4):
        at = (4 * g + k) * 128
        piece = normed[:, at : at + 128]
        shift = ((k - f) * 32) % 128
        if shift:
            piece = pltpu.roll(piece, shift, 1)
        out = piece if out is None else jnp.where(lane == k, piece, out)
    return out.astype(BF16)


def normalised(x, gain):
    wide = x.astype(F32)
    scale = lax.rsqrt(jnp.mean(wide * wide, axis=-1, keepdims=True) + EPS)
    return (wide * scale * gain).astype(BF16)


def prep_kernel(*refs):
    x_hbm, gain_hbm, ws_hbm = refs[:3]
    sources = refs[3:12]
    xs_ref, step_ref, first_ref, second_ref = refs[12:16]
    x_ref, gain_ref, ws_ref, third_ref, sems, wsems = refs[16:]
    early = pull(((x_hbm.at[0], x_ref), (gain_hbm, gain_ref), (ws_hbm, ws_ref)), sems)
    pairs = []
    outs = (first_ref, second_ref, third_ref)
    at, which = 0, 0
    for n, src in enumerate(sources):
        if n in (4, 8):
            at, which = 0, which + 1
        pairs.append((src, outs[which].at[:, pl.ds(at, src.shape[1])]))
        at += src.shape[1]
    later = pull(pairs, wsems)
    for copy in early:
        copy.wait()
    normed = normalised(x_ref[...], gain_ref[...])
    step_ref[...] = softplus(
        lax.dot_general(ws_ref[...], normed, NT, preferred_element_type=F32)
    )
    wide = normed.astype(F32)
    for f in range(4):
        for g in range(4):
            xs_ref[f, 0:BLOCK, g * 128 : (g + 1) * 128] = shuffled(wide, f, g)
    for copy in later:
        copy.wait()
    for f in range(4):
        xs_ref[f, BLOCK:, 0:256] = third_ref[0:16, :]
        xs_ref[f, BLOCK:, 256:512] = third_ref[16:32, :]


def prep_call(inputs, gain, w_step_t, *arrays):
    rows, width = inputs.shape[1:]
    heads = w_step_t.shape[0]
    part = arrays[0].shape[0]
    widths = [sum(a.shape[1] for a in group) for group in (arrays[:4], arrays[4:8], arrays[8:])]
    hbm = pl.BlockSpec(memory_space=pltpu.HBM)
    return pl.pallas_call(
        prep_kernel,
        in_specs=[hbm] * 12,
        out_shape=(
            jax.ShapeDtypeStruct((4, rows + HALO, width // 4), BF16),
            jax.ShapeDtypeStruct((heads, rows), F32),
            jax.ShapeDtypeStruct((part, widths[0]), BF16),
            jax.ShapeDtypeStruct((part, widths[1]), BF16),
        ),
        scratch_shapes=[
            pltpu.VMEM((rows, width), BF16),
            pltpu.VMEM((1, width), F32),
            pltpu.VMEM((heads, width), BF16),
            pltpu.VMEM((part, widths[2]), BF16),
            pltpu.SemaphoreType.DMA((3,)),
            pltpu.SemaphoreType.DMA((9,)),
        ],
        name="prep",
    )(inputs, gain.reshape(1, -1), w_step_t, *arrays)


def project_kernel(has_rim, x_ref, *rest):
    rim_ref, rest = (rest[0], rest[1:]) if has_rim else (None, rest)
    w_ref, out_hbm = rest[:2]
    kept, (out_ref, sems) = rest[2:-2], rest[-2:]
    width = out_hbm.shape[2]
    weights = w_ref[:, 0:width]
    copies = []
    for f in range(4):
        rows = x_ref[f, 0:BLOCK, :]
        if has_rim:
            rows = jnp.concatenate([rim_ref[f], rows], axis=0)
        out_ref[f] = jnp.dot(rows, weights, preferred_element_type=F32)
        copies.append(pltpu.make_async_copy(out_ref.at[f], out_hbm.at[f], sems.at[f]))
        copies[-1].start()
    for ref in kept:
        ref[...] = w_ref[:, width:]
    for copy in copies:
        copy.wait()


def project_call(x, rim, w, width):
    whole = pl.BlockSpec(memory_space=pltpu.VMEM)
    rows = BLOCK if rim is None else ROWS
    outs = [jax.ShapeDtypeStruct((4, rows, width), F32)]
    specs = [pl.BlockSpec(memory_space=pltpu.HBM)]
    if w.shape[1] > width:
        outs.append(jax.ShapeDtypeStruct((w.shape[0], w.shape[1] - width), BF16))
        specs.append(whole)
    given = [x, w] if rim is None else [x, rim, w]
    return pl.pallas_call(
        functools.partial(project_kernel, rim is not None),
        in_specs=[whole] * len(given),
        out_specs=specs,
        out_shape=outs,
        scratch_shapes=[pltpu.VMEM((4, rows, width), F32), pltpu.SemaphoreType.DMA((4,))],
        compiler_params=vmem(),
        name="project",
    )(*given)


def rim_kernel(ids, rim_ref, w_ref, *outs):
    rows = rim_ref[...].reshape(4 * HALO, 512)
    act = jnp.dot(rows, w_ref[:, 512:], preferred_element_type=F32)
    for f in range(4):
        for r in range(4):

            @pl.when((f + 4 - ids[2]) % 4 == r)
            def _(f=f, r=r):
                outs[r][...] = act[f * HALO : (f + 1) * HALO]


def rim_call(ids, rim, w):
    width = w.shape[1] - 512
    full = lambda *shape: pl.BlockSpec(shape, lambda i, ids: (0,) * len(shape))
    return pl.pallas_call(
        rim_kernel,
        grid_spec=pltpu.PrefetchScalarGridSpec(
            num_scalar_prefetch=1,
            grid=(1,),
            in_specs=[full(*rim.shape), full(*w.shape)],
            out_specs=[full(HALO, width)] * 4,
        ),
        out_shape=[jax.ShapeDtypeStruct((HALO, width), F32)] * 4,
        compiler_params=vmem(),
        name="project_rim",
    )(ids, rim, w)


def added(ref, at, width):
    total = ref[0, :, at : at + width].astype(F32)
    for j in range(1, 4):
        total = total + ref[j, :, at : at + width].astype(F32)
    return total.astype(BF16)


def convolved(wide_ref, taps):
    summed = None
    for i in range(CONV):
        at = HALO - CONV + 1 + i
        part = taps[i : i + 1] * wide_ref[at : at + BLOCK, :]
        summed = part if summed is None else summed + part
    return silu(summed).astype(BF16)


def local_kernel(
    ids, rate, act_ref, e0, e1, e2, e3, step_ref, off_ref, ci_ref, cb_ref, buf_ref,
    send_hbm, xin_ref, bkey_ref, rows_ref, cols_ref, wide_ref, send_ref, sems,
):
    tensor = ids[1]
    moved = pull(
        [
            (buf_ref.at[f, pl.ds(BLOCK, HALO)], send_hbm.at[pl.ds(KEPT + HALO * f, HALO)])
            for f in range(4)
        ],
        sems,
    )
    send_ref[0:BLOCK, :] = added(act_ref, 0, 512)
    moved.append(
        pltpu.make_async_copy(
            send_ref.at[pl.ds(0, BLOCK)], send_hbm.at[pl.ds(0, BLOCK)], sems.at[4]
        )
    )
    moved[-1].start()
    edge = e0[...].astype(F32) + e1[...].astype(F32)
    edge = edge + (e2[...].astype(F32) + e3[...].astype(F32))
    wide_ref[0:HALO, :] = edge.astype(BF16).astype(F32)
    wide_ref[HALO:, :] = added(act_ref, 512, 384).astype(F32)
    conv = convolved(wide_ref, jnp.concatenate([ci_ref[...], cb_ref[...]], axis=1))
    xin, bkey = conv[:, 0:256], conv[:, 256:384]
    xin_ref[...] = xin
    bkey_ref[...] = bkey
    row = iota((BLOCK, BLOCK), 0)
    col = iota((BLOCK, BLOCK), 1)
    step = jnp.concatenate([step_ref[pl.ds(4 * tensor + h, 1), :] for h in range(4)], axis=0)
    rates = jnp.concatenate(
        [jnp.full((1, BLOCK), rate[4 * tensor + h], F32) for h in range(4)], axis=0
    )
    decay = off_ref[...] - rates * step
    decay8 = jnp.concatenate([decay, jnp.zeros((4, BLOCK), F32)], axis=0)
    upper = (row <= col).astype(F32)
    cum = jnp.dot(decay8, upper, precision=HIGH, preferred_element_type=F32)
    last = jnp.sum(decay, axis=1, keepdims=True)
    to_end = jnp.exp(last - cum[0:4]) * step
    eye = (row == col).astype(F32)
    cols = lax.dot_general(
        eye, jnp.concatenate([cum[0:4], to_end], axis=0), NT, precision=HIGH,
        preferred_element_type=F32,
    )
    rows_ref[...] = jnp.concatenate([cum[0:4], step], axis=0)
    cols_ref[...] = cols
    wide_key = bkey.astype(F32)
    for h in range(4):
        wk = (wide_key * cols[:, 4 + h : 5 + h]).astype(BF16)
        state = lax.dot_general(
            xin[:, h * 64 : (h + 1) * 64], wk, TN, preferred_element_type=F32
        )
        log = jnp.broadcast_to(last[h : h + 1], (8, BLOCK))
        high = log.astype(BF16).astype(F32)
        logs = jnp.concatenate([high, log - high], axis=0).astype(BF16)
        send_ref[BLOCK : BLOCK + 64, h * 128 : (h + 1) * 128] = state.astype(BF16)
        send_ref[BLOCK + 64 : KEPT, h * 128 : (h + 1) * 128] = logs
    kept = pl.ds(BLOCK, KEPT - BLOCK)
    moved.append(pltpu.make_async_copy(send_ref.at[kept], send_hbm.at[kept], sems.at[5]))
    moved[-1].start()
    for copy in moved:
        copy.wait()


def local_call(ids, rate, act, rim, step, offset, conv_weight, buf):
    full = lambda *shape: pl.BlockSpec(shape, lambda i, ids, rate: (0,) * len(shape))
    return pl.pallas_call(
        local_kernel,
        grid_spec=pltpu.PrefetchScalarGridSpec(
            num_scalar_prefetch=2,
            grid=(1,),
            in_specs=[
                full(*act.shape),
                *(full(*e.shape) for e in rim),
                full(*step.shape),
                full(*offset.shape),
                pl.BlockSpec((CONV, 256), lambda i, ids, rate: (0, ids[1])),
                pl.BlockSpec((CONV, 128), lambda i, ids, rate: (0, 16 + ids[1])),
                pl.BlockSpec(memory_space=pl.ANY),
            ],
            out_specs=[
                pl.BlockSpec(memory_space=pltpu.HBM), full(BLOCK, 256), full(BLOCK, 128),
                full(8, BLOCK),
                full(BLOCK, 8),
            ],
            scratch_shapes=[
                pltpu.VMEM((ROWS, 384), F32),
                pltpu.VMEM((KEPT, 512), BF16),
                pltpu.SemaphoreType.DMA((6,)),
            ],
        ),
        out_shape=(
            jax.ShapeDtypeStruct((SENT, 512), BF16),
            jax.ShapeDtypeStruct((BLOCK, 256), BF16),
            jax.ShapeDtypeStruct((BLOCK, 128), BF16),
            jax.ShapeDtypeStruct((8, BLOCK), F32),
            jax.ShapeDtypeStruct((BLOCK, 8), F32),
        ),
        name="ssd_local",
    )(ids, rate, act, *rim, step, offset, conv_weight, conv_weight, buf)


def inner_kernel(
    ids, act_ref, cc_ref, xin_ref, bkey_ref, rows_ref, cols_ref,
    yin_ref, gate_ref, cq_ref, q_ref, wide_ref,
):
    gate_ref[...] = silu(added(act_ref, 0, 256)[HALO:].astype(F32))
    q_ref[...] = added(act_ref, 384, 256)[HALO:]
    wide_ref[...] = added(act_ref, 256, 128).astype(F32)
    cquery = convolved(wide_ref, cc_ref[...])
    cq_ref[...] = cquery
    lower = iota((BLOCK, BLOCK), 0) >= iota((BLOCK, BLOCK), 1)
    inner = lax.dot_general(cquery, bkey_ref[...], NT, preferred_element_type=F32)
    for h in range(4):
        spread = cols_ref[:, h : h + 1] - rows_ref[h : h + 1, :]
        decayed = jnp.exp(jnp.where(lower, spread, 0.0))
        mix = jnp.where(lower, inner * decayed * rows_ref[4 + h : 5 + h, :], 0.0).astype(BF16)
        yin_ref[:, h * 64 : (h + 1) * 64] = jnp.dot(
            mix, xin_ref[:, h * 64 : (h + 1) * 64], preferred_element_type=F32
        )


def inner_call(ids, act, conv_weight, xin, bkey, rows, cols):
    full = lambda *shape: pl.BlockSpec(shape, lambda i, ids: (0,) * len(shape))
    return pl.pallas_call(
        inner_kernel,
        grid_spec=pltpu.PrefetchScalarGridSpec(
            num_scalar_prefetch=1,
            grid=(1,),
            in_specs=[
                full(*act.shape),
                pl.BlockSpec((CONV, 128), lambda i, ids: (0, 24 + ids[1])),
                full(BLOCK, 256), full(BLOCK, 128), full(8, BLOCK), full(BLOCK, 8),
            ],
            out_specs=[full(BLOCK, 256), full(BLOCK, 256), full(BLOCK, 128), full(BLOCK, 256)],
            scratch_shapes=[pltpu.VMEM((BLOCK + HALO, 128), F32)],
        ),
        out_shape=(
            jax.ShapeDtypeStruct((BLOCK, 256), F32),
            jax.ShapeDtypeStruct((BLOCK, 256), F32),
            jax.ShapeDtypeStruct((BLOCK, 128), BF16),
            jax.ShapeDtypeStruct((BLOCK, 256), BF16),
        ),
        compiler_params=vmem(),
        name="ssd_inner",
    )(ids, act, conv_weight, xin, bkey, rows, cols)


KEYS = 512
KEPT = BLOCK + 80
SENT = KEPT + 64
LOG2E = 1.4426950408889634


def attend_kernel(
    ids, bias, q_ref, yin_ref, gate_ref, cq_ref, cols_ref, gain_ref, all_hbm, a0, a1, a2, a3,
    out_ref, kv_ref, st_ref, wm_ref, wa_ref, acc_ref, late_ref, hold_ref, sems, ksems, gsems,
):
    block, tensor, mine = ids[0], ids[1], ids[2]
    per = KEYS // BLOCK
    count = all_hbm.shape[0]
    chunks = range(count // per - 1, -1, -1)
    last = block // per

    def move(chunk):
        picked = pl.ds(chunk * per, per)
        return pltpu.make_async_copy(
            all_hbm.at[picked, pl.ds(0, BLOCK)], kv_ref.at[picked], ksems.at[chunk]
        )

    def states(group):
        picked = pl.ds(group * per, per)
        return pltpu.make_async_copy(
            all_hbm.at[picked, pl.ds(BLOCK, 80)], st_ref.at[picked], gsems.at[group]
        )

    weights = [pltpu.make_async_copy(all_hbm.at[:, pl.ds(KEPT, 64)], wm_ref, sems.at[0])]
    weights += [
        pltpu.make_async_copy(w, wa_ref.at[(mine + 4 - r) % 4], sems.at[1 + r])
        for r, w in enumerate((a0, a1, a2, a3))
    ]
    for group in range(count // per):
        pl.when(group * per < block)(lambda group=group: states(group).start())
    for chunk in chunks:
        pl.when((chunk <= last) & (chunk >= last - 1))(lambda chunk=chunk: move(chunk).start())
    acc_ref[...] = jnp.zeros_like(acc_ref)
    late_ref[...] = jnp.zeros_like(late_ref)
    hold_ref[...] = jnp.zeros_like(hold_ref)
    for group in range(count // per):
        pl.when(group * per < block)(lambda group=group: states(group).wait())

    def advance(k, carry):
        logs = st_ref[k, 64:80, :].astype(F32)
        decay = jnp.exp(logs[0:8] + logs[8:16])
        hold_ref[...] = hold_ref[...] * jnp.concatenate([decay] * 8, axis=0) + st_ref[
            k, 0:64, :
        ].astype(F32)
        return carry

    lax.fori_loop(0, block, advance, 0)
    cquery = cq_ref[...]
    ys = []
    for h in range(4):
        enter = hold_ref[:, h * 128 : (h + 1) * 128].astype(BF16)
        moved = lax.dot_general(cquery, enter, NT, preferred_element_type=F32)
        ys.append(moved * jnp.exp(cols_ref[:, h : h + 1]))
    gated = (yin_ref[...] + jnp.concatenate(ys, axis=1)) * gate_ref[...]
    scale = lax.rsqrt(jnp.mean(gated * gated, axis=-1, keepdims=True) + EPS)
    mixed = (gated * scale * gain_ref[...]).astype(BF16)
    row = iota((256, 256), 0) % 128
    col = iota((256, 256), 1)
    onward = ((row > col) | (col >= 128)).astype(BF16)

    def piece(turn, carry):
        chunk = last - turn
        move(chunk).wait()
        pl.when(chunk > 1)(lambda: move(chunk - 2).start())

        @pl.when(turn == jnp.minimum(last, 1))
        def _():
            for copy in weights:
                copy.start()

        picked = pl.ds(chunk * per, per)
        before = [
            chunk * KEYS + sub * BLOCK + iota((BLOCK, BLOCK), 1)
            < block * BLOCK + iota((BLOCK, BLOCK), 0)
            for sub in range(per)
        ]
        taken, parts = {}, []
        for h in range(2):
            query = q_ref[:, h * 128 : (h + 1) * 128]
            key = kv_ref[picked, :, h * 128 : (h + 1) * 128].reshape(KEYS, 128)
            logits = lax.dot_general(query, key, NT, preferred_element_type=F32)
            logits = logits * (128 ** -0.5 * LOG2E) + bias[2 * tensor + h] * LOG2E
            soft = jnp.maximum(logits, 0.0) + LOG2E * jnp.log(1.0 + jnp.exp2(-jnp.abs(logits)))
            for sub in range(per):
                at = slice(sub * BLOCK, (sub + 1) * BLOCK)
                taken[h, sub] = logits[:, at] - soft[:, at]
                kept = jnp.where(before[sub], soft[:, at], 0.0)
                high = kept.astype(BF16)
                low = (kept - high.astype(F32)).astype(BF16)
                parts.append(jnp.concatenate([high, low], axis=1))
        sums = jnp.dot(jnp.concatenate(parts, axis=0), onward, preferred_element_type=F32)
        for h in range(2):
            late = late_ref[h]
            weights_h = [None] * per
            for sub in range(per - 1, -1, -1):
                at = (h * per + sub) * BLOCK
                mine_sums = sums[at : at + BLOCK]
                weight = jnp.exp2(taken[h, sub] - (mine_sums[:, 0:128] + late))
                weights_h[sub] = jnp.where(before[sub], weight, 0.0).astype(BF16)
                late = late + mine_sums[:, 128:256]
            value = kv_ref[picked, :, 256 + h * 128 : 256 + (h + 1) * 128].reshape(KEYS, 128)
            acc_ref[h] += jnp.dot(
                jnp.concatenate(weights_h, axis=1), value, preferred_element_type=F32
            )
            late_ref[h] = late
        return carry

    lax.fori_loop(0, last + 1, piece, 0)
    attended = jnp.concatenate([acc_ref[0].astype(BF16), acc_ref[1].astype(BF16)], axis=1)
    for copy in weights:
        copy.wait()
    for s in range(count):
        halves = []
        for f in range(4):
            for half in range(2):
                halves.append(
                    wm_ref[s, 16 * f : 16 * (f + 1), 256 * half : 256 * (half + 1)]
                )
        rows_m = jnp.concatenate(halves, axis=0)
        rows_a = jnp.concatenate(
            [wa_ref[f, 32 * s : 32 * (s + 1), :] for f in range(4)], axis=0
        )
        out_ref[:, 128 * s : 128 * (s + 1)] = (
            lax.dot_general(mixed, rows_m, NT, preferred_element_type=F32)
            + lax.dot_general(attended, rows_a, NT, preferred_element_type=F32)
        ).astype(BF16)


def attend_call(ids, bias, q, yin, gate, cq, cols, gain, gathered, rows):
    full = lambda *shape: pl.BlockSpec(shape, lambda i, ids, bias: (0,) * len(shape))
    count = gathered.shape[0]
    near = pl.BlockSpec(memory_space=pltpu.VMEM)
    return pl.pallas_call(
        attend_kernel,
        grid_spec=pltpu.PrefetchScalarGridSpec(
            num_scalar_prefetch=2,
            grid=(1,),
            in_specs=[
                full(BLOCK, 256), full(BLOCK, 256), full(BLOCK, 256), full(BLOCK, 128),
                full(BLOCK, 8), pl.BlockSpec((1, 256), lambda i, ids, bias: (0, ids[1])),
                pl.BlockSpec(memory_space=pltpu.HBM), near, near, near, near,
            ],
            out_specs=full(BLOCK, 2048),
            scratch_shapes=[
                pltpu.VMEM((count, BLOCK, 512), BF16),
                pltpu.VMEM((count, 80, 512), BF16),
                pltpu.VMEM((count, 64, 512), BF16),
                pltpu.VMEM((4, 512, 256), BF16),
                pltpu.VMEM((2, BLOCK, 128), F32),
                pltpu.VMEM((2, BLOCK, 128), F32),
                pltpu.VMEM((64, 512), F32),
                pltpu.SemaphoreType.DMA((5,)),
                pltpu.SemaphoreType.DMA((count * BLOCK // KEYS,)),
                pltpu.SemaphoreType.DMA((count * BLOCK // KEYS,)),
            ],
        ),
        out_shape=jax.ShapeDtypeStruct((BLOCK, 2048), BF16),
        compiler_params=vmem(),
        name="attend",
    )(ids, bias, q, yin, gate, cq, cols, gain.reshape(1, -1), gathered, *rows)


def rotated(shard, axis, by):
    length = lax.axis_size(axis)
    return lax.ppermute(shard, axis, [(i, (i + by) % length) for i in range(length)])


def body(
    inputs, norm_gain, w_gate, w_input, w_bkey, w_cquery, w_step, conv_weight, decay_rate,
    decay_offset, ssd_gain, w_query, w_key, w_value, stick_bias, out_mixer, out_attend,
):
    length = lax.axis_size("sp")
    ids = jnp.stack([lax.axis_index(name) for name in ("sp", "tp", "fs")]).astype(jnp.int32)
    split, step, first, second = prep_call(
        inputs, norm_gain, w_step.T, w_key, w_value, w_input, w_bkey, w_gate, w_cquery, w_query,
        out_attend.T, out_mixer.T,
    )
    tokens = lax.all_to_all(split, "fs", 0, 0, tiled=True)
    early = lax.all_gather(first, "sp", axis=0, tiled=True)
    tokens, early = lax.optimization_barrier((tokens, early))
    rim = lax.ppermute(
        tokens[:, BLOCK - HALO : BLOCK], "sp", [(i, i + 1) for i in range(length - 1)]
    )

    def back(act):
        return lax.all_to_all(act, "fs", 0, 0, tiled=True)

    (act,) = project_call(tokens, None, early, 896)
    act = back(act)
    edge = rim_call(ids, rim, early)
    edge = [edge[0]] + [rotated(edge[by], "fs", by) for by in (1, 2, 3)]
    send, xin, bkey, srows, scols = local_call(
        ids, decay_rate, act, edge, step, decay_offset[0].T, conv_weight, tokens
    )
    gathered = lax.all_gather(send, "sp", axis=0)
    act, kept = project_call(tokens, rim, lax.all_gather(second, "sp", axis=0, tiled=True), 640)
    act = back(act)
    rows = [kept] + [rotated(kept, "fs", by) for by in (1, 2, 3)]
    yin, gate, cq, q = inner_call(ids, act, conv_weight, xin, bkey, srows, scols)
    partial = attend_call(ids, stick_bias, q, yin, gate, cq, scols, ssd_gain, gathered, rows)
    parts = lax.all_to_all(partial.reshape(8, 16, 2048), "tp", 0, 0, tiled=True)
    return jnp.sum(parts.astype(F32), axis=0).astype(BF16)[None]


def solution(mesh):
    shard = P(("sp", "fs"), "tp")
    return jax.shard_map(
        body,
        mesh=mesh,
        in_specs=(
            P("fs", "sp", None), P(), shard, shard, shard, shard, P(), P(), P(),
            P("fs", "sp", "tp"), P(), shard, shard, shard, P(),
            P("tp", ("sp", "fs")), P("tp", ("sp", "fs")),
        ),
        out_specs=P("fs", ("sp", "tp"), None),
        check_vma=False,
    )
```

```python
import functools

import jax
import jax.numpy as jnp
from jax import lax
from jax.experimental import pallas as pl
from jax.experimental.pallas import tpu as pltpu
from jax.sharding import PartitionSpec as P


BLOCK = 128
CONV = 4
EPS = 1e-06
HALO = 16
ROWS = BLOCK + HALO
F32 = jnp.float32
BF16 = jnp.bfloat16
HIGH = lax.Precision.HIGHEST
NT = (((1,), (1,)), ((), ()))
TN = (((0,), (0,)), ((), ()))


def vmem(limit=48):
    return pltpu.CompilerParams(vmem_limit_bytes=limit * 1024 * 1024)


def iota(shape, dim):
    return lax.broadcasted_iota(jnp.int32, shape, dim)


def softplus(x):
    return jnp.maximum(x, 0.0) + jnp.log1p(jnp.exp(-jnp.abs(x)))


def silu(x):
    return x / (1.0 + jnp.exp(-x))


def pull(pairs, sems):
    copies = [pltpu.make_async_copy(src, dst, sems.at[i]) for i, (src, dst) in enumerate(pairs)]
    for copy in copies:
        copy.start()
    return copies


def shuffled(normed, f, g):
    lane = iota((normed.shape[0], 128), 1) // 32
    out = None
    for k in range(4):
        at = (4 * g + k) * 128
        piece = normed[:, at : at + 128]
        shift = ((k - f) * 32) % 128
        if shift:
            piece = pltpu.roll(piece, shift, 1)
        out = piece if out is None else jnp.where(lane == k, piece, out)
    return out.astype(BF16)


def normalised(x, gain):
    wide = x.astype(F32)
    scale = lax.rsqrt(jnp.mean(wide * wide, axis=-1, keepdims=True) + EPS)
    return (wide * scale * gain).astype(BF16)


def prep_kernel(*refs):
    x_hbm, gain_hbm, ws_hbm = refs[:3]
    sources = refs[3:12]
    xs_ref, step_ref, first_ref, second_ref = refs[12:16]
    x_ref, gain_ref, ws_ref, third_ref, sems, wsems = refs[16:]
    early = pull(((x_hbm.at[0], x_ref), (gain_hbm, gain_ref), (ws_hbm, ws_ref)), sems)
    pairs = []
    outs = (first_ref, second_ref, third_ref)
    at, which = 0, 0
    for n, src in enumerate(sources):
        if n in (4, 8):
            at, which = 0, which + 1
        pairs.append((src, outs[which].at[:, pl.ds(at, src.shape[1])]))
        at += src.shape[1]
    later = pull(pairs, wsems)
    for copy in early:
        copy.wait()
    normed = normalised(x_ref[...], gain_ref[...])
    step_ref[...] = softplus(
        lax.dot_general(ws_ref[...], normed, NT, preferred_element_type=F32)
    )
    wide = normed.astype(F32)
    for f in range(4):
        for g in range(4):
            xs_ref[f, 0:BLOCK, g * 128 : (g + 1) * 128] = shuffled(wide, f, g)
    for copy in later:
        copy.wait()
    for f in range(4):
        xs_ref[f, BLOCK:, 0:256] = third_ref[0:16, :]
        xs_ref[f, BLOCK:, 256:512] = third_ref[16:32, :]


def prep_call(inputs, gain, w_step_t, *arrays):
    rows, width = inputs.shape[1:]
    heads = w_step_t.shape[0]
    part = arrays[0].shape[0]
    widths = [sum(a.shape[1] for a in group) for group in (arrays[:4], arrays[4:8], arrays[8:])]
    hbm = pl.BlockSpec(memory_space=pltpu.HBM)
    return pl.pallas_call(
        prep_kernel,
        in_specs=[hbm] * 12,
        out_shape=(
            jax.ShapeDtypeStruct((4, rows + HALO, width // 4), BF16),
            jax.ShapeDtypeStruct((heads, rows), F32),
            jax.ShapeDtypeStruct((part, widths[0]), BF16),
            jax.ShapeDtypeStruct((part, widths[1]), BF16),
        ),
        scratch_shapes=[
            pltpu.VMEM((rows, width), BF16),
            pltpu.VMEM((1, width), F32),
            pltpu.VMEM((heads, width), BF16),
            pltpu.VMEM((part, widths[2]), BF16),
            pltpu.SemaphoreType.DMA((3,)),
            pltpu.SemaphoreType.DMA((9,)),
        ],
        name="prep",
    )(inputs, gain.reshape(1, -1), w_step_t, *arrays)


def project_kernel(has_rim, x_ref, *rest):
    rim_ref, rest = (rest[0], rest[1:]) if has_rim else (None, rest)
    w_ref, out_hbm = rest[:2]
    kept, (out_ref, sems) = rest[2:-2], rest[-2:]
    width = out_hbm.shape[2]
    weights = w_ref[:, 0:width]
    copies = []
    for f in range(4):
        rows = x_ref[f, 0:BLOCK, :]
        if has_rim:
            rows = jnp.concatenate([rim_ref[f], rows], axis=0)
        out_ref[f] = jnp.dot(rows, weights, preferred_element_type=F32)
        copies.append(pltpu.make_async_copy(out_ref.at[f], out_hbm.at[f], sems.at[f]))
        copies[-1].start()
    for ref in kept:
        ref[...] = w_ref[:, width:]
    for copy in copies:
        copy.wait()


def project_call(x, rim, w, width):
    whole = pl.BlockSpec(memory_space=pltpu.VMEM)
    rows = BLOCK if rim is None else ROWS
    outs = [jax.ShapeDtypeStruct((4, rows, width), F32)]
    specs = [pl.BlockSpec(memory_space=pltpu.HBM)]
    if w.shape[1] > width:
        outs.append(jax.ShapeDtypeStruct((w.shape[0], w.shape[1] - width), BF16))
        specs.append(whole)
    given = [x, w] if rim is None else [x, rim, w]
    return pl.pallas_call(
        functools.partial(project_kernel, rim is not None),
        in_specs=[whole] * len(given),
        out_specs=specs,
        out_shape=outs,
        scratch_shapes=[pltpu.VMEM((4, rows, width), F32), pltpu.SemaphoreType.DMA((4,))],
        compiler_params=vmem(),
        name="project",
    )(*given)


def rim_kernel(ids, rim_ref, w_ref, *outs):
    rows = rim_ref[...].reshape(4 * HALO, 512)
    act = jnp.dot(rows, w_ref[:, 512:], preferred_element_type=F32)
    for f in range(4):
        for r in range(4):

            @pl.when((f + 4 - ids[2]) % 4 == r)
            def _(f=f, r=r):
                outs[r][...] = act[f * HALO + 8 : (f + 1) * HALO]


def rim_call(ids, rim, w):
    width = w.shape[1] - 512
    full = lambda *shape: pl.BlockSpec(shape, lambda i, ids: (0,) * len(shape))
    return pl.pallas_call(
        rim_kernel,
        grid_spec=pltpu.PrefetchScalarGridSpec(
            num_scalar_prefetch=1,
            grid=(1,),
            in_specs=[full(*rim.shape), full(*w.shape)],
            out_specs=[full(8, width)] * 4,
        ),
        out_shape=[jax.ShapeDtypeStruct((8, width), F32)] * 4,
        compiler_params=vmem(),
        name="project_rim",
    )(ids, rim, w)


def added(ref, at, width):
    total = ref[0, :, at : at + width].astype(F32)
    for j in range(1, 4):
        total = total + ref[j, :, at : at + width].astype(F32)
    return total.astype(BF16)


def convolved(wide_ref, taps):
    summed = None
    for i in range(CONV):
        at = HALO - CONV + 1 + i
        part = taps[i : i + 1] * wide_ref[at : at + BLOCK, :]
        summed = part if summed is None else summed + part
    return silu(summed).astype(BF16)


def local_kernel(
    ids, rate, act_ref, e0, e1, e2, e3, step_ref, off_ref, ci_ref, cb_ref, buf_ref,
    send_hbm, xin_ref, bkey_ref, rows_ref, cols_ref, wide_ref, send_ref, sems,
):
    tensor = ids[1]
    moved = pull(
        [
            (buf_ref.at[f, pl.ds(BLOCK, HALO)], send_hbm.at[pl.ds(KEPT + HALO * f, HALO)])
            for f in range(4)
        ],
        sems,
    )
    send_ref[0:BLOCK, :] = added(act_ref, 0, 512)
    moved.append(
        pltpu.make_async_copy(
            send_ref.at[pl.ds(0, BLOCK)], send_hbm.at[pl.ds(0, BLOCK)], sems.at[4]
        )
    )
    moved[-1].start()
    edge = e0[...].astype(F32) + e1[...].astype(F32)
    edge = edge + (e2[...].astype(F32) + e3[...].astype(F32))
    wide_ref[8:HALO, :] = edge.astype(BF16).astype(F32)
    wide_ref[HALO:, :] = added(act_ref, 512, 384).astype(F32)
    conv = convolved(wide_ref, jnp.concatenate([ci_ref[...], cb_ref[...]], axis=1))
    xin, bkey = conv[:, 0:256], conv[:, 256:384]
    xin_ref[...] = xin
    bkey_ref[...] = bkey
    row = iota((BLOCK, BLOCK), 0)
    col = iota((BLOCK, BLOCK), 1)
    step = jnp.concatenate([step_ref[pl.ds(4 * tensor + h, 1), :] for h in range(4)], axis=0)
    rates = jnp.concatenate(
        [jnp.full((1, BLOCK), rate[4 * tensor + h], F32) for h in range(4)], axis=0
    )
    decay = off_ref[...] - rates * step
    decay8 = jnp.concatenate([decay, jnp.zeros((4, BLOCK), F32)], axis=0)
    upper = (row <= col).astype(F32)
    cum = jnp.dot(decay8, upper, precision=HIGH, preferred_element_type=F32)
    last = jnp.sum(decay, axis=1, keepdims=True)
    to_end = jnp.exp(last - cum[0:4]) * step
    eye = (row == col).astype(F32)
    cols = lax.dot_general(
        eye, jnp.concatenate([cum[0:4], to_end], axis=0), NT, precision=HIGH,
        preferred_element_type=F32,
    )
    rows_ref[...] = jnp.concatenate([cum[0:4], step], axis=0)
    cols_ref[...] = cols
    wide_key = bkey.astype(F32)
    for h in range(4):
        wk = (wide_key * cols[:, 4 + h : 5 + h]).astype(BF16)
        state = lax.dot_general(
            xin[:, h * 64 : (h + 1) * 64], wk, TN, preferred_element_type=F32
        )
        log = jnp.broadcast_to(last[h : h + 1], (8, BLOCK))
        high = log.astype(BF16).astype(F32)
        logs = jnp.concatenate([high, log - high], axis=0).astype(BF16)
        send_ref[BLOCK : BLOCK + 64, h * 128 : (h + 1) * 128] = state.astype(BF16)
        send_ref[BLOCK + 64 : KEPT, h * 128 : (h + 1) * 128] = logs
    kept = pl.ds(BLOCK, KEPT - BLOCK)
    moved.append(pltpu.make_async_copy(send_ref.at[kept], send_hbm.at[kept], sems.at[5]))
    moved[-1].start()
    for copy in moved:
        copy.wait()


def local_call(ids, rate, act, rim, step, offset, conv_weight, buf):
    full = lambda *shape: pl.BlockSpec(shape, lambda i, ids, rate: (0,) * len(shape))
    return pl.pallas_call(
        local_kernel,
        grid_spec=pltpu.PrefetchScalarGridSpec(
            num_scalar_prefetch=2,
            grid=(1,),
            in_specs=[
                full(*act.shape),
                *(full(*e.shape) for e in rim),
                full(*step.shape),
                full(*offset.shape),
                pl.BlockSpec((CONV, 256), lambda i, ids, rate: (0, ids[1])),
                pl.BlockSpec((CONV, 128), lambda i, ids, rate: (0, 16 + ids[1])),
                pl.BlockSpec(memory_space=pl.ANY),
            ],
            out_specs=[
                pl.BlockSpec(memory_space=pltpu.HBM), full(BLOCK, 256), full(BLOCK, 128),
                full(8, BLOCK),
                full(BLOCK, 8),
            ],
            scratch_shapes=[
                pltpu.VMEM((ROWS, 384), F32),
                pltpu.VMEM((KEPT, 512), BF16),
                pltpu.SemaphoreType.DMA((6,)),
            ],
        ),
        out_shape=(
            jax.ShapeDtypeStruct((SENT, 512), BF16),
            jax.ShapeDtypeStruct((BLOCK, 256), BF16),
            jax.ShapeDtypeStruct((BLOCK, 128), BF16),
            jax.ShapeDtypeStruct((8, BLOCK), F32),
            jax.ShapeDtypeStruct((BLOCK, 8), F32),
        ),
        name="ssd_local",
    )(ids, rate, act, *rim, step, offset, conv_weight, conv_weight, buf)


def inner_kernel(
    ids, act_ref, cc_ref, xin_ref, bkey_ref, rows_ref, cols_ref,
    yin_ref, gate_ref, cq_ref, q_ref, wide_ref,
):
    gate_ref[...] = silu(added(act_ref, 0, 256)[HALO:].astype(F32))
    q_ref[...] = added(act_ref, 384, 256)[HALO:]
    wide_ref[...] = added(act_ref, 256, 128).astype(F32)
    cquery = convolved(wide_ref, cc_ref[...])
    cq_ref[...] = cquery
    lower = iota((BLOCK, BLOCK), 0) >= iota((BLOCK, BLOCK), 1)
    inner = lax.dot_general(cquery, bkey_ref[...], NT, preferred_element_type=F32)
    for h in range(4):
        spread = cols_ref[:, h : h + 1] - rows_ref[h : h + 1, :]
        decayed = jnp.exp(jnp.where(lower, spread, 0.0))
        mix = jnp.where(lower, inner * decayed * rows_ref[4 + h : 5 + h, :], 0.0).astype(BF16)
        yin_ref[:, h * 64 : (h + 1) * 64] = jnp.dot(
            mix, xin_ref[:, h * 64 : (h + 1) * 64], preferred_element_type=F32
        )


def inner_call(ids, act, conv_weight, xin, bkey, rows, cols):
    full = lambda *shape: pl.BlockSpec(shape, lambda i, ids: (0,) * len(shape))
    return pl.pallas_call(
        inner_kernel,
        grid_spec=pltpu.PrefetchScalarGridSpec(
            num_scalar_prefetch=1,
            grid=(1,),
            in_specs=[
                full(*act.shape),
                pl.BlockSpec((CONV, 128), lambda i, ids: (0, 24 + ids[1])),
                full(BLOCK, 256), full(BLOCK, 128), full(8, BLOCK), full(BLOCK, 8),
            ],
            out_specs=[full(BLOCK, 256), full(BLOCK, 256), full(BLOCK, 128), full(BLOCK, 256)],
            scratch_shapes=[pltpu.VMEM((BLOCK + HALO, 128), F32)],
        ),
        out_shape=(
            jax.ShapeDtypeStruct((BLOCK, 256), F32),
            jax.ShapeDtypeStruct((BLOCK, 256), F32),
            jax.ShapeDtypeStruct((BLOCK, 128), BF16),
            jax.ShapeDtypeStruct((BLOCK, 256), BF16),
        ),
        compiler_params=vmem(),
        name="ssd_inner",
    )(ids, act, conv_weight, xin, bkey, rows, cols)


KEYS = 512
KEPT = BLOCK + 80
SENT = KEPT + 64
LOG2E = 1.4426950408889634


def attend_kernel(
    ids, bias, q_ref, yin_ref, gate_ref, cq_ref, cols_ref, gain_ref, all_hbm, a0, a1, a2, a3,
    out_ref, kv_ref, st_ref, wm_ref, wa_ref, acc_ref, late_ref, hold_ref, sems, ksems, gsems,
):
    block, tensor, mine = ids[0], ids[1], ids[2]
    per = KEYS // BLOCK
    count = all_hbm.shape[0]
    chunks = range(count // per - 1, -1, -1)
    last = block // per

    def move(chunk):
        picked = pl.ds(chunk * per, per)
        return pltpu.make_async_copy(
            all_hbm.at[picked, pl.ds(0, BLOCK)], kv_ref.at[picked], ksems.at[chunk]
        )

    def states(group):
        picked = pl.ds(group * per, per)
        return pltpu.make_async_copy(
            all_hbm.at[picked, pl.ds(BLOCK, 80)], st_ref.at[picked], gsems.at[group]
        )

    weights = [pltpu.make_async_copy(all_hbm.at[:, pl.ds(KEPT, 64)], wm_ref, sems.at[0])]
    weights += [
        pltpu.make_async_copy(w, wa_ref.at[(mine + 4 - r) % 4], sems.at[1 + r])
        for r, w in enumerate((a0, a1, a2, a3))
    ]
    for group in range(count // per):
        pl.when(group * per < block)(lambda group=group: states(group).start())
    for chunk in chunks:
        pl.when((chunk <= last) & (chunk >= last - 1))(lambda chunk=chunk: move(chunk).start())
    acc_ref[...] = jnp.zeros_like(acc_ref)
    late_ref[...] = jnp.zeros_like(late_ref)
    hold_ref[...] = jnp.zeros_like(hold_ref)
    for group in range(count // per):
        pl.when(group * per < block)(lambda group=group: states(group).wait())

    def advance(k, carry):
        logs = st_ref[k, 64:80, :].astype(F32)
        decay = jnp.exp(logs[0:8] + logs[8:16])
        hold_ref[...] = hold_ref[...] * jnp.concatenate([decay] * 8, axis=0) + st_ref[
            k, 0:64, :
        ].astype(F32)
        return carry

    lax.fori_loop(0, block, advance, 0)
    cquery = cq_ref[...]
    ys = []
    for h in range(4):
        enter = hold_ref[:, h * 128 : (h + 1) * 128].astype(BF16)
        moved = lax.dot_general(cquery, enter, NT, preferred_element_type=F32)
        ys.append(moved * jnp.exp(cols_ref[:, h : h + 1]))
    gated = (yin_ref[...] + jnp.concatenate(ys, axis=1)) * gate_ref[...]
    scale = lax.rsqrt(jnp.mean(gated * gated, axis=-1, keepdims=True) + EPS)
    mixed = (gated * scale * gain_ref[...]).astype(BF16)
    row = iota((256, 256), 0) % 128
    col = iota((256, 256), 1)
    onward = ((row > col) | (col >= 128)).astype(BF16)

    def piece(turn, carry):
        chunk = last - turn
        move(chunk).wait()
        pl.when(chunk > 1)(lambda: move(chunk - 2).start())

        @pl.when(turn == jnp.minimum(last, 1))
        def _():
            for copy in weights:
                copy.start()

        picked = pl.ds(chunk * per, per)
        before = [
            chunk * KEYS + sub * BLOCK + iota((BLOCK, BLOCK), 1)
            < block * BLOCK + iota((BLOCK, BLOCK), 0)
            for sub in range(per)
        ]
        taken, parts = {}, []
        for h in range(2):
            query = q_ref[:, h * 128 : (h + 1) * 128]
            key = kv_ref[picked, :, h * 128 : (h + 1) * 128].reshape(KEYS, 128)
            logits = lax.dot_general(query, key, NT, preferred_element_type=F32)
            logits = logits * (128 ** -0.5 * LOG2E) + bias[2 * tensor + h] * LOG2E
            soft = jnp.maximum(logits, 0.0) + LOG2E * jnp.log(1.0 + jnp.exp2(-jnp.abs(logits)))
            for sub in range(per):
                at = slice(sub * BLOCK, (sub + 1) * BLOCK)
                taken[h, sub] = logits[:, at] - soft[:, at]
                kept = jnp.where(before[sub], soft[:, at], 0.0)
                high = kept.astype(BF16)
                low = (kept - high.astype(F32)).astype(BF16)
                parts.append(jnp.concatenate([high, low], axis=1))
        sums = jnp.dot(jnp.concatenate(parts, axis=0), onward, preferred_element_type=F32)
        for h in range(2):
            late = late_ref[h]
            weights_h = [None] * per
            for sub in range(per - 1, -1, -1):
                at = (h * per + sub) * BLOCK
                mine_sums = sums[at : at + BLOCK]
                weight = jnp.exp2(taken[h, sub] - (mine_sums[:, 0:128] + late))
                weights_h[sub] = jnp.where(before[sub], weight, 0.0).astype(BF16)
                late = late + mine_sums[:, 128:256]
            value = kv_ref[picked, :, 256 + h * 128 : 256 + (h + 1) * 128].reshape(KEYS, 128)
            acc_ref[h] += jnp.dot(
                jnp.concatenate(weights_h, axis=1), value, preferred_element_type=F32
            )
            late_ref[h] = late
        return carry

    lax.fori_loop(0, last + 1, piece, 0)
    attended = jnp.concatenate([acc_ref[0].astype(BF16), acc_ref[1].astype(BF16)], axis=1)
    for copy in weights:
        copy.wait()
    for s in range(count):
        halves = []
        for f in range(4):
            for half in range(2):
                halves.append(
                    wm_ref[s, 16 * f : 16 * (f + 1), 256 * half : 256 * (half + 1)]
                )
        rows_m = jnp.concatenate(halves, axis=0)
        rows_a = jnp.concatenate(
            [wa_ref[f, 32 * s : 32 * (s + 1), :] for f in range(4)], axis=0
        )
        out_ref[:, 128 * s : 128 * (s + 1)] = (
            lax.dot_general(mixed, rows_m, NT, preferred_element_type=F32)
            + lax.dot_general(attended, rows_a, NT, preferred_element_type=F32)
        ).astype(BF16)


def attend_call(ids, bias, q, yin, gate, cq, cols, gain, gathered, rows):
    full = lambda *shape: pl.BlockSpec(shape, lambda i, ids, bias: (0,) * len(shape))
    count = gathered.shape[0]
    near = pl.BlockSpec(memory_space=pltpu.VMEM)
    return pl.pallas_call(
        attend_kernel,
        grid_spec=pltpu.PrefetchScalarGridSpec(
            num_scalar_prefetch=2,
            grid=(1,),
            in_specs=[
                full(BLOCK, 256), full(BLOCK, 256), full(BLOCK, 256), full(BLOCK, 128),
                full(BLOCK, 8), pl.BlockSpec((1, 256), lambda i, ids, bias: (0, ids[1])),
                pl.BlockSpec(memory_space=pltpu.HBM), near, near, near, near,
            ],
            out_specs=full(BLOCK, 2048),
            scratch_shapes=[
                pltpu.VMEM((count, BLOCK, 512), BF16),
                pltpu.VMEM((count, 80, 512), BF16),
                pltpu.VMEM((count, 64, 512), BF16),
                pltpu.VMEM((4, 512, 256), BF16),
                pltpu.VMEM((2, BLOCK, 128), F32),
                pltpu.VMEM((2, BLOCK, 128), F32),
                pltpu.VMEM((64, 512), F32),
                pltpu.SemaphoreType.DMA((5,)),
                pltpu.SemaphoreType.DMA((count * BLOCK // KEYS,)),
                pltpu.SemaphoreType.DMA((count * BLOCK // KEYS,)),
            ],
        ),
        out_shape=jax.ShapeDtypeStruct((BLOCK, 2048), BF16),
        compiler_params=vmem(),
        name="attend",
    )(ids, bias, q, yin, gate, cq, cols, gain.reshape(1, -1), gathered, *rows)


def rotated(shard, axis, by):
    length = lax.axis_size(axis)
    return lax.ppermute(shard, axis, [(i, (i + by) % length) for i in range(length)])


def body(
    inputs, norm_gain, w_gate, w_input, w_bkey, w_cquery, w_step, conv_weight, decay_rate,
    decay_offset, ssd_gain, w_query, w_key, w_value, stick_bias, out_mixer, out_attend,
):
    length = lax.axis_size("sp")
    ids = jnp.stack([lax.axis_index(name) for name in ("sp", "tp", "fs")]).astype(jnp.int32)
    split, step, first, second = prep_call(
        inputs, norm_gain, w_step.T, w_key, w_value, w_input, w_bkey, w_gate, w_cquery, w_query,
        out_attend.T, out_mixer.T,
    )
    tokens = lax.all_to_all(split, "fs", 0, 0, tiled=True)
    early = lax.all_gather(first, "sp", axis=0, tiled=True)
    tokens, early = lax.optimization_barrier((tokens, early))
    rim = lax.ppermute(
        tokens[:, BLOCK - HALO : BLOCK], "sp", [(i, i + 1) for i in range(length - 1)]
    )

    def back(act):
        return lax.all_to_all(act, "fs", 0, 0, tiled=True)

    (act,) = project_call(tokens, None, early, 896)
    act = back(act)
    edge = rim_call(ids, rim, early)
    edge = [edge[0]] + [rotated(edge[by], "fs", by) for by in (1, 2, 3)]
    send, xin, bkey, srows, scols = local_call(
        ids, decay_rate, act, edge, step, decay_offset[0].T, conv_weight, tokens
    )
    gathered = lax.all_gather(send, "sp", axis=0)
    act, kept = project_call(tokens, rim, lax.all_gather(second, "sp", axis=0, tiled=True), 640)
    act = back(act)
    rows = [kept] + [rotated(kept, "fs", by) for by in (1, 2, 3)]
    yin, gate, cq, q = inner_call(ids, act, conv_weight, xin, bkey, srows, scols)
    partial = attend_call(ids, stick_bias, q, yin, gate, cq, scols, ssd_gain, gathered, rows)
    parts = lax.all_to_all(partial.reshape(8, 16, 2048), "tp", 0, 0, tiled=True)
    return jnp.sum(parts.astype(F32), axis=0).astype(BF16)[None]


def solution(mesh):
    shard = P(("sp", "fs"), "tp")
    return jax.shard_map(
        body,
        mesh=mesh,
        in_specs=(
            P("fs", "sp", None), P(), shard, shard, shard, shard, P(), P(), P(),
            P("fs", "sp", "tp"), P(), shard, shard, shard, P(),
            P("tp", ("sp", "fs")), P("tp", ("sp", "fs")),
        ),
        out_specs=P("fs", ("sp", "tp"), None),
        check_vma=False,
    )
```
